512 devices in a mesh: ep: 128 (over z, x, core), tp: 4 (over y).
Axes of the slice: x: 4, y: 4, z: 16, core: 2. Of those that a mesh axis runs over, the one named last changes fastest.
Arguments:
- tokens: bfloat16 [512, 2048], P('ep'), may hold values from -6 to 6
- norm_gain: bfloat16 [2048], replicated, may hold values from 0.099609375 to 1.8984375
- in_weight: bfloat16 [2048, 1024], P(None, 'tp'), may hold values from -0.125 to 0.125
- decay_rate: float32 [64, 64], P('tp'), may hold values from 0.05 to 1
- frequency: float32 [64, 64], P('tp'), may hold values from -3 to 3
- log_step: float32 [64], P('tp'), may hold values from -2.3 to 0.7
- input_real: float32 [64, 64, 16], P('tp'), may hold values from -1.75 to 1.75
- input_imag: float32 [64, 64, 16], P('tp'), may hold values from -1.75 to 1.75
- output_real: float32 [64, 16, 64], P('tp'), may hold values from -0.5 to 0.5
- output_imag: float32 [64, 16, 64], P('tp'), may hold values from -0.5 to 0.5
- skip_gain: float32 [1024], P('tp'), may hold values from -3 to 3
- state_real: float32 [512, 64, 64], P('ep', 'tp'), may hold values from -6 to 6
- state_imag: float32 [512, 64, 64], P('ep', 'tp'), may hold values from -6 to 6
- out_weight: bfloat16 [1024, 2048], P('tp'), may hold values from -0.1875 to 0.1875
- ffn_gain: bfloat16 [2048], replicated, may hold values from 0.099609375 to 1.8984375
- expert_ids: int32 [512, 2], replicated, may hold values from 0 to 7, all different within a row; in each aligned block of 4 rows (0 to 3, 4 to 7, ...) at most 2 rows name the same one
- route_weights: float32 [512, 2], P('ep'), may hold values from 0.2 to 1
- gate_weight: bfloat16 [2048, 65536], P(None, ('ep', 'tp')), may hold values from -0.125 to 0.125
- up_weight: bfloat16 [2048, 65536], P(None, ('ep', 'tp')), may hold values from -0.125 to 0.125
- down_weight: bfloat16 [65536, 2048], P('ep', 'tp'), may hold values from -0.0625 to 0.0625
Outputs:
- mixed: bfloat16 [512, 2048], P('ep', 'tp')
- new_real: float32 [512, 64, 64], P('ep', 'tp')
- new_imag: float32 [512, 64, 64], P('ep', 'tp')
The draws below stay inside these ranges and needn't reach their ends.
Inputs may be any that keep to these rules, and one draw needn't show every extreme that they name: `expert_ids`: the 2 experts of a row differ. In each aligned block of 4 rows (the rows of one index of ep) no expert is named by more than 2 rows, and in some blocks one expert is named by exactly 2 rows.
All inputs are finite; a program needn't handle non-finite values.
Results may differ from the reference program's by a relative error of at most 0.007.
Values may be sent and summed in bfloat16 or wider, within the bound.
A program may use at most 64 MiB of HBM per device.

```python
import math
import jax
import jax.numpy as jnp
import numpy as np
from jax import lax

D = 2048
S5W = 1024
GROUP = 16
STATE = 64
EXPERTS = 8
TOP = 2
FF = 8192
SEQ_DEV = 4
GROUPS = 64
CAP = 2
TOKENS = 512
SPAN = 16
N_EP = 128


def block_levels(stream_key, dims, cuts, low, largest):
    factor_of, own = 1.0, jax.random.fold_in(stream_key, 6)
    for position, shards_of in cuts:
        steps = jnp.exp(jax.random.uniform(jax.random.fold_in(own, position), (shards_of,), jnp.float32, low / len(cuts), largest / len(cuts)))
        factor_of = factor_of * jnp.repeat(steps, dims[position] // shards_of).reshape([-1 if axis == position else 1 for axis in range(len(dims))])
    return factor_of


def assign_block(key, own, number, rows, amount, top, most, slope):
    sequence = jax.random.permutation(key, amount)
    packed, ordinary = load_shares(amount, rows * top, most, slope, True), load_shares(amount, rows * top, most, slope, False)
    places = jnp.arange(amount)

    def named(sizes, turn):
        used = int((sizes > 0).sum())
        fixed = max(1, used // 4)
        moved = fixed + (places - fixed + turn * (used - fixed)) % max(1, amount - fixed)
        return jnp.zeros((amount,), jnp.int32).at[sequence[jnp.where(places < fixed, places, moved)]].set(jnp.asarray(sizes, jnp.int32))

    sizes = jnp.where(number % 4 == 0, named(packed, number // 4), named(ordinary, number - number // 4 - 1))
    mixed = jax.random.permutation(jax.random.fold_in(own, 3), amount)
    donor, taker = mixed[0:amount // 2 * 2:2], mixed[1:amount // 2 * 2:2]
    slack = jnp.minimum(sizes[donor] - 1, most - sizes[taker]) // 2
    slack = jnp.where((donor == sequence[0]) | (taker == sequence[0]) | (sizes[taker] == 0), 0, jnp.maximum(slack, 0))
    moved = jax.random.randint(jax.random.fold_in(own, 4), (amount // 2,), 0, 1 << 20) % (slack + 1)
    sizes = sizes.at[donor].add(-moved).at[taker].add(moved)
    members = jnp.searchsorted(jnp.cumsum(sizes), jnp.arange(rows * top), side="right").astype(jnp.int32)
    grid = members.reshape(top, rows).T
    grid = grid[jax.random.permutation(jax.random.fold_in(own, 1), rows)]
    turn = jax.random.randint(jax.random.fold_in(own, 2), (rows, 1), 0, top)
    return jnp.take_along_axis(grid, (jnp.arange(top)[None, :] + turn) % top, axis=1)


def load_shares(amount, total, bound, slope, full):
    loads = [(1 << 20) // math.isqrt(grade ** slope) + 1 for grade in range(1, amount + 1)]
    largest = bound if full else min(bound, max(-(-total // amount), total * loads[0] // sum(loads)))
    least = 1 if total - largest >= amount - 1 else 0
    counts, rest = [largest] + [least] * (amount - 1), total - largest - least * (amount - 1)
    while rest > 0:
        candidates = [i for i in range(1, amount) if counts[i] < largest] or [i for i in range(1, amount) if counts[i] < bound]
        pool, left = sum([loads[i] for i in candidates]), rest
        for i in candidates:
            more = min(bound - counts[i], max(1, left * loads[i] // pool), rest)
            counts[i] = counts[i] + more
            rest = rest - more
    return np.array(counts)


def bell_draw(stream_key, shape, spread, most, cuts=(), held_as=jnp.bfloat16):
    entries = jax.random.normal(stream_key, shape, jnp.float32) * spread
    if len(cuts) > 0:
        entries = block_levels(stream_key, shape, cuts, -0.22, 0.18) * entries
    return jnp.clip(entries, min=-most, max=most).astype(held_as)


def setup_inputs(seed: int = 0) -> dict:
    splits = jax.random.split(jax.random.key(seed), 21)
    tokens = bell_draw(splits[0], (TOKENS, D), 1.0, 6.0, ((0, 128),))
    norm_gain = jnp.clip(1.0 + 0.18 * jax.random.normal(splits[1], (D,), jnp.float32), 0.099609375, 1.8984375).astype(jnp.bfloat16)
    in_weight = bell_draw(splits[2], (D, S5W), D ** -0.5, 0.125, ((1, 4),))
    decay_rate = jnp.clip(jnp.exp(math.log(1.0) - 2.9957323 * jax.random.uniform(splits[3], (GROUPS, STATE), jnp.float32) ** block_levels(splits[3], (GROUPS, STATE), ((0, 4),), -0.2, 0.2)), 0.05, 1.0)
    frequency = jnp.clip(jax.random.uniform(splits[4], (GROUPS, STATE), jnp.float32, -3.0, 3.0) * block_levels(splits[4], (GROUPS, STATE), ((0, 4),), -0.4, 0.0), -3.0, 3.0)
    log_step = jnp.clip(-2.3 + 3 * jax.random.uniform(splits[5], (GROUPS,), jnp.float32) ** block_levels(splits[5], (GROUPS,), ((0, 4),), -0.2, 0.2), -2.3, 0.7)
    input_real = bell_draw(splits[6], (GROUPS, STATE, GROUP), 0.3, 1.75, ((0, 4),), jnp.float32)
    input_imag = bell_draw(splits[7], (GROUPS, STATE, GROUP), 0.3, 1.75, ((0, 4),), jnp.float32)
    output_real = bell_draw(splits[8], (GROUPS, GROUP, STATE), (2 * STATE) ** -0.5, 0.5, ((0, 4),), jnp.float32)
    output_imag = bell_draw(splits[9], (GROUPS, GROUP, STATE), (2 * STATE) ** -0.5, 0.5, ((0, 4),), jnp.float32)
    skip_gain = bell_draw(splits[10], (S5W,), 0.5, 3.0, ((0, 4),), jnp.float32)
    state_real = bell_draw(splits[11], (TOKENS, GROUPS, STATE), 1.0, 6.0, ((0, 128), (1, 4)), jnp.float32)
    state_imag = bell_draw(splits[12], (TOKENS, GROUPS, STATE), 1.0, 6.0, ((0, 128), (1, 4)), jnp.float32)
    out_weight = bell_draw(splits[13], (S5W, D), S5W ** -0.5, 0.1875, ((0, 4),))
    ffn_gain = jnp.clip(1.0 + 0.18 * jax.random.normal(splits[14], (D,), jnp.float32), 0.099609375, 1.8984375).astype(jnp.bfloat16)
    expert_ids_keys = jax.random.split(jax.random.fold_in(splits[15], 1), TOKENS // SEQ_DEV)
    expert_ids_turns = jax.random.permutation(jax.random.fold_in(splits[15], 3), TOKENS // SEQ_DEV)
    expert_ids = jax.vmap(lambda own, number: assign_block(jax.random.fold_in(splits[15], 2), own, number, SEQ_DEV, EXPERTS, TOP, CAP, 2))(expert_ids_keys, expert_ids_turns).reshape((TOKENS, TOP))
    route_weights = jnp.clip(0.2 + 0.8 * jax.random.uniform(splits[16], (TOKENS, TOP), jnp.float32) ** block_levels(splits[16], (TOKENS, TOP), ((0, 128),), -0.2, 0.2), 0.2, 1.0)
    gate_weight = bell_draw(splits[17], (D, EXPERTS * FF), D ** -0.5, 0.125, ((1, 512),))
    up_weight = bell_draw(splits[18], (D, EXPERTS * FF), D ** -0.5, 0.125, ((1, 512),))
    down_weight = bell_draw(splits[19], (EXPERTS * FF, D), FF ** -0.5, 0.0625, ((0, 128), (1, 4)))
    return {"tokens": tokens, "norm_gain": norm_gain, "in_weight": in_weight, "decay_rate": decay_rate, "frequency": frequency, "log_step": log_step, "input_real": input_real, "input_imag": input_imag, "output_real": output_real, "output_imag": output_imag, "skip_gain": skip_gain, "state_real": state_real, "state_imag": state_imag, "out_weight": out_weight, "ffn_gain": ffn_gain, "expert_ids": expert_ids, "route_weights": route_weights, "gate_weight": gate_weight, "up_weight": up_weight, "down_weight": down_weight}


EPSILON = 1e-06

def rms_scale(values, gain):
    floats = values.astype(jnp.float32)
    return floats * lax.rsqrt(lax.optimization_barrier(jnp.mean(floats * floats, axis=-1, keepdims=True)) + EPSILON) * gain.astype(jnp.float32)

def discretize(decay_rate, frequency, log_step, input_real, input_imag):
    step_size = jnp.exp(log_step)[:, None]
    lam_real = -decay_rate
    magnitude = jnp.exp(lam_real * step_size)
    turned = frequency * step_size
    bar_real = magnitude * jnp.cos(turned)
    bar_imag = magnitude * jnp.sin(turned)
    denom = lam_real * lam_real + frequency * frequency
    minus_one = bar_real - 1.0
    factor_real = (minus_one * lam_real + bar_imag * frequency) / denom
    factor_imag = (bar_imag * lam_real - minus_one * frequency) / denom
    b_real = factor_real[..., None] * input_real - factor_imag[..., None] * input_imag
    b_imag = factor_real[..., None] * input_imag + factor_imag[..., None] * input_real
    return (bar_real, bar_imag, b_real, b_imag)

def state_update(projected, state_real, state_imag, decay_rate, frequency, log_step, input_real, input_imag, output_real, output_imag, skip_gain):
    bar_real, bar_imag, b_real, b_imag = discretize(decay_rate, frequency, log_step, input_real, input_imag)
    count, groups, _ = state_real.shape
    high = lax.Precision.HIGHEST
    grouped = projected.astype(jnp.float32).reshape(count, groups, -1)
    drive_real = jnp.einsum('sgp,gnp->sgn', grouped, b_real, precision=high)
    drive_imag = jnp.einsum('sgp,gnp->sgn', grouped, b_imag, precision=high)
    new_real = bar_real * state_real - bar_imag * state_imag + drive_real
    new_imag = bar_real * state_imag + bar_imag * state_real + drive_imag
    readout = jnp.einsum('sgn,gpn->sgp', new_real, output_real, precision=high) - jnp.einsum('sgn,gpn->sgp', new_imag, output_imag, precision=high)
    readout = readout.reshape(count, -1) + skip_gain * grouped.reshape(count, -1)
    return (jax.nn.gelu(readout).astype(jnp.bfloat16), new_real, new_imag)

def reference(tokens, norm_gain, in_weight, decay_rate, frequency, log_step, input_real, input_imag, output_real, output_imag, skip_gain, state_real, state_imag, out_weight, ffn_gain, expert_ids, route_weights, gate_weight, up_weight, down_weight):
    normed_in = rms_scale(tokens, norm_gain).astype(jnp.bfloat16)
    projected = jnp.dot(normed_in, in_weight, preferred_element_type=jnp.float32).astype(jnp.bfloat16)
    activated, new_real, new_imag = state_update(projected, state_real, state_imag, decay_rate, frequency, log_step, input_real, input_imag, output_real, output_imag, skip_gain)
    delta = jnp.dot(activated, out_weight, preferred_element_type=jnp.float32)
    hidden_state = (tokens.astype(jnp.float32) + delta).astype(jnp.bfloat16)
    normed = rms_scale(hidden_state, ffn_gain).astype(jnp.bfloat16)
    limit = min(TOKENS, N_EP * CAP)
    piece = FF // SPAN

    def expert_block(carry, expert):
        hits = expert_ids == expert
        row_weight = lax.optimization_barrier(jnp.sum(jnp.where(hits, route_weights, 0.0), axis=1))
        used = jnp.any(hits, axis=1)
        indices = jnp.nonzero(used, size=limit, fill_value=0)[0].astype(jnp.int32)
        valid = jnp.arange(limit, dtype=jnp.int32) < jnp.sum(used.astype(jnp.int32))
        chosen = normed[indices]
        start = (expert * FF).astype(jnp.int32)
        gate_cols = lax.dynamic_slice_in_dim(gate_weight, start, FF, 1)
        up_cols = lax.dynamic_slice_in_dim(up_weight, start, FF, 1)
        down_rows = lax.dynamic_slice_in_dim(down_weight, start, FF, 0)
        gate_pre = jnp.dot(chosen, gate_cols, preferred_element_type=jnp.float32)
        up_pre = jnp.dot(chosen, up_cols, preferred_element_type=jnp.float32)
        expert_hidden = (jax.nn.silu(gate_pre) * up_pre).astype(jnp.bfloat16)

        def one_piece(index):
            first = (index * piece).astype(jnp.int32)
            units = lax.dynamic_slice_in_dim(expert_hidden, first, piece, 1)
            rows = lax.dynamic_slice_in_dim(down_rows, first, piece, 0)
            part = jnp.dot(units, rows, preferred_element_type=jnp.float32).astype(jnp.bfloat16)
            return lax.optimization_barrier(part).astype(jnp.float32)
        pieces = lax.map(one_piece, jnp.arange(SPAN, dtype=jnp.int32))
        expert_out = lax.optimization_barrier(jnp.sum(pieces, axis=0))
        scale = jnp.where(valid, row_weight[indices], 0.0)
        return (carry.at[indices].add(scale[:, None] * expert_out), None)
    routed, _ = lax.scan(expert_block, jnp.zeros(normed.shape, jnp.float32), jnp.arange(EXPERTS, dtype=jnp.int32))
    mixed = (hidden_state.astype(jnp.float32) + routed).astype(jnp.bfloat16)
    return (mixed, new_real, new_imag)
```

```python
import jax
import jax.numpy as jnp
from jax import lax
from jax.experimental import pallas as pl
from jax.experimental.pallas import tpu as pltpu
from jax.sharding import PartitionSpec as P

EPS = 1e-06
F32, BF16, I32 = jnp.float32, jnp.bfloat16, jnp.int32
MESH = pl.DeviceIdType.MESH
NX, NY, NC, NZ = 4, 4, 2, 16
SEQ, WIDTH, QUARTER = 4, 2048, 512
GROUPS, STATE, CHANNELS = 16, 64, 256
HID = 128
CHUNKS = ((0, 1, 15, 2, 14, 3, 13, 4), (12, 5, 11, 6, 10, 7, 9, 8))
PLANE = sorted(
    [(dx, dy) for dx in range(NX) for dy in range(NY)],
    key=lambda d: min(d[0], NX - d[0]) + min(d[1], NY - d[1]),
)


def iota(shape, dim):
    return lax.broadcasted_iota(I32, shape, dim)


def dot(a, b):
    return jnp.dot(a, b, preferred_element_type=F32)


def dot_t(a, b):
    return lax.dot_general(a, b, (((1,), (1,)), ((), ())), preferred_element_type=F32)


def split(x):
    high = x.astype(BF16)
    return high, (x - high.astype(F32)).astype(BF16)


def row_of(block):
    block = block.astype(F32)
    return jnp.concatenate([block[i : i + 1, :] for i in range(block.shape[0])], axis=1)


def rms(floats, gain):
    scale = lax.rsqrt(jnp.mean(floats * floats, axis=-1, keepdims=True) + EPS)
    return (floats * scale * gain).astype(BF16)


def kernel(*refs):
    hbm, outs, scratch = refs[:20], refs[20:23], refs[23:]
    (tok_h, gain_h, inw_h, decay_h, freq_h, step_h, inr_h, ini_h, outr_h, outi_h) = hbm[:10]
    (skip_h, str_h, sti_h, outw_h, fgain_h, ids_h, rw_h, gw_h, uw_h, dw_h) = hbm[10:]
    mixed_o, newr_o, newi_o = outs
    (tok, gain, inw, decay, freq, steps, inr, ini, outr, outi) = scratch[:10]
    (skip, st_r, st_i, outw, fgain, ids, rw, gw, uw, dw) = scratch[10:20]
    (newr, newi, mixed, delta, norm32, hid32, pick32, pick, zin) = scratch[20:29]
    (gat, hid, send, recv, sum32, back, zout, load, store) = scratch[29:38]
    (ds_sem, dr_sem, zs_sem, zr_sem, gs_sem, gr_sem, fs_sem, fr_sem) = scratch[38:46]
    (hs_sem, hr_sem, rs_sem, rr_sem, bs_sem, br_sem) = scratch[46:52]

    ep, y = lax.axis_index("ep"), lax.axis_index("tp")
    z, x, c = ep // 8, (ep // 2) % NX, ep % 2

    def at(zz, xx, cc, yy):
        return (zz * 8 + xx * 2 + cc, yy)

    def turn(a, d, n):
        return lax.rem(a + d, n)

    barrier = pltpu.get_barrier_semaphore()
    partners = [at(turn(z, d, NZ), x, c, y) for d in range(1, NZ)]
    partners += [at(z, turn(x, dx, NX), c, turn(y, dy, NY)) for dx, dy in PLANE if dx or dy]
    partners += [at(z, turn(x, dx, NX), 1 - c, y) for dx in range(NX)]
    for device in partners:
        pl.semaphore_signal(barrier, inc=1, device_id=device, device_id_type=MESH)

    wide = pl.multiple_of((ep // 32) * 128, 128)
    sources = list(hbm)
    sources[15] = ids_h.at[:, pl.ds(wide, 128)]
    loads = [
        pltpu.make_async_copy(source, target, load.at[i])
        for i, (source, target) in enumerate(zip(sources, scratch[:20]))
    ]
    for i in (0, 1, 2, 3, 4, 5, 6, 7, 11, 12, 8, 9, 10, 13, 14, 15, 16, 17, 18, 19):
        loads[i].start()

    loads[0].wait()
    loads[1].wait()
    tokens = tok[...].astype(F32)
    normed_in = rms(tokens, row_of(gain[...]))
    loads[2].wait()
    u = dot(normed_in, inw[...]).astype(BF16).astype(F32)

    rows = SEQ * GROUPS
    own_group = iota((rows, CHANNELS), 0) % GROUPS == iota((rows, CHANNELS), 1) // 16
    spread = jnp.broadcast_to(u[:, None, :], (SEQ, GROUPS, CHANNELS)).reshape(rows, CHANNELS)
    spread = jnp.where(own_group, spread, 0.0).astype(BF16)
    for i in (3, 4, 5, 6, 7):
        loads[i].wait()
    group_row = iota((GROUPS, STATE), 0)
    log_step = jnp.zeros((GROUPS, STATE), F32)
    for g in range(GROUPS):
        log_step = jnp.where(group_row == g, steps[g], log_step)
    step_size = jnp.exp(log_step)
    lam_real, frequency = -decay[...], freq[...]
    magnitude = jnp.exp(lam_real * step_size)
    turned = frequency * step_size
    bar_real = magnitude * jnp.cos(turned)
    bar_imag = magnitude * jnp.sin(turned)
    denom = lam_real * lam_real + frequency * frequency
    minus_one = bar_real - 1.0
    factor_real = (minus_one * lam_real + bar_imag * frequency) / denom
    factor_imag = (bar_imag * lam_real - minus_one * frequency) / denom

    def per_row(v):
        return jnp.broadcast_to(v[None], (SEQ, GROUPS, STATE)).reshape(rows, STATE)

    def drive(ref):
        high, low = split(ref[...].reshape(CHANNELS, STATE))
        return dot(spread, high) + dot(spread, low)

    drive_r, drive_i = drive(inr), drive(ini)
    bar_real, bar_imag = per_row(bar_real), per_row(bar_imag)
    factor_real, factor_imag = per_row(factor_real), per_row(factor_imag)
    loads[11].wait()
    loads[12].wait()
    state_r, state_i = st_r[...].reshape(rows, STATE), st_i[...].reshape(rows, STATE)
    new_r = (bar_real * state_r - bar_imag * state_i) + (factor_real * drive_r - factor_imag * drive_i)
    new_i = (bar_real * state_i + bar_imag * state_r) + (factor_real * drive_i + factor_imag * drive_r)
    newr[...] = new_r.reshape(SEQ, GROUPS, STATE)
    newi[...] = new_i.reshape(SEQ, GROUPS, STATE)

    for i in (8, 9, 10):
        loads[i].wait()

    def read(values, ref):
        high, low = split(values)
        ref_high, ref_low = split(ref[...].reshape(CHANNELS, STATE))
        return dot_t(high, ref_high) + dot_t(high, ref_low) + dot_t(low, ref_high)

    readout = jnp.where(own_group, read(new_r, outr) - read(new_i, outi), 0.0)
    readout = readout.reshape(SEQ, GROUPS, CHANNELS).sum(axis=1)
    readout = readout + row_of(skip[...]) * u
    activated = jax.nn.gelu(readout).astype(BF16)
    loads[13].wait()
    delta[y] = dot(activated, outw[...]).astype(BF16)

    pl.semaphore_wait(barrier, len(partners))
    delta_copies = [
        pltpu.make_async_remote_copy(
            delta.at[y], delta.at[y], ds_sem.at[d], dr_sem.at[d],
            device_id=at(z, x, c, turn(y, d, NY)), device_id_type=MESH,
        )
        for d in range(1, NY)
    ]
    for copy in delta_copies:
        copy.start()
    stores = [
        pltpu.make_async_copy(newr, newr_o, store.at[0]),
        pltpu.make_async_copy(newi, newi_o, store.at[1]),
    ]
    for copy in stores:
        copy.start()

    for i in (14, 15, 16):
        loads[i].wait()
    first = (ep % 32) * SEQ
    names = [[ids[k, first + s] for k in range(2)] for s in range(SEQ)]
    weights = [[rw[k, s] for k in range(2)] for s in range(SEQ)]

    def table(expert, slot, shape):
        taken = jnp.zeros(shape, I32)
        picks, scales = [], []
        for s in range(SEQ):
            routes = [expert == names[s][k] for k in range(2)]
            named = routes[0] | routes[1]
            here = named & (taken == slot)
            picks.append(jnp.where(here, 1.0, 0.0))
            scale = jnp.where(routes[0], weights[s][0], 0.0) + jnp.where(routes[1], weights[s][1], 0.0)
            scales.append(jnp.where(here, scale, 0.0))
            taken = taken + jnp.where(named, 1, 0)
        return picks, scales

    pick_row = iota((16, QUARTER), 0)
    picks, _ = table(pick_row // 2, pick_row % 2, (16, QUARTER))
    ffn_gain = row_of(fgain[...])

    for copy in delta_copies:
        copy.wait_recv()
    total = tokens
    for i in range(NY):
        total = total + delta[i].astype(F32)
    hidden_state = total.astype(BF16).astype(F32)
    hid32[...] = hidden_state
    norm32[...] = rms(hidden_state, ffn_gain).astype(F32)
    lanes = pl.ds(pl.multiple_of(y * QUARTER, QUARTER), QUARTER)
    own = norm32[:, lanes]
    chosen = picks[0] * own[0:1, :]
    for s in range(1, SEQ):
        chosen = chosen + picks[s] * own[s : s + 1, :]
    pick32[...] = chosen
    for e in range(8):
        pick[e] = pick32[2 * e : 2 * e + 2, :].astype(BF16)

    z_copies = {}
    for d in (8, 7, 9, 6, 10, 5, 11, 4, 12, 3, 13, 2, 14, 1, 15):
        to = turn(z, d, NZ)
        z_copies[d] = pltpu.make_async_remote_copy(
            pick.at[to // 2], zin.at[d], zs_sem.at[d], zr_sem.at[d],
            device_id=at(to, x, c, y), device_id_type=MESH,
        )
        z_copies[d].start()

    gathers, forwards = [], []
    for k, chunk in enumerate(CHUNKS):
        for i, d in enumerate(chunk):
            if d:
                z_copies[d].wait_recv()
                piece = zin[d]
            else:
                piece = pick[z // 2]
            sum32[2 * i : 2 * i + 2, :] = piece.astype(F32)
        gat[k, y, c, x] = sum32[...].astype(BF16)
        copies = {}
        for dx, dy in reversed(PLANE):
            if dx or dy:
                copies[dx, dy] = pltpu.make_async_remote_copy(
                    gat.at[k, y, c, x], gat.at[k, y, c, x], gs_sem.at[k, dx, dy], gr_sem.at[k, dx, dy],
                    device_id=at(z, turn(x, dx, NX), c, turn(y, dy, NY)), device_id_type=MESH,
                )
                copies[dx, dy].start()
        gathers.append(copies)

    h_copies, r_copies = [], []

    def spread_chunk(k):
        copies = []
        for dx, dy in PLANE:
            if dx or dy:
                gathers[k][dx, dy].wait_recv()
            slot = gat.at[k, turn(y, NY - dy, NY), c, turn(x, NX - dx, NX)]
            copies.append(
                pltpu.make_async_remote_copy(
                    slot, slot, fs_sem.at[k, dx, dy], fr_sem.at[k, dx, dy],
                    device_id=at(z, x, 1 - c, y), device_id_type=MESH,
                )
            )
            copies[-1].start()
        forwards.append(copies)

    def up_chunk(k):
        for copy in forwards[k]:
            copy.wait_recv()
        gate_pre = jnp.zeros((128, HID), F32)
        up_pre = jnp.zeros((128, HID), F32)
        for q in range(NY):
            block = gat[k, q].reshape(128, QUARTER)
            gate_pre = gate_pre + dot(block, gw[q * QUARTER : (q + 1) * QUARTER, :])
            up_pre = up_pre + dot(block, uw[q * QUARTER : (q + 1) * QUARTER, :])
        units = pl.ds(pl.multiple_of(y * HID, HID), HID)
        hid[k, :, units] = (jax.nn.silu(gate_pre) * up_pre).astype(BF16)
        copies = []
        for d in (2, 1, 3):
            copies.append(
                pltpu.make_async_remote_copy(
                    hid.at[k, :, units], hid.at[k, :, units], hs_sem.at[k, d], hr_sem.at[k, d],
                    device_id=at(z, x, c, turn(y, d, NY)), device_id_type=MESH,
                )
            )
            copies[-1].start()
        h_copies.append(copies)

    def down_chunk(k):
        for copy in h_copies[k]:
            copy.wait_recv()
        send[k] = dot(hid[k], dw[...]).astype(BF16).reshape(NC, NX, 16, QUARTER)
        copies = []
        for dx in (2, 1, 3, 0):
            for dc in range(NC):
                if dx or dc:
                    to_x, to_c = turn(x, dx, NX), c if dc == 0 else 1 - c
                    copies.append(
                        pltpu.make_async_remote_copy(
                            send.at[k, to_c, to_x], recv.at[k, dc, dx], rs_sem.at[k, dc, dx], rr_sem.at[k, dc, dx],
                            device_id=at(z, to_x, to_c, y), device_id_type=MESH,
                        )
                    )
                    copies[-1].start()
        r_copies.append(copies)

    b_copies = {}

    def home_chunk(k):
        for copy in r_copies[k]:
            copy.wait_recv()
        total = send[k, c, x].astype(F32)
        for dc in range(NC):
            for dx in range(NX):
                if dx or dc:
                    total = total + recv[k, dc, dx].astype(F32)
        sum32[...] = total
        for i, d in enumerate(CHUNKS[k]):
            back[k, i] = sum32[2 * i : 2 * i + 2, :].astype(BF16)
        for i, d in reversed(list(enumerate(CHUNKS[k]))):
            if d:
                b_copies[d] = pltpu.make_async_remote_copy(
                    back.at[k, i], zout.at[d], bs_sem.at[d], br_sem.at[d],
                    device_id=at(turn(z, NZ - d, NZ), x, c, y), device_id_type=MESH,
                )
                b_copies[d].start()

    spread_chunk(0)
    loads[17].wait()
    loads[18].wait()
    up_chunk(0)
    spread_chunk(1)
    loads[19].wait()
    down_chunk(0)
    up_chunk(1)
    down_chunk(1)
    home_chunk(0)
    home_chunk(1)

    back_row = iota((2 * NZ, QUARTER), 0)
    _, scales = table(((z + back_row // 2) % NZ) // 2, back_row % 2, (2 * NZ, QUARTER))
    out32, mix32 = scratch[52], scratch[53]
    for d in (0, 1, 15, 2, 14, 3, 13, 4, 12, 5, 11, 6, 10, 7, 9, 8):
        if d:
            b_copies[d].wait_recv()
            piece = zout[d]
        else:
            piece = back[0, 0]
        out32[2 * d : 2 * d + 2, :] = piece.astype(F32)
    pieces = out32[...]
    for s in range(SEQ):
        mix32[s : s + 1, :] = jnp.sum(scales[s] * pieces, axis=0, keepdims=True)
    mixed[...] = (hid32[:, lanes] + mix32[...]).astype(BF16)
    stores.append(pltpu.make_async_copy(mixed, mixed_o, store.at[2]))
    stores[2].start()

    for copy in delta_copies + list(z_copies.values()) + list(b_copies.values()):
        copy.wait_send()
    for copies in gathers:
        for copy in copies.values():
            copy.wait_send()
    for copies in forwards + h_copies + r_copies:
        for copy in copies:
            copy.wait_send()
    for copy in stores:
        copy.wait()


def shards(*args):
    args = list(args)
    for i in (1, 14):
        args[i] = args[i].reshape(16, 128)
    args[10] = args[10].reshape(2, 128)
    for i in (6, 7):
        args[i] = args[i].transpose(0, 2, 1)
    args[15], args[16] = args[15].T, args[16].T
    held = []
    for i, arg in enumerate(args):
        if i in (5, 16):
            held.append(pltpu.SMEM(arg.shape, arg.dtype))
        elif i == 15:
            held.append(pltpu.SMEM((2, 128), arg.dtype))
        else:
            held.append(pltpu.VMEM(arg.shape, arg.dtype))
    dma = pltpu.SemaphoreType.DMA
    out_shapes = (
        jax.ShapeDtypeStruct((SEQ, QUARTER), BF16),
        jax.ShapeDtypeStruct((SEQ, GROUPS, STATE), F32),
        jax.ShapeDtypeStruct((SEQ, GROUPS, STATE), F32),
    )
    scratch = held + [
        pltpu.VMEM((SEQ, GROUPS, STATE), F32),
        pltpu.VMEM((SEQ, GROUPS, STATE), F32),
        pltpu.VMEM((SEQ, QUARTER), BF16),
        pltpu.VMEM((NY, SEQ, WIDTH), BF16),
        pltpu.VMEM((SEQ, WIDTH), F32),
        pltpu.VMEM((SEQ, WIDTH), F32),
        pltpu.VMEM((16, QUARTER), F32),
        pltpu.VMEM((8, 2, QUARTER), BF16),
        pltpu.VMEM((NZ, 2, QUARTER), BF16),
        pltpu.VMEM((2, NY, NC, NX, 16, QUARTER), BF16),
        pltpu.VMEM((2, 128, NY * HID), BF16),
        pltpu.VMEM((2, NC, NX, 16, QUARTER), BF16),
        pltpu.VMEM((2, NC, NX, 16, QUARTER), BF16),
        pltpu.VMEM((16, QUARTER), F32),
        pltpu.VMEM((2, 8, 2, QUARTER), BF16),
        pltpu.VMEM((NZ, 2, QUARTER), BF16),
        dma((20,)), dma((3,)),
        dma((NY,)), dma((NY,)), dma((NZ,)), dma((NZ,)),
        dma((2, NX, NY)), dma((2, NX, NY)), dma((2, NX, NY)), dma((2, NX, NY)),
        dma((2, NY)), dma((2, NY)), dma((2, NC, NX)), dma((2, NC, NX)), dma((NZ,)), dma((NZ,)),
        pltpu.VMEM((2 * NZ, QUARTER), F32),
        pltpu.VMEM((SEQ, QUARTER), F32),
    ]
    anywhere = pl.BlockSpec(memory_space=pl.ANY)
    return pl.pallas_call(
        kernel,
        out_shape=out_shapes,
        in_specs=[anywhere] * 20,
        out_specs=(anywhere,) * 3,
        scratch_shapes=scratch,
        compiler_params=pltpu.CompilerParams(collective_id=0, has_side_effects=True),
    )(*args)


def solution(mesh):
    in_specs = (
        P("ep", None), P(), P(None, "tp"), P("tp", None), P("tp", None), P("tp"),
        P("tp", None, None), P("tp", None, None), P("tp", None, None), P("tp", None, None), P("tp"),
        P("ep", "tp", None), P("ep", "tp", None), P("tp", None), P(), P(), P("ep", None),
        P(None, ("ep", "tp")), P(None, ("ep", "tp")), P("ep", "tp"),
    )
    out_specs = (P("ep", "tp"), P("ep", "tp", None), P("ep", "tp", None))
    return jax.shard_map(shards, mesh=mesh, in_specs=in_specs, out_specs=out_specs, check_vma=False)
```

```python
import jax
import jax.numpy as jnp
from jax import lax
from jax.experimental import pallas as pl
from jax.experimental.pallas import tpu as pltpu
from jax.sharding import PartitionSpec as P

EPS = 1e-06
F32, BF16, I32 = jnp.float32, jnp.bfloat16, jnp.int32
MESH = pl.DeviceIdType.MESH
NX, NY, NC, NZ = 4, 4, 2, 16
SEQ, WIDTH, QUARTER = 4, 2048, 512
GROUPS, STATE, CHANNELS = 16, 64, 256
HID = 128
HALF = NZ // 2
PLANE = sorted(
    [(dx, dy) for dx in range(NX) for dy in range(NY)],
    key=lambda d: min(d[0], NX - d[0]) + min(d[1], NY - d[1]),
)


def iota(shape, dim):
    return lax.broadcasted_iota(I32, shape, dim)


def dot(a, b):
    return jnp.dot(a, b, preferred_element_type=F32)


def dot_t(a, b):
    return lax.dot_general(a, b, (((1,), (1,)), ((), ())), preferred_element_type=F32)


def split(x):
    high = x.astype(BF16)
    return high, (x - high.astype(F32)).astype(BF16)


def row_of(block):
    block = block.astype(F32)
    return jnp.concatenate([block[i : i + 1, :] for i in range(block.shape[0])], axis=1)


def rms(floats, gain):
    scale = lax.rsqrt(jnp.mean(floats * floats, axis=-1, keepdims=True) + EPS)
    return (floats * scale * gain).astype(BF16)


def kernel(*refs):
    hbm, outs, scratch = refs[:20], refs[20:23], refs[23:]
    (tok_h, gain_h, inw_h, decay_h, freq_h, step_h, inr_h, ini_h, outr_h, outi_h) = hbm[:10]
    (skip_h, str_h, sti_h, outw_h, fgain_h, ids_h, rw_h, gw_h, uw_h, dw_h) = hbm[10:]
    mixed_o, newr_o, newi_o = outs
    (tok, gain, inw, decay, freq, steps, inr, ini, outr, outi) = scratch[:10]
    (skip, st_r, st_i, outw, fgain, ids, rw, gw, uw, dw) = scratch[10:20]
    (newr, newi, mixed, delta, norm32, hid32, pick32, pick, zin) = scratch[20:29]
    (gat, hid, send, recv, sum32, back, zout, load, store) = scratch[29:38]
    (ds_sem, dr_sem, zs_sem, zr_sem, gs_sem, gr_sem, fs_sem, fr_sem) = scratch[38:46]
    (hs_sem, hr_sem, rs_sem, rr_sem, bs_sem, br_sem) = scratch[46:52]
    out32, mix32, near_sem, far_sem = scratch[52:56]

    ep, y = lax.axis_index("ep"), lax.axis_index("tp")
    z, x, c = ep // 8, (ep // 2) % NX, ep % 2

    def at(zz, xx, cc, yy):
        return (zz * 8 + xx * 2 + cc, yy)

    def turn(a, d, n):
        return lax.rem(a + d, n)

    barrier = pltpu.get_barrier_semaphore()

    def enter(device):
        pl.semaphore_signal(barrier, inc=1, device_id=device, device_id_type=MESH)

    for d in range(1, NY):
        enter(at(z, x, 0, turn(y, d, NY)))
    for d in range(1, NZ):
        enter(at(turn(z, d, NZ), x, 1, y))
    for dx, dy in PLANE:
        if dx or dy:
            enter(at(z, turn(x, dx, NX), 1, turn(y, dy, NY)))
    enter(at(z, x, 1 - c, y))
    near_count = 2 * (NY - 1) + 1
    far_count = 2 * (NZ - 1) + 2 * (NX * NY - 1) + 1

    wide = pl.multiple_of((ep // 32) * 128, 128)
    sources = list(hbm)
    sources[15] = ids_h.at[:, pl.ds(wide, 128)]
    loads = [
        pltpu.make_async_copy(source, target, load.at[i])
        for i, (source, target) in enumerate(zip(sources, scratch[:20]))
    ]
    for i in (0, 1, 2, 3, 4, 5, 6, 7, 11, 12, 8, 9, 10, 13, 14, 15, 16, 17, 18, 19):
        loads[i].start()

    loads[0].wait()
    loads[1].wait()
    tokens = tok[...].astype(F32)
    normed_in = rms(tokens, row_of(gain[...]))
    loads[2].wait()
    u = dot(normed_in, inw[...]).astype(BF16).astype(F32)

    rows = SEQ * GROUPS
    own_group = iota((rows, CHANNELS), 0) % GROUPS == iota((rows, CHANNELS), 1) // 16
    spread = jnp.broadcast_to(u[:, None, :], (SEQ, GROUPS, CHANNELS)).reshape(rows, CHANNELS)
    spread = jnp.where(own_group, spread, 0.0).astype(BF16)
    for i in (3, 4, 5, 6, 7):
        loads[i].wait()
    group_row = iota((GROUPS, STATE), 0)
    log_step = jnp.zeros((GROUPS, STATE), F32)
    for g in range(GROUPS):
        log_step = jnp.where(group_row == g, steps[g], log_step)
    step_size = jnp.exp(log_step)
    lam_real, frequency = -decay[...], freq[...]
    magnitude = jnp.exp(lam_real * step_size)
    turned = frequency * step_size
    bar_real = magnitude * jnp.cos(turned)
    bar_imag = magnitude * jnp.sin(turned)
    denom = lam_real * lam_real + frequency * frequency
    minus_one = bar_real - 1.0
    factor_real = (minus_one * lam_real + bar_imag * frequency) / denom
    factor_imag = (bar_imag * lam_real - minus_one * frequency) / denom

    def per_row(v):
        return jnp.broadcast_to(v[None], (SEQ, GROUPS, STATE)).reshape(rows, STATE)

    def drive(ref):
        high, low = split(ref[...].reshape(CHANNELS, STATE))
        return dot(spread, high) + dot(spread, low)

    drive_r, drive_i = drive(inr), drive(ini)
    bar_real, bar_imag = per_row(bar_real), per_row(bar_imag)
    factor_real, factor_imag = per_row(factor_real), per_row(factor_imag)
    loads[11].wait()
    loads[12].wait()
    state_r, state_i = st_r[...].reshape(rows, STATE), st_i[...].reshape(rows, STATE)
    new_r = (bar_real * state_r - bar_imag * state_i) + (factor_real * drive_r - factor_imag * drive_i)
    new_i = (bar_real * state_i + bar_imag * state_r) + (factor_real * drive_i + factor_imag * drive_r)
    newr[...] = new_r.reshape(SEQ, GROUPS, STATE)
    newi[...] = new_i.reshape(SEQ, GROUPS, STATE)

    for i in (8, 9, 10):
        loads[i].wait()

    def read(values, ref):
        high, low = split(values)
        ref_high, ref_low = split(ref[...].reshape(CHANNELS, STATE))
        return dot_t(high, ref_high) + dot_t(high, ref_low) + dot_t(low, ref_high)

    readout = jnp.where(own_group, read(new_r, outr) - read(new_i, outi), 0.0)
    readout = readout.reshape(SEQ, GROUPS, CHANNELS).sum(axis=1)
    readout = readout + row_of(skip[...]) * u
    activated = jax.nn.gelu(readout).astype(BF16)
    loads[13].wait()
    delta[y] = dot(activated, outw[...]).astype(BF16)

    @pl.when(c == 0)
    def _():
        pl.semaphore_wait(barrier, near_count)
        pl.semaphore_signal(near_sem, inc=1, device_id=at(z, x, 1, y), device_id_type=MESH)

    @pl.when(c == 1)
    def _():
        pl.semaphore_wait(near_sem, 1)

    delta_copies = [
        pltpu.make_async_remote_copy(
            delta.at[y], delta.at[y], ds_sem.at[d], dr_sem.at[d],
            device_id=at(z, x, c, turn(y, d, NY)), device_id_type=MESH,
        )
        for d in range(1, NY)
    ]
    for copy in delta_copies:
        copy.start()
    stores = [
        pltpu.make_async_copy(newr, newr_o, store.at[0]),
        pltpu.make_async_copy(newi, newi_o, store.at[1]),
    ]
    for copy in stores:
        copy.start()

    for i in (14, 15, 16):
        loads[i].wait()
    first = (ep % 32) * SEQ
    names = [[ids[k, first + s] for k in range(2)] for s in range(SEQ)]
    weights = [[rw[k, s] for k in range(2)] for s in range(SEQ)]

    def table(expert, slot, shape):
        taken = jnp.zeros(shape, I32)
        picks, scales = [], []
        for s in range(SEQ):
            routes = [expert == names[s][k] for k in range(2)]
            named = routes[0] | routes[1]
            here = named & (taken == slot)
            picks.append(jnp.where(here, 1.0, 0.0))
            scale = jnp.where(routes[0], weights[s][0], 0.0) + jnp.where(routes[1], weights[s][1], 0.0)
            scales.append(jnp.where(here, scale, 0.0))
            taken = taken + jnp.where(named, 1, 0)
        return picks, scales

    pick_row = iota((16, QUARTER), 0)
    picks, _ = table(pick_row // 2, pick_row % 2, (16, QUARTER))
    ffn_gain = row_of(fgain[...])

    for copy in delta_copies:
        copy.wait_recv()
    total = tokens
    for i in range(NY):
        total = total + delta[i].astype(F32)
    hidden_state = total.astype(BF16).astype(F32)
    hid32[...] = hidden_state
    norm32[...] = rms(hidden_state, ffn_gain).astype(F32)
    lanes = pl.ds(pl.multiple_of(y * QUARTER, QUARTER), QUARTER)
    own = norm32[:, lanes]
    chosen = picks[0] * own[0:1, :]
    for s in range(1, SEQ):
        chosen = chosen + picks[s] * own[s : s + 1, :]
    pick32[...] = chosen
    for e in range(8):
        pick[e] = pick32[2 * e : 2 * e + 2, :].astype(BF16)

    @pl.when(c == 1)
    def _():
        pl.semaphore_wait(barrier, far_count)
        pl.semaphore_signal(far_sem, inc=1, device_id=at(z, x, 0, y), device_id_type=MESH)

    @pl.when(c == 0)
    def _():
        pl.semaphore_wait(far_sem, 1)

    z_copies = []
    for d in (8, 7, 9, 6, 10, 5, 11, 4, 12, 3, 13, 2, 14, 1, 15):
        to = turn(z, d, NZ)
        z_copies.append(
            pltpu.make_async_remote_copy(
                pick.at[to // 2], zin.at[z], zs_sem.at[d], zr_sem.at[z],
                device_id=at(to, x, c, y), device_id_type=MESH,
            )
        )
        z_copies[-1].start()
    pltpu.make_async_copy(pick.at[z // 2], zin.at[z], zr_sem.at[z]).start()

    def landed(ref, sem):
        pltpu.make_async_remote_copy(
            ref, ref, zs_sem.at[0], sem, device_id=at(z, x, 1 - c, y), device_id_type=MESH
        ).wait_recv()

    gathers, forwards = [], {}

    def gather_chunk(k):
        for i in range(HALF):
            home = k * HALF + i
            landed(zin.at[home], zr_sem.at[home])
            sum32[2 * i : 2 * i + 2, :] = zin[home].astype(F32)
        gat[k, y, c, x] = sum32[...].astype(BF16)
        copies = {}
        for dx, dy in reversed(PLANE):
            if dx or dy:
                copies[dx, dy] = pltpu.make_async_remote_copy(
                    gat.at[k, y, c, x], gat.at[k, y, c, x], gs_sem.at[k, dx, dy], gr_sem.at[k, dx, dy],
                    device_id=at(z, turn(x, dx, NX), c, turn(y, dy, NY)), device_id_type=MESH,
                )
                copies[dx, dy].start()
        gathers.append(copies)

    h_copies, r_copies = {}, {}

    def spread_chunk(k):
        copies = []
        for dx, dy in PLANE:
            if dx or dy:
                gathers[k][dx, dy].wait_recv()
            slot = gat.at[k, turn(y, NY - dy, NY), c, turn(x, NX - dx, NX)]
            copies.append(
                pltpu.make_async_remote_copy(
                    slot, slot, fs_sem.at[k, dx, dy], fr_sem.at[k, dx, dy],
                    device_id=at(z, x, 1 - c, y), device_id_type=MESH,
                )
            )
            copies[-1].start()
        forwards[k] = copies

    def up_chunk(k):
        for copy in forwards[k]:
            copy.wait_recv()
        gate_pre = jnp.zeros((128, HID), F32)
        up_pre = jnp.zeros((128, HID), F32)
        for q in range(NY):
            block = gat[k, q].reshape(128, QUARTER)
            gate_pre = gate_pre + dot(block, gw[q * QUARTER : (q + 1) * QUARTER, :])
            up_pre = up_pre + dot(block, uw[q * QUARTER : (q + 1) * QUARTER, :])
        units = pl.ds(pl.multiple_of(y * HID, HID), HID)
        hid[k, :, units] = (jax.nn.silu(gate_pre) * up_pre).astype(BF16)
        copies = []
        for d in (2, 1, 3):
            copies.append(
                pltpu.make_async_remote_copy(
                    hid.at[k, :, units], hid.at[k, :, units], hs_sem.at[k, d], hr_sem.at[k, d],
                    device_id=at(z, x, c, turn(y, d, NY)), device_id_type=MESH,
                )
            )
            copies[-1].start()
        h_copies[k] = copies

    def down_chunk(k):
        for copy in h_copies[k]:
            copy.wait_recv()
        send[k] = dot(hid[k], dw[...]).astype(BF16).reshape(NC, NX, 16, QUARTER)
        copies = []
        for dx in (2, 1, 3, 0):
            for dc in range(NC):
                if dx or dc:
                    to_x, to_c = turn(x, dx, NX), c if dc == 0 else 1 - c
                    copies.append(
                        pltpu.make_async_remote_copy(
                            send.at[k, to_c, to_x], recv.at[k, dc, dx], rs_sem.at[k, dc, dx], rr_sem.at[k, dc, dx],
                            device_id=at(z, to_x, to_c, y), device_id_type=MESH,
                        )
                    )
                    copies[-1].start()
        r_copies[k] = copies

    b_copies = {}

    def home_chunk(k):
        for copy in r_copies[k]:
            copy.wait_recv()
        total = send[k, c, x].astype(F32)
        for dc in range(NC):
            for dx in range(NX):
                if dx or dc:
                    total = total + recv[k, dc, dx].astype(F32)
        sum32[...] = total
        for i in range(HALF):
            back[k, i] = sum32[2 * i : 2 * i + 2, :].astype(BF16)
        for i in range(HALF):
            home = k * HALF + i
            b_copies[home] = pltpu.make_async_remote_copy(
                back.at[k, i], zout.at[z], bs_sem.at[home], br_sem.at[z],
                device_id=at(home, x, c, y), device_id_type=MESH,
            )

            @pl.when(z != home)
            def _():
                b_copies[home].start()

            @pl.when(z == home)
            def _():
                pltpu.make_async_copy(back.at[k, i], zout.at[z], br_sem.at[z]).start()

    gather_chunk(0)
    gather_chunk(1)
    spread_chunk(0)
    loads[17].wait()
    loads[18].wait()
    up_chunk(0)
    spread_chunk(1)
    loads[19].wait()
    down_chunk(0)
    up_chunk(1)
    home_chunk(0)
    down_chunk(1)
    home_chunk(1)

    back_row = iota((2 * NZ, QUARTER), 0)
    _, scales = table(back_row // 4, back_row % 2, (2 * NZ, QUARTER))
    for p in range(NZ):
        landed(zout.at[p], br_sem.at[p])
        out32[2 * p : 2 * p + 2, :] = zout[p].astype(F32)
    pieces = out32[...]
    for s in range(SEQ):
        mix32[s : s + 1, :] = jnp.sum(scales[s] * pieces, axis=0, keepdims=True)
    mixed[...] = (hid32[:, lanes] + mix32[...]).astype(BF16)
    stores.append(pltpu.make_async_copy(mixed, mixed_o, store.at[2]))
    stores[2].start()

    for copy in delta_copies + z_copies:
        copy.wait_send()
    for home, copy in b_copies.items():

        @pl.when(z != home)
        def _():
            copy.wait_send()

    for copies in gathers:
        for copy in copies.values():
            copy.wait_send()
    for copies in (forwards, h_copies, r_copies):
        for copy in copies[0] + copies[1]:
            copy.wait_send()
    for copy in stores:
        copy.wait()


def shards(*args):
    args = list(args)
    for i in (1, 14):
        args[i] = args[i].reshape(16, 128)
    args[10] = args[10].reshape(2, 128)
    for i in (6, 7):
        args[i] = args[i].transpose(0, 2, 1)
    args[15], args[16] = args[15].T, args[16].T
    held = []
    for i, arg in enumerate(args):
        if i in (5, 16):
            held.append(pltpu.SMEM(arg.shape, arg.dtype))
        elif i == 15:
            held.append(pltpu.SMEM((2, 128), arg.dtype))
        else:
            held.append(pltpu.VMEM(arg.shape, arg.dtype))
    dma = pltpu.SemaphoreType.DMA
    out_shapes = (
        jax.ShapeDtypeStruct((SEQ, QUARTER), BF16),
        jax.ShapeDtypeStruct((SEQ, GROUPS, STATE), F32),
        jax.ShapeDtypeStruct((SEQ, GROUPS, STATE), F32),
    )
    scratch = held + [
        pltpu.VMEM((SEQ, GROUPS, STATE), F32),
        pltpu.VMEM((SEQ, GROUPS, STATE), F32),
        pltpu.VMEM((SEQ, QUARTER), BF16),
        pltpu.VMEM((NY, SEQ, WIDTH), BF16),
        pltpu.VMEM((SEQ, WIDTH), F32),
        pltpu.VMEM((SEQ, WIDTH), F32),
        pltpu.VMEM((16, QUARTER), F32),
        pltpu.VMEM((8, 2, QUARTER), BF16),
        pltpu.VMEM((NZ, 2, QUARTER), BF16),
        pltpu.VMEM((2, NY, NC, NX, 16, QUARTER), BF16),
        pltpu.VMEM((2, 128, NY * HID), BF16),
        pltpu.VMEM((2, NC, NX, 16, QUARTER), BF16),
        pltpu.VMEM((2, NC, NX, 16, QUARTER), BF16),
        pltpu.VMEM((16, QUARTER), F32),
        pltpu.VMEM((2, 8, 2, QUARTER), BF16),
        pltpu.VMEM((NZ, 2, QUARTER), BF16),
        dma((20,)), dma((3,)),
        dma((NY,)), dma((NY,)), dma((NZ,)), dma((NZ,)),
        dma((2, NX, NY)), dma((2, NX, NY)), dma((2, NX, NY)), dma((2, NX, NY)),
        dma((2, NY)), dma((2, NY)), dma((2, NC, NX)), dma((2, NC, NX)), dma((NZ,)), dma((NZ,)),
        pltpu.VMEM((2 * NZ, QUARTER), F32),
        pltpu.VMEM((SEQ, QUARTER), F32),
        pltpu.SemaphoreType.REGULAR,
        pltpu.SemaphoreType.REGULAR,
    ]
    anywhere = pl.BlockSpec(memory_space=pl.ANY)
    return pl.pallas_call(
        kernel,
        out_shape=out_shapes,
        in_specs=[anywhere] * 20,
        out_specs=(anywhere,) * 3,
        scratch_shapes=scratch,
        compiler_params=pltpu.CompilerParams(collective_id=0, has_side_effects=True),
    )(*args)


def solution(mesh):
    in_specs = (
        P("ep", None), P(), P(None, "tp"), P("tp", None), P("tp", None), P("tp"),
        P("tp", None, None), P("tp", None, None), P("tp", None, None), P("tp", None, None), P("tp"),
        P("ep", "tp", None), P("ep", "tp", None), P("tp", None), P(), P(), P("ep", None),
        P(None, ("ep", "tp")), P(None, ("ep", "tp")), P("ep", "tp"),
    )
    out_specs = (P("ep", "tp"), P("ep", "tp", None), P("ep", "tp", None))
    return jax.shard_map(shards, mesh=mesh, in_specs=in_specs, out_specs=out_specs, check_vma=False)
```

```python
import jax
import jax.numpy as jnp
from jax import lax
from jax.experimental import pallas as pl
from jax.experimental.pallas import tpu as pltpu
from jax.sharding import PartitionSpec as P

EPS = 1e-06
F32, BF16, I32 = jnp.float32, jnp.bfloat16, jnp.int32
MESH = pl.DeviceIdType.MESH
NX, NY, NC, NZ = 4, 4, 2, 16
SEQ, WIDTH, QUARTER = 4, 2048, 512
GROUPS, STATE, CHANNELS = 16, 64, 256
HID = 128
HALF = NZ // 2
VMEM_LIMIT = 67043328 - 72 * 1024
LOAD_GROUP = (0, 0, 1, 2, 2, 2, 2, 2, 4, 4, 4, 3, 3, 5, 6, 6, 6, 7, 7, 8)
PLANE = sorted(
    [(dx, dy) for dx in range(NX) for dy in range(NY)],
    key=lambda d: min(d[0], NX - d[0]) + min(d[1], NY - d[1]),
)


def iota(shape, dim):
    return lax.broadcasted_iota(I32, shape, dim)


def dot(a, b):
    return jnp.dot(a, b, preferred_element_type=F32)


def dot_t(a, b):
    return lax.dot_general(a, b, (((1,), (1,)), ((), ())), preferred_element_type=F32)


def split(x):
    high = x.astype(BF16)
    return high, (x - high.astype(F32)).astype(BF16)


def row_of(block):
    block = block.astype(F32)
    return jnp.concatenate([block[i : i + 1, :] for i in range(block.shape[0])], axis=1)


def rms(floats, gain):
    scale = lax.rsqrt(jnp.mean(floats * floats, axis=-1, keepdims=True) + EPS)
    return (floats * scale * gain).astype(BF16)


def kernel(*refs):
    hbm, outs, scratch = refs[:20], refs[20:23], refs[23:]
    (tok_h, gain_h, inw_h, decay_h, freq_h, step_h, inr_h, ini_h, outr_h, outi_h) = hbm[:10]
    (skip_h, str_h, sti_h, outw_h, fgain_h, ids_h, rw_h, gw_h, uw_h, dw_h) = hbm[10:]
    mixed_o, newr_o, newi_o = outs
    (tok, gain, inw, decay, freq, steps, inr, ini, outr, outi) = scratch[:10]
    (skip, st_r, st_i, outw, fgain, ids, rw, gw, uw, dw) = scratch[10:20]
    (delta, norm32, hid32, pick32, pick, zin) = scratch[20:26]
    (gat, hid, send, recv, sum32, back, zout, out32) = scratch[26:34]
    load, sent, dr_sem, zr_sem, gr_sem, fr_sem, hr_sem, rr_sem, br_sem, near_sem, far_sem = scratch[34:]
    D_SENT, Z_SENT, G_SENT, F_SENT, H_SENT, R_SENT, B_SENT = (sent.at[i] for i in range(7))

    ep, y = lax.axis_index("ep"), lax.axis_index("tp")
    z, x, c = ep // 8, (ep // 2) % NX, ep % 2

    def at(zz, xx, cc, yy):
        return (zz * 8 + xx * 2 + cc, yy)

    def turn(a, d, n):
        return lax.rem(a + d, n)

    def landed(ref, sem):
        pltpu.make_async_remote_copy(
            ref, ref, D_SENT, sem, device_id=at(z, x, 1 - c, y), device_id_type=MESH
        ).wait_recv()

    barrier = pltpu.get_barrier_semaphore()

    def enter(device):
        pl.semaphore_signal(barrier, inc=1, device_id=device, device_id_type=MESH)

    for d in range(1, NY):
        enter(at(z, x, 0, turn(y, d, NY)))
    for d in range(1, NZ):
        enter(at(turn(z, d, NZ), x, 1, y))
    for dx, dy in PLANE:
        if dx or dy:
            enter(at(z, turn(x, dx, NX), 1, turn(y, dy, NY)))
    enter(at(z, x, 1 - c, y))
    near_count = 2 * (NY - 1) + 1
    far_count = 2 * (NZ - 1) + 2 * (NX * NY - 1) + 1

    wide = pl.multiple_of((ep // 32) * 128, 128)
    sources = list(hbm)
    sources[15] = ids_h.at[:, pl.ds(wide, 128)]
    loads = [
        pltpu.make_async_copy(source, target, load.at[LOAD_GROUP[i]])
        for i, (source, target) in enumerate(zip(sources, scratch[:20]))
    ]
    for i in (0, 1, 2, 3, 4, 5, 6, 7, 11, 12, 8, 9, 10, 13, 14, 15, 16, 17, 18, 19):
        loads[i].start()

    loads[0].wait()
    loads[1].wait()
    tokens = tok[...].astype(F32)
    normed_in = rms(tokens, row_of(gain[...]))
    loads[2].wait()
    u = dot(normed_in, inw[...]).astype(BF16).astype(F32)

    rows = SEQ * GROUPS
    own_group = iota((rows, CHANNELS), 0) % GROUPS == iota((rows, CHANNELS), 1) // 16
    spread = jnp.broadcast_to(u[:, None, :], (SEQ, GROUPS, CHANNELS)).reshape(rows, CHANNELS)
    spread = jnp.where(own_group, spread, 0.0).astype(BF16)
    for i in (3, 4, 5, 6, 7):
        loads[i].wait()
    group_row = iota((GROUPS, STATE), 0)
    log_step = jnp.zeros((GROUPS, STATE), F32)
    for g in range(GROUPS):
        log_step = jnp.where(group_row == g, steps[g], log_step)
    step_size = jnp.exp(log_step)
    lam_real, frequency = -decay[...], freq[...]
    magnitude = jnp.exp(lam_real * step_size)
    turned = frequency * step_size
    bar_real = magnitude * jnp.cos(turned)
    bar_imag = magnitude * jnp.sin(turned)
    denom = lam_real * lam_real + frequency * frequency
    minus_one = bar_real - 1.0
    factor_real = (minus_one * lam_real + bar_imag * frequency) / denom
    factor_imag = (bar_imag * lam_real - minus_one * frequency) / denom

    def per_row(v):
        return jnp.broadcast_to(v[None], (SEQ, GROUPS, STATE)).reshape(rows, STATE)

    def drive(ref):
        high, low = split(ref[...].reshape(CHANNELS, STATE))
        return dot(spread, high) + dot(spread, low)

    drive_r, drive_i = drive(inr), drive(ini)
    bar_real, bar_imag = per_row(bar_real), per_row(bar_imag)
    factor_real, factor_imag = per_row(factor_real), per_row(factor_imag)
    loads[11].wait()
    loads[12].wait()
    state_r, state_i = st_r[...].reshape(rows, STATE), st_i[...].reshape(rows, STATE)
    new_r = (bar_real * state_r - bar_imag * state_i) + (factor_real * drive_r - factor_imag * drive_i)
    new_i = (bar_real * state_i + bar_imag * state_r) + (factor_real * drive_i + factor_imag * drive_r)
    newr_o[...] = new_r.reshape(SEQ, GROUPS, STATE)
    newi_o[...] = new_i.reshape(SEQ, GROUPS, STATE)

    for i in (8, 9, 10):
        loads[i].wait()

    def read(values, ref):
        high, low = split(values)
        ref_high, ref_low = split(ref[...].reshape(CHANNELS, STATE))
        return dot_t(high, ref_high) + dot_t(high, ref_low) + dot_t(low, ref_high)

    readout = jnp.where(own_group, read(new_r, outr) - read(new_i, outi), 0.0)
    readout = readout.reshape(SEQ, GROUPS, CHANNELS).sum(axis=1)
    readout = readout + row_of(skip[...]) * u
    activated = jax.nn.gelu(readout).astype(BF16)
    loads[13].wait()
    delta[y] = dot(activated, outw[...]).astype(BF16)

    @pl.when(c == 0)
    def _():
        pl.semaphore_wait(barrier, near_count)
        pl.semaphore_signal(near_sem, inc=1, device_id=at(z, x, 1, y), device_id_type=MESH)

    @pl.when(c == 1)
    def _():
        pl.semaphore_wait(near_sem, 1)

    delta_copies = [
        pltpu.make_async_remote_copy(
            delta.at[y], delta.at[y], D_SENT, dr_sem,
            device_id=at(z, x, c, turn(y, d, NY)), device_id_type=MESH,
        )
        for d in range(1, NY)
    ]
    for copy in delta_copies:
        copy.start()

    for i in (14, 15, 16):
        loads[i].wait()
    first = (ep % 32) * SEQ
    names = [[ids[k, first + s] for k in range(2)] for s in range(SEQ)]
    weights = [[rw[k, s] for k in range(2)] for s in range(SEQ)]

    def table(expert, slot, shape):
        taken = jnp.zeros(shape, I32)
        picks, scales = [], []
        for s in range(SEQ):
            routes = [expert == names[s][k] for k in range(2)]
            named = routes[0] | routes[1]
            here = named & (taken == slot)
            picks.append(jnp.where(here, 1.0, 0.0))
            scale = jnp.where(routes[0], weights[s][0], 0.0) + jnp.where(routes[1], weights[s][1], 0.0)
            scales.append(jnp.where(here, scale, 0.0))
            taken = taken + jnp.where(named, 1, 0)
        return picks, scales

    pick_row = iota((16, QUARTER), 0)
    picks, _ = table(pick_row // 2, pick_row % 2, (16, QUARTER))
    ffn_gain = row_of(fgain[...])

    landed(delta.at[0 : NY - 1], dr_sem)
    total = tokens
    for i in range(NY):
        total = total + delta[i].astype(F32)
    hidden_state = total.astype(BF16).astype(F32)
    hid32[...] = hidden_state
    norm32[...] = rms(hidden_state, ffn_gain).astype(F32)
    lanes = pl.ds(pl.multiple_of(y * QUARTER, QUARTER), QUARTER)
    own = norm32[:, lanes]
    chosen = picks[0] * own[0:1, :]
    for s in range(1, SEQ):
        chosen = chosen + picks[s] * own[s : s + 1, :]
    pick32[...] = chosen
    for e in range(8):
        pick[e] = pick32[2 * e : 2 * e + 2, :].astype(BF16)

    @pl.when(c == 1)
    def _():
        pl.semaphore_wait(barrier, far_count)
        pl.semaphore_signal(far_sem, inc=1, device_id=at(z, x, 0, y), device_id_type=MESH)

    @pl.when(c == 0)
    def _():
        pl.semaphore_wait(far_sem, 1)

    z_copies = []
    for d in (8, 7, 9, 6, 10, 5, 11, 4, 12, 3, 13, 2, 14, 1, 15):
        to = turn(z, d, NZ)
        z_copies.append(
            pltpu.make_async_remote_copy(
                pick.at[to // 2], zin.at[z], Z_SENT, zr_sem.at[z // HALF],
                device_id=at(to, x, c, y), device_id_type=MESH,
            )
        )
        z_copies[-1].start()
    pltpu.make_async_copy(pick.at[z // 2], zin.at[z], zr_sem.at[z // HALF]).start()

    gathers, forwards = [], {}

    def gather_chunk(k):
        landed(zin.at[k * HALF : (k + 1) * HALF], zr_sem.at[k])
        for i in range(HALF):
            sum32[2 * i : 2 * i + 2, :] = zin[k * HALF + i].astype(F32)
        gat[k, y, c, x] = sum32[...].astype(BF16)
        copies = []
        for dx, dy in reversed(PLANE):
            if dx or dy:
                copies.append(
                    pltpu.make_async_remote_copy(
                        gat.at[k, y, c, x], gat.at[k, y, c, x], G_SENT, gr_sem.at[k, dx],
                        device_id=at(z, turn(x, dx, NX), c, turn(y, dy, NY)), device_id_type=MESH,
                    )
                )
                copies[-1].start()
        gathers.append(copies)

    h_copies, r_copies = {}, {}

    def spread_chunk(k):
        copies = []
        for dx in (0, 1, 3, 2):
            rows_x = turn(x, NX - dx, NX)
            landed(gat.at[k, (0 if dx else 1) : NY, c, rows_x], gr_sem.at[k, dx])
            slots = gat.at[k, :, c, rows_x]
            copies.append(
                pltpu.make_async_remote_copy(
                    slots, slots, F_SENT, fr_sem.at[k], device_id=at(z, x, 1 - c, y), device_id_type=MESH
                )
            )
            copies[-1].start()
        forwards[k] = copies

    def up_chunk(k):
        landed(gat.at[k, :, 1 - c], fr_sem.at[k])
        gate_pre = jnp.zeros((128, HID), F32)
        up_pre = jnp.zeros((128, HID), F32)
        for q in range(NY):
            block = gat[k, q].reshape(128, QUARTER)
            gate_pre = gate_pre + dot(block, gw[q * QUARTER : (q + 1) * QUARTER, :])
            up_pre = up_pre + dot(block, uw[q * QUARTER : (q + 1) * QUARTER, :])
        units = pl.ds(pl.multiple_of(y * HID, HID), HID)
        hid[k, :, units] = (jax.nn.silu(gate_pre) * up_pre).astype(BF16)
        copies = []
        for d in (2, 1, 3):
            copies.append(
                pltpu.make_async_remote_copy(
                    hid.at[k, :, units], hid.at[k, :, units], H_SENT, hr_sem.at[k],
                    device_id=at(z, x, c, turn(y, d, NY)), device_id_type=MESH,
                )
            )
            copies[-1].start()
        h_copies[k] = copies

    def down_chunk(k):
        landed(hid.at[k, :, 0 : (NY - 1) * HID], hr_sem.at[k])
        send[k] = dot(hid[k], dw[...]).astype(BF16).reshape(NC, NX, 16, QUARTER)
        copies = []
        for dx in (2, 1, 3, 0):
            for dc in range(NC):
                if dx or dc:
                    to_x, to_c = turn(x, dx, NX), c if dc == 0 else 1 - c
                    copies.append(
                        pltpu.make_async_remote_copy(
                            send.at[k, to_c, to_x], recv.at[k, dc * NX + dx - 1], R_SENT, rr_sem.at[k],
                            device_id=at(z, to_x, to_c, y), device_id_type=MESH,
                        )
                    )
                    copies[-1].start()
        r_copies[k] = copies

    b_copies = {}

    def home_chunk(k):
        landed(recv.at[k], rr_sem.at[k])
        total = send[k, c, x].astype(F32)
        for i in range(NC * NX - 1):
            total = total + recv[k, i].astype(F32)
        sum32[...] = total
        for i in range(HALF):
            back[k, i] = sum32[2 * i : 2 * i + 2, :].astype(BF16)
        for i in range(HALF):
            home = k * HALF + i
            b_copies[home] = pltpu.make_async_remote_copy(
                back.at[k, i], zout.at[z], B_SENT, br_sem,
                device_id=at(home, x, c, y), device_id_type=MESH,
            )

            @pl.when(z != home)
            def _():
                b_copies[home].start()

            @pl.when(z == home)
            def _():
                pltpu.make_async_copy(back.at[k, i], zout.at[z], br_sem).start()

    gather_chunk(0)
    gather_chunk(1)
    spread_chunk(0)
    loads[17].wait()
    loads[18].wait()
    up_chunk(0)
    spread_chunk(1)
    up_chunk(1)
    loads[19].wait()
    down_chunk(0)
    down_chunk(1)
    home_chunk(0)
    home_chunk(1)

    back_row = iota((2 * NZ, QUARTER), 0)
    _, scales = table(back_row // 4, back_row % 2, (2 * NZ, QUARTER))
    landed(zout, br_sem)
    for p in range(NZ):
        out32[2 * p : 2 * p + 2, :] = zout[p].astype(F32)
    pieces = out32[...]
    routed = [jnp.sum(scales[s] * pieces, axis=0, keepdims=True) for s in range(SEQ)]
    mixed_o[...] = (hid32[:, lanes] + jnp.concatenate(routed, axis=0)).astype(BF16)

    for copy in delta_copies + z_copies:
        copy.wait_send()
    for home, copy in b_copies.items():

        @pl.when(z != home)
        def _():
            copy.wait_send()

    for copies in gathers + [group[k] for group in (forwards, h_copies, r_copies) for k in range(2)]:
        for copy in copies:
            copy.wait_send()


def store_kernel(*refs):
    sources, targets, sem = refs[:3], refs[3:6], refs[6]
    copies = [pltpu.make_async_copy(s, t, sem.at[i]) for i, (s, t) in enumerate(zip(sources, targets))]
    for copy in copies:
        copy.start()
    for copy in copies:
        copy.wait()


def shards(*args):
    args = list(args)
    for i in (1, 14):
        args[i] = args[i].reshape(16, 128)
    args[10] = args[10].reshape(2, 128)
    for i in (6, 7):
        args[i] = args[i].transpose(0, 2, 1)
    args[15], args[16] = args[15].T, args[16].T
    held = []
    for i, arg in enumerate(args):
        if i in (5, 16):
            held.append(pltpu.SMEM(arg.shape, arg.dtype))
        elif i == 15:
            held.append(pltpu.SMEM((2, 128), arg.dtype))
        else:
            held.append(pltpu.VMEM(arg.shape, arg.dtype))
    dma = pltpu.SemaphoreType.DMA
    shapes = (((SEQ, QUARTER), BF16), ((SEQ, GROUPS, STATE), F32), ((SEQ, GROUPS, STATE), F32))
    scratch = held + [
        pltpu.VMEM((NY, SEQ, WIDTH), BF16),
        pltpu.VMEM((SEQ, WIDTH), F32),
        pltpu.VMEM((SEQ, WIDTH), F32),
        pltpu.VMEM((16, QUARTER), F32),
        pltpu.VMEM((8, 2, QUARTER), BF16),
        pltpu.VMEM((NZ, 2, QUARTER), BF16),
        pltpu.VMEM((2, NY, NC, NX, 16, QUARTER), BF16),
        pltpu.VMEM((2, 128, NY * HID), BF16),
        pltpu.VMEM((2, NC, NX, 16, QUARTER), BF16),
        pltpu.VMEM((2, NC * NX - 1, 16, QUARTER), BF16),
        pltpu.VMEM((16, QUARTER), F32),
        pltpu.VMEM((2, 8, 2, QUARTER), BF16),
        pltpu.VMEM((NZ, 2, QUARTER), BF16),
        pltpu.VMEM((2 * NZ, QUARTER), F32),
        dma((9,)), dma((7,)),
        dma, dma((2,)), dma((2, NX)), dma((2,)), dma((2,)), dma((2,)), dma,
        pltpu.SemaphoreType.REGULAR,
        pltpu.SemaphoreType.REGULAR,
    ]
    anywhere = pl.BlockSpec(memory_space=pl.ANY)
    near = pl.BlockSpec(memory_space=pltpu.VMEM)
    results = pl.pallas_call(
        kernel,
        out_shape=tuple(pltpu.VMEM(*shape) for shape in shapes),
        in_specs=[anywhere] * 20,
        out_specs=(near,) * 3,
        scratch_shapes=scratch,
        compiler_params=pltpu.CompilerParams(
            collective_id=0, has_side_effects=True, vmem_limit_bytes=VMEM_LIMIT
        ),
    )(*args)
    return pl.pallas_call(
        store_kernel,
        out_shape=tuple(jax.ShapeDtypeStruct(*shape) for shape in shapes),
        in_specs=[anywhere] * 3,
        out_specs=(anywhere,) * 3,
        scratch_shapes=[dma((3,))],
        compiler_params=pltpu.CompilerParams(vmem_limit_bytes=VMEM_LIMIT),
    )(*[pltpu.with_memory_space_constraint(r, pltpu.VMEM) for r in results])


def solution(mesh):
    in_specs = (
        P("ep", None), P(), P(None, "tp"), P("tp", None), P("tp", None), P("tp"),
        P("tp", None, None), P("tp", None, None), P("tp", None, None), P("tp", None, None), P("tp"),
        P("ep", "tp", None), P("ep", "tp", None), P("tp", None), P(), P(), P("ep", None),
        P(None, ("ep", "tp")), P(None, ("ep", "tp")), P("ep", "tp"),
    )
    out_specs = (P("ep", "tp"), P("ep", "tp", None), P("ep", "tp", None))
    return jax.shard_map(shards, mesh=mesh, in_specs=in_specs, out_specs=out_specs, check_vma=False)
```

```python
import jax
import jax.numpy as jnp
from jax import lax
from jax.experimental import pallas as pl
from jax.experimental.pallas import tpu as pltpu
from jax.sharding import PartitionSpec as P

EPS = 1e-06
F32, BF16, I32 = jnp.float32, jnp.bfloat16, jnp.int32
MESH = pl.DeviceIdType.MESH
NX, NY, NC, NZ = 4, 4, 2, 16
SEQ, WIDTH, QUARTER = 4, 2048, 512
GROUPS, STATE, CHANNELS = 16, 64, 256
HID = 128
HALF = NZ // 2
FAR_FIRST = (8, 7, 9, 6, 10, 5, 11, 4, 12, 3, 13, 2, 14, 1, 15)
VMEM_LIMIT = 67043328 - 72 * 1024
LOAD_GROUP = (0, 0, 1, 2, 2, 2, 2, 2, 4, 4, 4, 3, 3, 5, 6, 6, 6, 7, 7, 8)
PLANE = sorted(
    [(dx, dy) for dx in range(NX) for dy in range(NY)],
    key=lambda d: min(d[0], NX - d[0]) + min(d[1], NY - d[1]),
)


def iota(shape, dim):
    return lax.broadcasted_iota(I32, shape, dim)


def dot(a, b):
    return jnp.dot(a, b, preferred_element_type=F32)


def dot_t(a, b):
    return lax.dot_general(a, b, (((1,), (1,)), ((), ())), preferred_element_type=F32)


def split(x):
    high = x.astype(BF16)
    return high, (x - high.astype(F32)).astype(BF16)


def row_of(block):
    block = block.astype(F32)
    return jnp.concatenate([block[i : i + 1, :] for i in range(block.shape[0])], axis=1)


def rms(floats, gain):
    scale = lax.rsqrt(jnp.mean(floats * floats, axis=-1, keepdims=True) + EPS)
    return (floats * scale * gain).astype(BF16)


def kernel(*refs):
    hbm, outs, scratch = refs[:20], refs[20:23], refs[23:]
    (tok_h, gain_h, inw_h, decay_h, freq_h, step_h, inr_h, ini_h, outr_h, outi_h) = hbm[:10]
    (skip_h, str_h, sti_h, outw_h, fgain_h, ids_h, rw_h, gw_h, uw_h, dw_h) = hbm[10:]
    mixed_o, newr_o, newi_o = outs
    (tok, gain, inw, decay, freq, steps, inr, ini, outr, outi) = scratch[:10]
    (skip, st_r, st_i, outw, fgain, ids, rw, gw, uw, dw) = scratch[10:20]
    (delta, norm32, hid32, pick32, pick, zin) = scratch[20:26]
    (gat, hid, send, recv, sum32, back, zout, out32) = scratch[26:34]
    load, sent, dr_sem, zr_sem, gr_sem, fr_sem, hr_sem, rr_sem, br_sem, near_sem, far_sem = scratch[34:]
    D_SENT, Z_SENT, G_SENT, F_SENT, H_SENT, R_SENT, B_SENT = (sent.at[i] for i in range(7))

    ep, y = lax.axis_index("ep"), lax.axis_index("tp")
    z, x, c = ep // 8, (ep // 2) % NX, ep % 2

    def at(zz, xx, cc, yy):
        return (zz * 8 + xx * 2 + cc, yy)

    def turn(a, d, n):
        return lax.rem(a + d, n)

    def landed(ref, sem):
        pltpu.make_async_remote_copy(
            ref, ref, D_SENT, sem, device_id=at(z, x, 1 - c, y), device_id_type=MESH
        ).wait_recv()

    barrier = pltpu.get_barrier_semaphore()

    def enter(device):
        pl.semaphore_signal(barrier, inc=1, device_id=device, device_id_type=MESH)

    for d in FAR_FIRST:
        enter(at(turn(z, d, NZ), x, 1, y))
    for d in range(1, NY):
        enter(at(z, x, 0, turn(y, d, NY)))
    for dx, dy in PLANE:
        if dx or dy:
            enter(at(z, turn(x, dx, NX), 1, turn(y, dy, NY)))
    enter(at(z, x, 1 - c, y))
    near_count = 2 * (NY - 1) + 1
    far_count = 2 * (NZ - 1) + 2 * (NX * NY - 1) + 1

    wide = pl.multiple_of((ep // 32) * 128, 128)
    sources = list(hbm)
    sources[15] = ids_h.at[:, pl.ds(wide, 128)]
    loads = [
        pltpu.make_async_copy(source, target, load.at[LOAD_GROUP[i]])
        for i, (source, target) in enumerate(zip(sources, scratch[:20]))
    ]
    for i in (0, 1, 2, 3, 4, 5, 6, 7, 11, 12, 8, 9, 10, 13, 14, 15, 16, 17, 18, 19):
        loads[i].start()

    loads[0].wait()
    loads[1].wait()
    tokens = tok[...].astype(F32)
    normed_in = rms(tokens, row_of(gain[...]))
    loads[2].wait()
    u = dot(normed_in, inw[...]).astype(BF16).astype(F32)

    rows = SEQ * GROUPS
    own_group = iota((rows, CHANNELS), 0) % GROUPS == iota((rows, CHANNELS), 1) // 16
    spread = jnp.broadcast_to(u[:, None, :], (SEQ, GROUPS, CHANNELS)).reshape(rows, CHANNELS)
    spread = jnp.where(own_group, spread, 0.0).astype(BF16)
    for i in (3, 4, 5, 6, 7):
        loads[i].wait()
    group_row = iota((GROUPS, STATE), 0)
    log_step = jnp.zeros((GROUPS, STATE), F32)
    for g in range(GROUPS):
        log_step = jnp.where(group_row == g, steps[g], log_step)
    step_size = jnp.exp(log_step)
    lam_real, frequency = -decay[...], freq[...]
    magnitude = jnp.exp(lam_real * step_size)
    turned = frequency * step_size
    bar_real = magnitude * jnp.cos(turned)
    bar_imag = magnitude * jnp.sin(turned)
    denom = lam_real * lam_real + frequency * frequency
    minus_one = bar_real - 1.0
    factor_real = (minus_one * lam_real + bar_imag * frequency) / denom
    factor_imag = (bar_imag * lam_real - minus_one * frequency) / denom

    def per_row(v):
        return jnp.broadcast_to(v[None], (SEQ, GROUPS, STATE)).reshape(rows, STATE)

    def drive(ref):
        high, low = split(ref[...].reshape(CHANNELS, STATE))
        return dot(spread, high) + dot(spread, low)

    drive_r, drive_i = drive(inr), drive(ini)
    bar_real, bar_imag = per_row(bar_real), per_row(bar_imag)
    factor_real, factor_imag = per_row(factor_real), per_row(factor_imag)
    loads[11].wait()
    loads[12].wait()
    state_r, state_i = st_r[...].reshape(rows, STATE), st_i[...].reshape(rows, STATE)
    new_r = (bar_real * state_r - bar_imag * state_i) + (factor_real * drive_r - factor_imag * drive_i)
    new_i = (bar_real * state_i + bar_imag * state_r) + (factor_real * drive_i + factor_imag * drive_r)
    newr_o[...] = new_r.reshape(SEQ, GROUPS, STATE)
    newi_o[...] = new_i.reshape(SEQ, GROUPS, STATE)

    for i in (8, 9, 10):
        loads[i].wait()

    def read(values, ref):
        high, low = split(values)
        ref_high, ref_low = split(ref[...].reshape(CHANNELS, STATE))
        return dot_t(high, ref_high) + dot_t(high, ref_low) + dot_t(low, ref_high)

    readout = jnp.where(own_group, read(new_r, outr) - read(new_i, outi), 0.0)
    readout = readout.reshape(SEQ, GROUPS, CHANNELS).sum(axis=1)
    readout = readout + row_of(skip[...]) * u
    activated = jax.nn.gelu(readout).astype(BF16)
    loads[13].wait()
    delta[y] = dot(activated, outw[...]).astype(BF16)

    @pl.when(c == 0)
    def _():
        pl.semaphore_wait(barrier, near_count)
        pl.semaphore_signal(near_sem, inc=1, device_id=at(z, x, 1, y), device_id_type=MESH)

    @pl.when(c == 1)
    def _():
        pl.semaphore_wait(near_sem, 1)

    delta_copies = [
        pltpu.make_async_remote_copy(
            delta.at[y], delta.at[y], D_SENT, dr_sem,
            device_id=at(z, x, c, turn(y, d, NY)), device_id_type=MESH,
        )
        for d in range(1, NY)
    ]
    for copy in delta_copies:
        copy.start()

    for i in (14, 15, 16):
        loads[i].wait()
    first = (ep % 32) * SEQ
    names = [[ids[k, first + s] for k in range(2)] for s in range(SEQ)]
    weights = [[rw[k, s] for k in range(2)] for s in range(SEQ)]

    def table(expert, slot, shape):
        taken = jnp.zeros(shape, I32)
        picks, scales = [], []
        for s in range(SEQ):
            routes = [expert == names[s][k] for k in range(2)]
            named = routes[0] | routes[1]
            here = named & (taken == slot)
            picks.append(jnp.where(here, 1.0, 0.0))
            scale = jnp.where(routes[0], weights[s][0], 0.0) + jnp.where(routes[1], weights[s][1], 0.0)
            scales.append(jnp.where(here, scale, 0.0))
            taken = taken + jnp.where(named, 1, 0)
        return picks, scales

    pick_row = iota((16, QUARTER), 0)
    picks, _ = table(pick_row // 2, pick_row % 2, (16, QUARTER))
    ffn_gain = row_of(fgain[...])

    landed(delta.at[0 : NY - 1], dr_sem)
    total = tokens
    for i in range(NY):
        total = total + delta[i].astype(F32)
    hidden_state = total.astype(BF16).astype(F32)
    hid32[...] = hidden_state
    norm32[...] = rms(hidden_state, ffn_gain).astype(F32)
    lanes = pl.ds(pl.multiple_of(y * QUARTER, QUARTER), QUARTER)
    own = norm32[:, lanes]
    chosen = picks[0] * own[0:1, :]
    for s in range(1, SEQ):
        chosen = chosen + picks[s] * own[s : s + 1, :]
    pick32[...] = chosen
    for e in range(8):
        pick[e] = pick32[2 * e : 2 * e + 2, :].astype(BF16)

    @pl.when(c == 1)
    def _():
        pl.semaphore_wait(barrier, far_count)
        pl.semaphore_signal(far_sem, inc=1, device_id=at(z, x, 0, y), device_id_type=MESH)

    @pl.when(c == 0)
    def _():
        pl.semaphore_wait(far_sem, 1)

    z_copies = []
    for d in FAR_FIRST:
        to = turn(z, d, NZ)
        z_copies.append(
            pltpu.make_async_remote_copy(
                pick.at[to // 2], zin.at[z], Z_SENT, zr_sem.at[z // HALF],
                device_id=at(to, x, c, y), device_id_type=MESH,
            )
        )
        z_copies[-1].start()
    pltpu.make_async_copy(pick.at[z // 2], zin.at[z], zr_sem.at[z // HALF]).start()

    gathers, forwards = [], []

    def take_chunk(k):
        landed(zin.at[k * HALF : (k + 1) * HALF], zr_sem.at[k])
        for i in range(HALF):
            sum32[2 * i : 2 * i + 2, :] = zin[k * HALF + i].astype(F32)
        gat[k, y, c, x] = sum32[...].astype(BF16)

    def pass_on(slots, k, dx, dy):
        copy = pltpu.make_async_remote_copy(
            slots, slots, G_SENT, gr_sem.at[k, dx],
            device_id=at(z, turn(x, dx, NX), c, turn(y, dy, NY)), device_id_type=MESH,
        )
        copy.start()
        gathers.append(copy)

    def gather_at_once(k):
        for dx, dy in reversed(PLANE):
            if dx or dy:
                pass_on(gat.at[k, y, c, x], k, dx, dy)

    def gather_along_y(k):
        for dy in (2, 1, 3):
            pass_on(gat.at[k, y, c, x], k, 0, dy)

    def gather_along_x(k):
        spread_chunk(k, (0,))
        for dx in (2, 1, 3):
            pass_on(gat.at[k, :, c, x], k, dx, 0)

    h_copies, r_copies = {}, {}

    def spread_chunk(k, distances):
        for dx in distances:
            rows_x = turn(x, NX - dx, NX)
            landed(gat.at[k, (0 if dx else 1) : NY, c, rows_x], gr_sem.at[k, dx])
            slots = gat.at[k, :, c, rows_x]
            copy = pltpu.make_async_remote_copy(
                slots, slots, F_SENT, fr_sem.at[k], device_id=at(z, x, 1 - c, y), device_id_type=MESH
            )
            copy.start()
            forwards.append(copy)

    def up_chunk(k):
        landed(gat.at[k, :, 1 - c], fr_sem.at[k])
        gate_pre = jnp.zeros((128, HID), F32)
        up_pre = jnp.zeros((128, HID), F32)
        for q in range(NY):
            block = gat[k, q].reshape(128, QUARTER)
            gate_pre = gate_pre + dot(block, gw[q * QUARTER : (q + 1) * QUARTER, :])
            up_pre = up_pre + dot(block, uw[q * QUARTER : (q + 1) * QUARTER, :])
        units = pl.ds(pl.multiple_of(y * HID, HID), HID)
        hid[k, :, units] = (jax.nn.silu(gate_pre) * up_pre).astype(BF16)
        copies = []
        for d in (2, 1, 3):
            copies.append(
                pltpu.make_async_remote_copy(
                    hid.at[k, :, units], hid.at[k, :, units], H_SENT, hr_sem.at[k],
                    device_id=at(z, x, c, turn(y, d, NY)), device_id_type=MESH,
                )
            )
            copies[-1].start()
        h_copies[k] = copies

    def down_chunk(k):
        landed(hid.at[k, :, 0 : (NY - 1) * HID], hr_sem.at[k])
        send[k] = dot(hid[k], dw[...]).astype(BF16).reshape(NC, NX, 16, QUARTER)
        copies = []
        for dx in (2, 1, 3, 0):
            for dc in range(NC):
                if dx or dc:
                    to_x, to_c = turn(x, dx, NX), c if dc == 0 else 1 - c
                    copies.append(
                        pltpu.make_async_remote_copy(
                            send.at[k, to_c, to_x], recv.at[k, dc * NX + dx - 1], R_SENT, rr_sem.at[k],
                            device_id=at(z, to_x, to_c, y), device_id_type=MESH,
                        )
                    )
                    copies[-1].start()
        r_copies[k] = copies

    b_copies = {}

    def home_chunk(k):
        landed(recv.at[k], rr_sem.at[k])
        total = send[k, c, x].astype(F32)
        for i in range(NC * NX - 1):
            total = total + recv[k, i].astype(F32)
        sum32[...] = total
        for i in range(HALF):
            back[k, i] = sum32[2 * i : 2 * i + 2, :].astype(BF16)
        for i in range(HALF):
            home = k * HALF + i
            b_copies[home] = pltpu.make_async_remote_copy(
                back.at[k, i], zout.at[z], B_SENT, br_sem,
                device_id=at(home, x, c, y), device_id_type=MESH,
            )

            @pl.when(z != home)
            def _():
                b_copies[home].start()

            @pl.when(z == home)
            def _():
                pltpu.make_async_copy(back.at[k, i], zout.at[z], br_sem).start()

    take_chunk(0)
    gather_at_once(0)
    take_chunk(1)
    gather_along_y(1)
    spread_chunk(0, (0, 1, 3, 2))
    gather_along_x(1)
    loads[17].wait()
    loads[18].wait()
    up_chunk(0)
    loads[19].wait()
    down_chunk(0)
    spread_chunk(1, (1, 3, 2))
    up_chunk(1)
    home_chunk(0)
    down_chunk(1)
    home_chunk(1)

    back_row = iota((2 * NZ, QUARTER), 0)
    _, scales = table(back_row // 4, back_row % 2, (2 * NZ, QUARTER))
    landed(zout, br_sem)
    for p in range(NZ):
        out32[2 * p : 2 * p + 2, :] = zout[p].astype(F32)
    pieces = out32[...]
    routed = [jnp.sum(scales[s] * pieces, axis=0, keepdims=True) for s in range(SEQ)]
    mixed_o[...] = (hid32[:, lanes] + jnp.concatenate(routed, axis=0)).astype(BF16)

    for copy in delta_copies + z_copies:
        copy.wait_send()
    for home, copy in b_copies.items():

        @pl.when(z != home)
        def _():
            copy.wait_send()

    for copy in gathers + forwards + h_copies[0] + h_copies[1] + r_copies[0] + r_copies[1]:
        copy.wait_send()


def store_kernel(*refs):
    sources, targets, sem = refs[:3], refs[3:6], refs[6]
    copies = [pltpu.make_async_copy(s, t, sem.at[i]) for i, (s, t) in enumerate(zip(sources, targets))]
    for copy in copies:
        copy.start()
    for copy in copies:
        copy.wait()


def shards(*args):
    args = list(args)
    for i in (1, 14):
        args[i] = args[i].reshape(16, 128)
    args[10] = args[10].reshape(2, 128)
    for i in (6, 7):
        args[i] = args[i].transpose(0, 2, 1)
    args[15], args[16] = args[15].T, args[16].T
    held = []
    for i, arg in enumerate(args):
        if i in (5, 16):
            held.append(pltpu.SMEM(arg.shape, arg.dtype))
        elif i == 15:
            held.append(pltpu.SMEM((2, 128), arg.dtype))
        else:
            held.append(pltpu.VMEM(arg.shape, arg.dtype))
    dma = pltpu.SemaphoreType.DMA
    shapes = (((SEQ, QUARTER), BF16), ((SEQ, GROUPS, STATE), F32), ((SEQ, GROUPS, STATE), F32))
    scratch = held + [
        pltpu.VMEM((NY, SEQ, WIDTH), BF16),
        pltpu.VMEM((SEQ, WIDTH), F32),
        pltpu.VMEM((SEQ, WIDTH), F32),
        pltpu.VMEM((16, QUARTER), F32),
        pltpu.VMEM((8, 2, QUARTER), BF16),
        pltpu.VMEM((NZ, 2, QUARTER), BF16),
        pltpu.VMEM((2, NY, NC, NX, 16, QUARTER), BF16),
        pltpu.VMEM((2, 128, NY * HID), BF16),
        pltpu.VMEM((2, NC, NX, 16, QUARTER), BF16),
        pltpu.VMEM((2, NC * NX - 1, 16, QUARTER), BF16),
        pltpu.VMEM((16, QUARTER), F32),
        pltpu.VMEM((2, 8, 2, QUARTER), BF16),
        pltpu.VMEM((NZ, 2, QUARTER), BF16),
        pltpu.VMEM((2 * NZ, QUARTER), F32),
        dma((9,)), dma((7,)),
        dma, dma((2,)), dma((2, NX)), dma((2,)), dma((2,)), dma((2,)), dma,
        pltpu.SemaphoreType.REGULAR,
        pltpu.SemaphoreType.REGULAR,
    ]
    anywhere = pl.BlockSpec(memory_space=pl.ANY)
    near = pl.BlockSpec(memory_space=pltpu.VMEM)
    results = pl.pallas_call(
        kernel,
        out_shape=tuple(pltpu.VMEM(*shape) for shape in shapes),
        in_specs=[anywhere] * 20,
        out_specs=(near,) * 3,
        scratch_shapes=scratch,
        compiler_params=pltpu.CompilerParams(
            collective_id=0, has_side_effects=True, vmem_limit_bytes=VMEM_LIMIT
        ),
    )(*args)
    return pl.pallas_call(
        store_kernel,
        out_shape=tuple(jax.ShapeDtypeStruct(*shape) for shape in shapes),
        in_specs=[anywhere] * 3,
        out_specs=(anywhere,) * 3,
        scratch_shapes=[dma((3,))],
        compiler_params=pltpu.CompilerParams(vmem_limit_bytes=VMEM_LIMIT),
    )(*[pltpu.with_memory_space_constraint(r, pltpu.VMEM) for r in results])


def solution(mesh):
    in_specs = (
        P("ep", None), P(), P(None, "tp"), P("tp", None), P("tp", None), P("tp"),
        P("tp", None, None), P("tp", None, None), P("tp", None, None), P("tp", None, None), P("tp"),
        P("ep", "tp", None), P("ep", "tp", None), P("tp", None), P(), P(), P("ep", None),
        P(None, ("ep", "tp")), P(None, ("ep", "tp")), P("ep", "tp"),
    )
    out_specs = (P("ep", "tp"), P("ep", "tp", None), P("ep", "tp", None))
    return jax.shard_map(shards, mesh=mesh, in_specs=in_specs, out_specs=out_specs, check_vma=False)
```

```python
import jax
import jax.numpy as jnp
from jax import lax
from jax.experimental import pallas as pl
from jax.experimental.pallas import tpu as pltpu
from jax.sharding import PartitionSpec as P

EPS = 1e-06
F32, BF16, I32 = jnp.float32, jnp.bfloat16, jnp.int32
MESH = pl.DeviceIdType.MESH
NX, NY, NC, NZ = 4, 4, 2, 16
SEQ, WIDTH, QUARTER = 4, 2048, 512
GROUPS, STATE, CHANNELS = 16, 64, 256
HID = 128
CHUNKS = ((0, 4), (4, 8), (8, 16))
FAR_FIRST = (8, 7, 9, 6, 10, 5, 11, 4, 12, 3, 13, 2, 14, 1, 15)
VMEM_LIMIT = 67043328 - 72 * 1024
LOAD_GROUP = (0, 0, 1, 2, 2, 2, 2, 2, 4, 4, 4, 3, 3, 5, 6, 6, 6, 7, 7, 8)
PLANE = sorted(
    [(dx, dy) for dx in range(NX) for dy in range(NY)],
    key=lambda d: min(d[0], NX - d[0]) + min(d[1], NY - d[1]),
)


def iota(shape, dim):
    return lax.broadcasted_iota(I32, shape, dim)


def dot(a, b):
    return jnp.dot(a, b, preferred_element_type=F32)


def dot_t(a, b):
    return lax.dot_general(a, b, (((1,), (1,)), ((), ())), preferred_element_type=F32)


def split(x):
    high = x.astype(BF16)
    return high, (x - high.astype(F32)).astype(BF16)


def row_of(block):
    block = block.astype(F32)
    return jnp.concatenate([block[i : i + 1, :] for i in range(block.shape[0])], axis=1)


def rms(floats, gain):
    scale = lax.rsqrt(jnp.mean(floats * floats, axis=-1, keepdims=True) + EPS)
    return (floats * scale * gain).astype(BF16)


def kernel(*refs):
    hbm, outs, scratch = refs[:20], refs[20:23], refs[23:]
    (tok_h, gain_h, inw_h, decay_h, freq_h, step_h, inr_h, ini_h, outr_h, outi_h) = hbm[:10]
    (skip_h, str_h, sti_h, outw_h, fgain_h, ids_h, rw_h, gw_h, uw_h, dw_h) = hbm[10:]
    mixed_o, newr_o, newi_o = outs
    (tok, gain, inw, decay, freq, steps, inr, ini, outr, outi) = scratch[:10]
    (skip, st_r, st_i, outw, fgain, ids, rw, gw, uw, dw) = scratch[10:20]
    (delta, norm32, hid32, pick32, pick, zin) = scratch[20:26]
    sum32, zout, out32 = scratch[26:29]
    load, sent, dr_sem, zr_sem, gr_sem, fr_sem, hr_sem, rr_sem, br_sem, near_sem, far_sem = scratch[29:40]
    gat, hid, send, recv, back = (scratch[40 + i :: 5] for i in range(5))
    D_SENT, Z_SENT, G_SENT, F_SENT, H_SENT, R_SENT, B_SENT = (sent.at[i] for i in range(7))

    ep, y = lax.axis_index("ep"), lax.axis_index("tp")
    z, x, c = ep // 8, (ep // 2) % NX, ep % 2

    def at(zz, xx, cc, yy):
        return (zz * 8 + xx * 2 + cc, yy)

    def chunk_of(home):
        return lax.min(home // 4, 2)

    def turn(a, d, n):
        return lax.rem(a + d, n)

    def landed(ref, sem):
        pltpu.make_async_remote_copy(
            ref, ref, D_SENT, sem, device_id=at(z, x, 1 - c, y), device_id_type=MESH
        ).wait_recv()

    barrier = pltpu.get_barrier_semaphore()

    def enter(device):
        pl.semaphore_signal(barrier, inc=1, device_id=device, device_id_type=MESH)

    for d in FAR_FIRST:
        enter(at(turn(z, d, NZ), x, 1, y))
    for d in range(1, NY):
        enter(at(z, x, 0, turn(y, d, NY)))
    for dx, dy in PLANE:
        if dx or dy:
            enter(at(z, turn(x, dx, NX), 1, turn(y, dy, NY)))
    enter(at(z, x, 1 - c, y))
    near_count = 2 * (NY - 1) + 1
    far_count = 2 * (NZ - 1) + 2 * (NX * NY - 1) + 1

    wide = pl.multiple_of((ep // 32) * 128, 128)
    sources = list(hbm)
    sources[15] = ids_h.at[:, pl.ds(wide, 128)]
    loads = [
        pltpu.make_async_copy(source, target, load.at[LOAD_GROUP[i]])
        for i, (source, target) in enumerate(zip(sources, scratch[:20]))
    ]
    for i in (0, 1, 2, 3, 4, 5, 6, 7, 11, 12, 8, 9, 10, 13, 14, 15, 16, 17, 18, 19):
        loads[i].start()

    loads[0].wait()
    loads[1].wait()
    tokens = tok[...].astype(F32)
    normed_in = rms(tokens, row_of(gain[...]))
    loads[2].wait()
    u = dot(normed_in, inw[...]).astype(BF16).astype(F32)

    rows = SEQ * GROUPS
    own_group = iota((rows, CHANNELS), 0) % GROUPS == iota((rows, CHANNELS), 1) // 16
    spread = jnp.broadcast_to(u[:, None, :], (SEQ, GROUPS, CHANNELS)).reshape(rows, CHANNELS)
    spread = jnp.where(own_group, spread, 0.0).astype(BF16)
    for i in (3, 4, 5, 6, 7):
        loads[i].wait()
    group_row = iota((GROUPS, STATE), 0)
    log_step = jnp.zeros((GROUPS, STATE), F32)
    for g in range(GROUPS):
        log_step = jnp.where(group_row == g, steps[g], log_step)
    step_size = jnp.exp(log_step)
    lam_real, frequency = -decay[...], freq[...]
    magnitude = jnp.exp(lam_real * step_size)
    turned = frequency * step_size
    bar_real = magnitude * jnp.cos(turned)
    bar_imag = magnitude * jnp.sin(turned)
    denom = lam_real * lam_real + frequency * frequency
    minus_one = bar_real - 1.0
    factor_real = (minus_one * lam_real + bar_imag * frequency) / denom
    factor_imag = (bar_imag * lam_real - minus_one * frequency) / denom

    def per_row(v):
        return jnp.broadcast_to(v[None], (SEQ, GROUPS, STATE)).reshape(rows, STATE)

    def drive(ref):
        high, low = split(ref[...].reshape(CHANNELS, STATE))
        return dot(spread, high) + dot(spread, low)

    drive_r, drive_i = drive(inr), drive(ini)
    bar_real, bar_imag = per_row(bar_real), per_row(bar_imag)
    factor_real, factor_imag = per_row(factor_real), per_row(factor_imag)
    loads[11].wait()
    loads[12].wait()
    state_r, state_i = st_r[...].reshape(rows, STATE), st_i[...].reshape(rows, STATE)
    new_r = (bar_real * state_r - bar_imag * state_i) + (factor_real * drive_r - factor_imag * drive_i)
    new_i = (bar_real * state_i + bar_imag * state_r) + (factor_real * drive_i + factor_imag * drive_r)
    newr_o[...] = new_r.reshape(SEQ, GROUPS, STATE)
    newi_o[...] = new_i.reshape(SEQ, GROUPS, STATE)

    for i in (8, 9, 10):
        loads[i].wait()

    def read(values, ref):
        high, low = split(values)
        ref_high, ref_low = split(ref[...].reshape(CHANNELS, STATE))
        return dot_t(high, ref_high) + dot_t(high, ref_low) + dot_t(low, ref_high)

    readout = jnp.where(own_group, read(new_r, outr) - read(new_i, outi), 0.0)
    readout = readout.reshape(SEQ, GROUPS, CHANNELS).sum(axis=1)
    readout = readout + row_of(skip[...]) * u
    activated = jax.nn.gelu(readout).astype(BF16)
    loads[13].wait()
    delta[y] = dot(activated, outw[...]).astype(BF16)

    @pl.when(c == 0)
    def _():
        pl.semaphore_wait(barrier, near_count)
        pl.semaphore_signal(near_sem, inc=1, device_id=at(z, x, 1, y), device_id_type=MESH)

    @pl.when(c == 1)
    def _():
        pl.semaphore_wait(near_sem, 1)

    delta_copies = [
        pltpu.make_async_remote_copy(
            delta.at[y], delta.at[y], D_SENT, dr_sem,
            device_id=at(z, x, c, turn(y, d, NY)), device_id_type=MESH,
        )
        for d in range(1, NY)
    ]
    for copy in delta_copies:
        copy.start()

    for i in (14, 15, 16):
        loads[i].wait()
    first = (ep % 32) * SEQ
    names = [[ids[k, first + s] for k in range(2)] for s in range(SEQ)]
    weights = [[rw[k, s] for k in range(2)] for s in range(SEQ)]

    def table(expert, slot, shape):
        taken = jnp.zeros(shape, I32)
        picks, scales = [], []
        for s in range(SEQ):
            routes = [expert == names[s][k] for k in range(2)]
            named = routes[0] | routes[1]
            here = named & (taken == slot)
            picks.append(jnp.where(here, 1.0, 0.0))
            scale = jnp.where(routes[0], weights[s][0], 0.0) + jnp.where(routes[1], weights[s][1], 0.0)
            scales.append(jnp.where(here, scale, 0.0))
            taken = taken + jnp.where(named, 1, 0)
        return picks, scales

    pick_row = iota((16, QUARTER), 0)
    picks, _ = table(pick_row // 2, pick_row % 2, (16, QUARTER))
    ffn_gain = row_of(fgain[...])

    landed(delta.at[0 : NY - 1], dr_sem)
    total = tokens
    for i in range(NY):
        total = total + delta[i].astype(F32)
    hidden_state = total.astype(BF16).astype(F32)
    hid32[...] = hidden_state
    norm32[...] = rms(hidden_state, ffn_gain).astype(F32)
    lanes = pl.ds(pl.multiple_of(y * QUARTER, QUARTER), QUARTER)
    own = norm32[:, lanes]
    chosen = picks[0] * own[0:1, :]
    for s in range(1, SEQ):
        chosen = chosen + picks[s] * own[s : s + 1, :]
    pick32[...] = chosen
    for e in range(8):
        pick[e] = pick32[2 * e : 2 * e + 2, :].astype(BF16)

    @pl.when(c == 1)
    def _():
        pl.semaphore_wait(barrier, far_count)
        pl.semaphore_signal(far_sem, inc=1, device_id=at(z, x, 0, y), device_id_type=MESH)

    @pl.when(c == 0)
    def _():
        pl.semaphore_wait(far_sem, 1)

    z_copies = []
    for d in FAR_FIRST:
        to = turn(z, d, NZ)
        z_copies.append(
            pltpu.make_async_remote_copy(
                pick.at[to // 2], zin.at[z], Z_SENT, zr_sem.at[chunk_of(z)],
                device_id=at(to, x, c, y), device_id_type=MESH,
            )
        )
        z_copies[-1].start()
    pltpu.make_async_copy(pick.at[z // 2], zin.at[z], zr_sem.at[chunk_of(z)]).start()

    gathers, forwards = [], []

    def take_chunk(k):
        low, high = CHUNKS[k]
        landed(zin.at[low:high], zr_sem.at[k])
        for i in range(high - low):
            sum32[2 * i : 2 * i + 2, :] = zin[low + i].astype(F32)
        gat[k][y, c, x] = sum32[0 : 2 * (high - low), :].astype(BF16)

    def pass_on(slots, k, dx, dy):
        copy = pltpu.make_async_remote_copy(
            slots, slots, G_SENT, gr_sem.at[k, dx],
            device_id=at(z, turn(x, dx, NX), c, turn(y, dy, NY)), device_id_type=MESH,
        )
        copy.start()
        gathers.append(copy)

    def gather_at_once(k):
        for dx, dy in reversed(PLANE):
            if dx or dy:
                pass_on(gat[k].at[y, c, x], k, dx, dy)

    def gather_along_y(k):
        for dy in (2, 1, 3):
            pass_on(gat[k].at[y, c, x], k, 0, dy)

    def gather_along_x(k):
        spread_chunk(k, (0,))
        for dx in (2, 1, 3):
            pass_on(gat[k].at[:, c, x], k, dx, 0)

    h_copies, r_copies = {}, {}

    def spread_chunk(k, distances):
        for dx in distances:
            rows_x = turn(x, NX - dx, NX)
            landed(gat[k].at[(0 if dx else 1) : NY, c, rows_x], gr_sem.at[k, dx])
            slots = gat[k].at[:, c, rows_x]
            copy = pltpu.make_async_remote_copy(
                slots, slots, F_SENT, fr_sem.at[k], device_id=at(z, x, 1 - c, y), device_id_type=MESH
            )
            copy.start()
            forwards.append(copy)

    def up_chunk(k):
        landed(gat[k].at[:, 1 - c], fr_sem.at[k])
        rows = hid[k].shape[0]
        gate_pre = jnp.zeros((rows, HID), F32)
        up_pre = jnp.zeros((rows, HID), F32)
        for q in range(NY):
            block = gat[k][q].astype(F32).reshape(rows, QUARTER).astype(BF16)
            gate_pre = gate_pre + dot(block, gw[q * QUARTER : (q + 1) * QUARTER, :])
            up_pre = up_pre + dot(block, uw[q * QUARTER : (q + 1) * QUARTER, :])
        units = pl.ds(pl.multiple_of(y * HID, HID), HID)
        hid[k][:, units] = (jax.nn.silu(gate_pre) * up_pre).astype(BF16)
        copies = []
        for d in (2, 1, 3):
            copies.append(
                pltpu.make_async_remote_copy(
                    hid[k].at[:, units], hid[k].at[:, units], H_SENT, hr_sem.at[k],
                    device_id=at(z, x, c, turn(y, d, NY)), device_id_type=MESH,
                )
            )
            copies[-1].start()
        h_copies[k] = copies

    def down_chunk(k):
        landed(hid[k].at[:, 0 : (NY - 1) * HID], hr_sem.at[k])
        send[k][...] = dot(hid[k][...], dw[...]).reshape(send[k].shape).astype(BF16)
        copies = []
        for dx in (2, 1, 3, 0):
            for dc in range(NC):
                if dx or dc:
                    to_x, to_c = turn(x, dx, NX), c if dc == 0 else 1 - c
                    copies.append(
                        pltpu.make_async_remote_copy(
                            send[k].at[to_c, to_x], recv[k].at[dc * NX + dx - 1], R_SENT, rr_sem.at[k],
                            device_id=at(z, to_x, to_c, y), device_id_type=MESH,
                        )
                    )
                    copies[-1].start()
        r_copies[k] = copies

    b_copies = {}

    def home_chunk(k):
        landed(recv[k], rr_sem.at[k])
        total = send[k][c, x].astype(F32)
        for i in range(NC * NX - 1):
            total = total + recv[k][i].astype(F32)
        low, high = CHUNKS[k]
        sum32[0 : 2 * (high - low), :] = total
        for i in range(high - low):
            back[k][i] = sum32[2 * i : 2 * i + 2, :].astype(BF16)
        for i in range(high - low):
            home = low + i
            b_copies[home] = pltpu.make_async_remote_copy(
                back[k].at[i], zout.at[z], B_SENT, br_sem,
                device_id=at(home, x, c, y), device_id_type=MESH,
            )

            @pl.when(z != home)
            def _():
                b_copies[home].start()

            @pl.when(z == home)
            def _():
                pltpu.make_async_copy(back[k].at[i], zout.at[z], br_sem).start()

    take_chunk(0)
    gather_at_once(0)
    take_chunk(1)
    gather_along_y(1)
    take_chunk(2)
    gather_along_y(2)
    spread_chunk(0, (0, 1, 3, 2))
    gather_along_x(1)
    gather_along_x(2)
    loads[17].wait()
    loads[18].wait()
    up_chunk(0)
    spread_chunk(1, (1, 3, 2))
    loads[19].wait()
    down_chunk(0)
    spread_chunk(2, (1, 3, 2))
    up_chunk(1)
    up_chunk(2)
    home_chunk(0)
    down_chunk(1)
    down_chunk(2)
    home_chunk(1)
    home_chunk(2)

    back_row = iota((2 * NZ, QUARTER), 0)
    _, scales = table(back_row // 4, back_row % 2, (2 * NZ, QUARTER))
    landed(zout, br_sem)
    for p in range(NZ):
        out32[2 * p : 2 * p + 2, :] = zout[p].astype(F32)
    pieces = out32[...]
    routed = [jnp.sum(scales[s] * pieces, axis=0, keepdims=True) for s in range(SEQ)]
    mixed_o[...] = (hid32[:, lanes] + jnp.concatenate(routed, axis=0)).astype(BF16)

    for copy in delta_copies + z_copies:
        copy.wait_send()
    for home, copy in b_copies.items():

        @pl.when(z != home)
        def _():
            copy.wait_send()

    for copy in gathers + forwards + sum(h_copies.values(), []) + sum(r_copies.values(), []):
        copy.wait_send()


def store_kernel(*refs):
    sources, targets, sem = refs[:3], refs[3:6], refs[6]
    copies = [pltpu.make_async_copy(s, t, sem.at[i]) for i, (s, t) in enumerate(zip(sources, targets))]
    for copy in copies:
        copy.start()
    for copy in copies:
        copy.wait()


def shards(*args):
    args = list(args)
    for i in (1, 14):
        args[i] = args[i].reshape(16, 128)
    args[10] = args[10].reshape(2, 128)
    for i in (6, 7):
        args[i] = args[i].transpose(0, 2, 1)
    args[15], args[16] = args[15].T, args[16].T
    held = []
    for i, arg in enumerate(args):
        if i in (5, 16):
            held.append(pltpu.SMEM(arg.shape, arg.dtype))
        elif i == 15:
            held.append(pltpu.SMEM((2, 128), arg.dtype))
        else:
            held.append(pltpu.VMEM(arg.shape, arg.dtype))
    dma = pltpu.SemaphoreType.DMA
    shapes = (((SEQ, QUARTER), BF16), ((SEQ, GROUPS, STATE), F32), ((SEQ, GROUPS, STATE), F32))
    scratch = held + [
        pltpu.VMEM((NY, SEQ, WIDTH), BF16),
        pltpu.VMEM((SEQ, WIDTH), F32),
        pltpu.VMEM((SEQ, WIDTH), F32),
        pltpu.VMEM((16, QUARTER), F32),
        pltpu.VMEM((8, 2, QUARTER), BF16),
        pltpu.VMEM((NZ, 2, QUARTER), BF16),
        pltpu.VMEM((16, QUARTER), F32),
        pltpu.VMEM((NZ, 2, QUARTER), BF16),
        pltpu.VMEM((2 * NZ, QUARTER), F32),
        dma((9,)), dma((7,)),
        dma, dma((3,)), dma((3, NX)), dma((3,)), dma((3,)), dma((3,)), dma,
        pltpu.SemaphoreType.REGULAR,
        pltpu.SemaphoreType.REGULAR,
    ]
    for low, high in CHUNKS:
        block = 2 * (high - low)
        scratch += [
            pltpu.VMEM((NY, NC, NX, block, QUARTER), BF16),
            pltpu.VMEM((NC * NX * block, NY * HID), BF16),
            pltpu.VMEM((NC, NX, block, QUARTER), BF16),
            pltpu.VMEM((NC * NX - 1, block, QUARTER), BF16),
            pltpu.VMEM((high - low, 2, QUARTER), BF16),
        ]
    anywhere = pl.BlockSpec(memory_space=pl.ANY)
    near = pl.BlockSpec(memory_space=pltpu.VMEM)
    results = pl.pallas_call(
        kernel,
        out_shape=tuple(pltpu.VMEM(*shape) for shape in shapes),
        in_specs=[anywhere] * 20,
        out_specs=(near,) * 3,
        scratch_shapes=scratch,
        compiler_params=pltpu.CompilerParams(
            collective_id=0, has_side_effects=True, vmem_limit_bytes=VMEM_LIMIT
        ),
    )(*args)
    return pl.pallas_call(
        store_kernel,
        out_shape=tuple(jax.ShapeDtypeStruct(*shape) for shape in shapes),
        in_specs=[anywhere] * 3,
        out_specs=(anywhere,) * 3,
        scratch_shapes=[dma((3,))],
        compiler_params=pltpu.CompilerParams(vmem_limit_bytes=VMEM_LIMIT),
    )(*[pltpu.with_memory_space_constraint(r, pltpu.VMEM) for r in results])


def solution(mesh):
    in_specs = (
        P("ep", None), P(), P(None, "tp"), P("tp", None), P("tp", None), P("tp"),
        P("tp", None, None), P("tp", None, None), P("tp", None, None), P("tp", None, None), P("tp"),
        P("ep", "tp", None), P("ep", "tp", None), P("tp", None), P(), P(), P("ep", None),
        P(None, ("ep", "tp")), P(None, ("ep", "tp")), P("ep", "tp"),
    )
    out_specs = (P("ep", "tp"), P("ep", "tp", None), P("ep", "tp", None))
    return jax.shard_map(shards, mesh=mesh, in_specs=in_specs, out_specs=out_specs, check_vma=False)
```

```python
import jax
import jax.numpy as jnp
from jax import lax
from jax.experimental import pallas as pl
from jax.experimental.pallas import tpu as pltpu
from jax.sharding import PartitionSpec as P

EPS = 1e-06
F32, BF16, I32 = jnp.float32, jnp.bfloat16, jnp.int32
MESH = pl.DeviceIdType.MESH
NX, NY, NC, NZ = 4, 4, 2, 16
SEQ, WIDTH, QUARTER = 4, 2048, 512
GROUPS, STATE, CHANNELS = 16, 64, 256
HID = 128
CHUNKS = ((0, 4), (4, 8), (8, 16))
FAR_FIRST = (8, 7, 9, 6, 10, 5, 11, 4, 12, 3, 13, 2, 14, 1, 15)
VMEM_LIMIT = 67043328 - 72 * 1024
LOAD_GROUP = (0, 0, 1, 2, 2, 2, 2, 2, 4, 4, 4, 3, 3, 5, 6, 6, 6, 7, 7, 8)
PLANE = sorted(
    [(dx, dy) for dx in range(NX) for dy in range(NY)],
    key=lambda d: min(d[0], NX - d[0]) + min(d[1], NY - d[1]),
)


def iota(shape, dim):
    return lax.broadcasted_iota(I32, shape, dim)


def dot(a, b):
    return jnp.dot(a, b, preferred_element_type=F32)


def dot_t(a, b):
    return lax.dot_general(a, b, (((1,), (1,)), ((), ())), preferred_element_type=F32)


def split(x):
    high = x.astype(BF16)
    return high, (x - high.astype(F32)).astype(BF16)


def row_of(block):
    block = block.astype(F32)
    return jnp.concatenate([block[i : i + 1, :] for i in range(block.shape[0])], axis=1)


def rms(floats, gain):
    scale = lax.rsqrt(jnp.mean(floats * floats, axis=-1, keepdims=True) + EPS)
    return (floats * scale * gain).astype(BF16)


def kernel(*refs):
    hbm, outs, scratch = refs[:20], refs[20:23], refs[23:]
    (tok_h, gain_h, inw_h, decay_h, freq_h, step_h, inr_h, ini_h, outr_h, outi_h) = hbm[:10]
    (skip_h, str_h, sti_h, outw_h, fgain_h, ids_h, rw_h, gw_h, uw_h, dw_h) = hbm[10:]
    mixed_o, newr_o, newi_o = outs
    (tok, gain, inw, decay, freq, steps, inr, ini, outr, outi) = scratch[:10]
    (skip, st_r, st_i, outw, fgain, ids, rw, gw, uw, dw) = scratch[10:20]
    (delta, norm32, hid32, pick32, pick, zin) = scratch[20:26]
    sum32, zout, out32 = scratch[26:29]
    load, sent, dr_sem, zr_sem, gr_sem, fr_sem, hr_sem, rr_sem, br_sem, near_sem, far_sem = scratch[29:40]
    gat, hid, send, recv, back = (scratch[40 + i :: 5] for i in range(5))
    D_SENT, Z_SENT, G_SENT, F_SENT, H_SENT, R_SENT, B_SENT = (sent.at[i] for i in range(7))

    ep, y = lax.axis_index("ep"), lax.axis_index("tp")
    z, x, c = ep // 8, (ep // 2) % NX, ep % 2

    def at(zz, xx, cc, yy):
        return (zz * 8 + xx * 2 + cc, yy)

    def chunk_of(home):
        return lax.min(home // 4, 2)

    def turn(a, d, n):
        return lax.rem(a + d, n)

    def landed(ref, sem):
        pltpu.make_async_remote_copy(
            ref, ref, D_SENT, sem, device_id=at(z, x, 1 - c, y), device_id_type=MESH
        ).wait_recv()

    sent_by_all, sent_by, sent_home = [], ([], []), []

    def send_away(source, target, send_sem, recv_sem, device, sent_list, alike):
        pltpu.make_async_remote_copy(
            source, target, send_sem, recv_sem, device_id=device, device_id_type=MESH
        ).start()
        sent_list.append((alike, send_sem))

    def left(alike, sem):
        ref = alike[0].at[alike[1]]
        pltpu.make_async_remote_copy(
            ref, ref, sem, dr_sem, device_id=at(z, x, 1 - c, y), device_id_type=MESH
        ).wait_send()

    barrier = pltpu.get_barrier_semaphore()

    def enter(device):
        pl.semaphore_signal(barrier, inc=1, device_id=device, device_id_type=MESH)

    for d in FAR_FIRST:
        enter(at(turn(z, d, NZ), x, 1, y))
    for d in range(1, NY):
        enter(at(z, x, 0, turn(y, d, NY)))
    for dx, dy in PLANE:
        if dx or dy:
            enter(at(z, turn(x, dx, NX), 1, turn(y, dy, NY)))
    enter(at(z, x, 1 - c, y))
    near_count = 2 * (NY - 1) + 1
    far_count = 2 * (NZ - 1) + 2 * (NX * NY - 1) + 1

    wide = pl.multiple_of((ep // 32) * 128, 128)
    sources = list(hbm)
    sources[15] = ids_h.at[:, pl.ds(wide, 128)]
    loads = [
        pltpu.make_async_copy(source, target, load.at[LOAD_GROUP[i]])
        for i, (source, target) in enumerate(zip(sources, scratch[:20]))
    ]
    for i in (0, 1, 2, 3, 4, 5, 6, 7, 11, 12, 8, 9, 10, 13, 14, 15, 16, 17, 18, 19):
        loads[i].start()

    loads[0].wait()
    loads[1].wait()
    tokens = tok[...].astype(F32)
    normed_in = rms(tokens, row_of(gain[...]))
    loads[2].wait()
    u = dot(normed_in, inw[...]).astype(BF16).astype(F32)

    rows = SEQ * GROUPS
    own_group = iota((rows, CHANNELS), 0) % GROUPS == iota((rows, CHANNELS), 1) // 16
    spread = jnp.broadcast_to(u[:, None, :], (SEQ, GROUPS, CHANNELS)).reshape(rows, CHANNELS)
    spread = jnp.where(own_group, spread, 0.0).astype(BF16)
    for i in (3, 4, 5, 6, 7):
        loads[i].wait()
    group_row = iota((GROUPS, STATE), 0)
    log_step = jnp.zeros((GROUPS, STATE), F32)
    for g in range(GROUPS):
        log_step = jnp.where(group_row == g, steps[g], log_step)
    step_size = jnp.exp(log_step)
    lam_real, frequency = -decay[...], freq[...]
    magnitude = jnp.exp(lam_real * step_size)
    turned = frequency * step_size
    bar_real = magnitude * jnp.cos(turned)
    bar_imag = magnitude * jnp.sin(turned)
    denom = lam_real * lam_real + frequency * frequency
    minus_one = bar_real - 1.0
    factor_real = (minus_one * lam_real + bar_imag * frequency) / denom
    factor_imag = (bar_imag * lam_real - minus_one * frequency) / denom

    def per_row(v):
        return jnp.broadcast_to(v[None], (SEQ, GROUPS, STATE)).reshape(rows, STATE)

    def drive(ref):
        high, low = split(ref[...].reshape(CHANNELS, STATE))
        return dot(spread, high) + dot(spread, low)

    drive_r, drive_i = drive(inr), drive(ini)
    bar_real, bar_imag = per_row(bar_real), per_row(bar_imag)
    factor_real, factor_imag = per_row(factor_real), per_row(factor_imag)
    loads[11].wait()
    loads[12].wait()
    state_r, state_i = st_r[...].reshape(rows, STATE), st_i[...].reshape(rows, STATE)
    new_r = (bar_real * state_r - bar_imag * state_i) + (factor_real * drive_r - factor_imag * drive_i)
    new_i = (bar_real * state_i + bar_imag * state_r) + (factor_real * drive_i + factor_imag * drive_r)
    newr_o[...] = new_r.reshape(SEQ, GROUPS, STATE)
    newi_o[...] = new_i.reshape(SEQ, GROUPS, STATE)

    for i in (8, 9, 10):
        loads[i].wait()

    def read(values, ref):
        high, low = split(values)
        ref_high, ref_low = split(ref[...].reshape(CHANNELS, STATE))
        return dot_t(high, ref_high) + dot_t(high, ref_low) + dot_t(low, ref_high)

    readout = jnp.where(own_group, read(new_r, outr) - read(new_i, outi), 0.0)
    readout = readout.reshape(SEQ, GROUPS, CHANNELS).sum(axis=1)
    readout = readout + row_of(skip[...]) * u
    activated = jax.nn.gelu(readout).astype(BF16)
    loads[13].wait()
    delta[y] = dot(activated, outw[...]).astype(BF16)

    @pl.when(c == 0)
    def _():
        pl.semaphore_wait(barrier, near_count)
        pl.semaphore_signal(near_sem, inc=1, device_id=at(z, x, 1, y), device_id_type=MESH)

    @pl.when(c == 1)
    def _():
        pl.semaphore_wait(near_sem, 1)

    delta_copies = [
        pltpu.make_async_remote_copy(
            delta.at[y], delta.at[y], D_SENT, dr_sem,
            device_id=at(z, x, c, turn(y, d, NY)), device_id_type=MESH,
        )
        for d in range(1, NY)
    ]
    for copy in delta_copies:
        copy.start()

    for i in (14, 15, 16):
        loads[i].wait()
    first = (ep % 32) * SEQ
    names = [[ids[k, first + s] for k in range(2)] for s in range(SEQ)]
    weights = [[rw[k, s] for k in range(2)] for s in range(SEQ)]

    def table(expert, slot, shape):
        taken = jnp.zeros(shape, I32)
        picks, scales = [], []
        for s in range(SEQ):
            routes = [expert == names[s][k] for k in range(2)]
            named = routes[0] | routes[1]
            here = named & (taken == slot)
            picks.append(jnp.where(here, 1.0, 0.0))
            scale = jnp.where(routes[0], weights[s][0], 0.0) + jnp.where(routes[1], weights[s][1], 0.0)
            scales.append(jnp.where(here, scale, 0.0))
            taken = taken + jnp.where(named, 1, 0)
        return picks, scales

    pick_row = iota((16, QUARTER), 0)
    picks, _ = table(pick_row // 2, pick_row % 2, (16, QUARTER))
    ffn_gain = row_of(fgain[...])

    landed(delta.at[0 : NY - 1], dr_sem)
    total = tokens
    for i in range(NY):
        total = total + delta[i].astype(F32)
    hidden_state = total.astype(BF16).astype(F32)
    hid32[...] = hidden_state
    norm32[...] = rms(hidden_state, ffn_gain).astype(F32)
    lanes = pl.ds(pl.multiple_of(y * QUARTER, QUARTER), QUARTER)
    own = norm32[:, lanes]
    chosen = picks[0] * own[0:1, :]
    for s in range(1, SEQ):
        chosen = chosen + picks[s] * own[s : s + 1, :]
    pick32[...] = chosen
    for e in range(8):
        pick[e] = pick32[2 * e : 2 * e + 2, :].astype(BF16)

    @pl.when(c == 1)
    def _():
        pl.semaphore_wait(barrier, far_count)
        pl.semaphore_signal(far_sem, inc=1, device_id=at(z, x, 0, y), device_id_type=MESH)

    @pl.when(c == 0)
    def _():
        pl.semaphore_wait(far_sem, 1)

    for d in FAR_FIRST:
        to = turn(z, d, NZ)
        send_away(pick.at[to // 2], zin.at[z, c], Z_SENT, zr_sem.at[chunk_of(z)], at(to, x, 1, y), sent_by_all, (pick, 0))
    own_slots = (pick.at[z // 2], zin.at[z, c])

    @pl.when(c == 1)
    def _():
        pltpu.make_async_copy(*own_slots, zr_sem.at[chunk_of(z)]).start()

    @pl.when(c == 0)
    def _():
        send_away(*own_slots, Z_SENT, zr_sem.at[chunk_of(z)], at(z, x, 1, y), sent_by[0], (pick, 0))

    def take_chunk(k):
        low, high = CHUNKS[k]
        block = 2 * (high - low)
        landed(zin.at[low:high], zr_sem.at[k])
        for core in range(NC):
            for i in range(high - low):
                row = core * block + 2 * i
                sum32[row : row + 2, :] = zin[low + i, core].astype(F32)
        gat[k][y, x] = sum32[0 : 2 * block, :].astype(BF16)

    def pass_on(slots, alike, k, dx, dy):
        to = at(z, turn(x, dx, NX), 1, turn(y, dy, NY))
        send_away(slots, slots, G_SENT, gr_sem.at[k, dx], to, sent_by[1], alike)

    def gather_at_once(k):
        for dx, dy in reversed(PLANE):
            if dx or dy:
                pass_on(gat[k].at[y, x], (gat[k], (0, 0)), k, dx, dy)

    def gather_along_y(k):
        for dy in (2, 1, 3):
            pass_on(gat[k].at[y, x], (gat[k], (0, 0)), k, 0, dy)

    def gather_along_x(k):
        spread_chunk(k, (0,))
        for dx in (2, 1, 3):
            pass_on(gat[k].at[:, x], (gat[k], (slice(None), 0)), k, dx, 0)

    def spread_chunk(k, distances):
        for dx in distances:
            rows_x = turn(x, NX - dx, NX)
            landed(gat[k].at[(0 if dx else 1) : NY, rows_x], gr_sem.at[k, dx])
            slots = gat[k].at[:, rows_x]
            send_away(slots, slots, F_SENT, fr_sem.at[k], at(z, x, 0, y), sent_by[1], (gat[k], (slice(None), 0)))

    def up_chunk(k):
        @pl.when(c == 0)
        def _():
            landed(gat[k], fr_sem.at[k])

        rows = hid[k].shape[0]
        gate_pre = jnp.zeros((rows, HID), F32)
        up_pre = jnp.zeros((rows, HID), F32)
        for q in range(NY):
            block = gat[k][q].reshape(rows, QUARTER)
            gate_pre = gate_pre + dot(block, gw[q * QUARTER : (q + 1) * QUARTER, :])
            up_pre = up_pre + dot(block, uw[q * QUARTER : (q + 1) * QUARTER, :])
        units = pl.ds(pl.multiple_of(y * HID, HID), HID)
        hid[k][:, units] = (jax.nn.silu(gate_pre) * up_pre).astype(BF16)
        own_units = hid[k].at[:, units]
        for d in (2, 1, 3):
            to = at(z, x, c, turn(y, d, NY))
            send_away(own_units, own_units, H_SENT, hr_sem.at[k], to, sent_by_all, (hid[k], (slice(None), slice(0, HID))))

    def down_chunk(k):
        landed(hid[k].at[:, 0 : (NY - 1) * HID], hr_sem.at[k])
        send[k][...] = dot(hid[k][...], dw[...]).astype(BF16).reshape(send[k].shape)
        for dx in (2, 1, 3):
            to = turn(x, dx, NX)
            slot = recv[k].at[2 * dx - 1 + c]
            send_away(send[k].at[to], slot, R_SENT, rr_sem.at[k], at(z, to, 1, y), sent_by_all, (send[k], 0))

        @pl.when(c == 0)
        def _():
            home = at(z, x, 1, y)
            send_away(send[k].at[x], recv[k].at[0], R_SENT, rr_sem.at[k], home, sent_by[0], (send[k], 0))

    def home_chunk(k):
        landed(recv[k], rr_sem.at[k])
        total = send[k][x].astype(F32)
        for i in range(NC * NX - 1):
            total = total + recv[k][i].astype(F32)
        low, high = CHUNKS[k]
        block = 2 * (high - low)
        sum32[0 : 2 * block, :] = total
        for core in range(NC):
            for i in range(high - low):
                row = core * block + 2 * i
                back[k][i, core] = sum32[row : row + 2, :].astype(BF16)
        for i in range(high - low):
            home = low + i
            slots = back[k].at[i, 0]
            send_away(slots, zout.at[z], B_SENT, br_sem, at(home, x, 0, y), sent_by[1], (pick, 0))

            @pl.when(z != home)
            def _():
                slots = back[k].at[i, 1]
                send_away(slots, zout.at[z], B_SENT, br_sem, at(home, x, 1, y), sent_home, (pick, 0))

            @pl.when(z == home)
            def _():
                pltpu.make_async_copy(back[k].at[i, 1], zout.at[z], br_sem).start()

    on_core_1 = pl.when(c == 1)

    @on_core_1
    def _():
        take_chunk(0)
        gather_at_once(0)
        take_chunk(1)
        gather_along_y(1)
        take_chunk(2)
        gather_along_y(2)
        spread_chunk(0, (0, 1, 3, 2))
        gather_along_x(1)
        gather_along_x(2)

    loads[17].wait()
    loads[18].wait()
    up_chunk(0)
    on_core_1(lambda: spread_chunk(1, (1, 3, 2)))
    loads[19].wait()
    down_chunk(0)
    on_core_1(lambda: spread_chunk(2, (1, 3, 2)))
    up_chunk(1)
    up_chunk(2)
    on_core_1(lambda: home_chunk(0))
    down_chunk(1)
    down_chunk(2)
    on_core_1(lambda: home_chunk(1))
    on_core_1(lambda: home_chunk(2))

    back_row = iota((2 * NZ, QUARTER), 0)
    _, scales = table(back_row // 4, back_row % 2, (2 * NZ, QUARTER))
    landed(zout, br_sem)
    for p in range(NZ):
        out32[2 * p : 2 * p + 2, :] = zout[p].astype(F32)
    pieces = out32[...]
    routed = [jnp.sum(scales[s] * pieces, axis=0, keepdims=True) for s in range(SEQ)]
    mixed_o[...] = (hid32[:, lanes] + jnp.concatenate(routed, axis=0)).astype(BF16)

    for copy in delta_copies:
        copy.wait_send()
    for copy in sent_by_all:
        left(*copy)
    for core in range(NC):

        @pl.when(c == core)
        def _():
            for copy in sent_by[core]:
                left(*copy)

    for home, copy in enumerate(sent_home):

        @pl.when((c == 1) & (z != home))
        def _():
            left(*copy)


def store_kernel(*refs):
    sources, targets, sem = refs[:3], refs[3:6], refs[6]
    copies = [pltpu.make_async_copy(s, t, sem.at[i]) for i, (s, t) in enumerate(zip(sources, targets))]
    for copy in copies:
        copy.start()
    for copy in copies:
        copy.wait()


def shards(*args):
    args = list(args)
    for i in (1, 14):
        args[i] = args[i].reshape(16, 128)
    args[10] = args[10].reshape(2, 128)
    for i in (6, 7):
        args[i] = args[i].transpose(0, 2, 1)
    args[15], args[16] = args[15].T, args[16].T
    held = []
    for i, arg in enumerate(args):
        if i in (5, 16):
            held.append(pltpu.SMEM(arg.shape, arg.dtype))
        elif i == 15:
            held.append(pltpu.SMEM((2, 128), arg.dtype))
        else:
            held.append(pltpu.VMEM(arg.shape, arg.dtype))
    dma = pltpu.SemaphoreType.DMA
    shapes = (((SEQ, QUARTER), BF16), ((SEQ, GROUPS, STATE), F32), ((SEQ, GROUPS, STATE), F32))
    scratch = held + [
        pltpu.VMEM((NY, SEQ, WIDTH), BF16),
        pltpu.VMEM((SEQ, WIDTH), F32),
        pltpu.VMEM((SEQ, WIDTH), F32),
        pltpu.VMEM((16, QUARTER), F32),
        pltpu.VMEM((8, 2, QUARTER), BF16),
        pltpu.VMEM((NZ, NC, 2, QUARTER), BF16),
        pltpu.VMEM((32, QUARTER), F32),
        pltpu.VMEM((NZ, 2, QUARTER), BF16),
        pltpu.VMEM((2 * NZ, QUARTER), F32),
        dma((9,)), dma((7,)),
        dma, dma((3,)), dma((3, NX)), dma((3,)), dma((3,)), dma((3,)), dma,
        pltpu.SemaphoreType.REGULAR,
        pltpu.SemaphoreType.REGULAR,
    ]
    for low, high in CHUNKS:
        block = 2 * NC * (high - low)
        scratch += [
            pltpu.VMEM((NY, NX, block, QUARTER), BF16),
            pltpu.VMEM((NX * block, NY * HID), BF16),
            pltpu.VMEM((NX, block, QUARTER), BF16),
            pltpu.VMEM((NC * NX - 1, block, QUARTER), BF16),
            pltpu.VMEM((high - low, NC, 2, QUARTER), BF16),
        ]
    anywhere = pl.BlockSpec(memory_space=pl.ANY)
    near = pl.BlockSpec(memory_space=pltpu.VMEM)
    results = pl.pallas_call(
        kernel,
        out_shape=tuple(pltpu.VMEM(*shape) for shape in shapes),
        in_specs=[anywhere] * 20,
        out_specs=(near,) * 3,
        scratch_shapes=scratch,
        compiler_params=pltpu.CompilerParams(
            collective_id=0, has_side_effects=True, vmem_limit_bytes=VMEM_LIMIT
        ),
    )(*args)
    return pl.pallas_call(
        store_kernel,
        out_shape=tuple(jax.ShapeDtypeStruct(*shape) for shape in shapes),
        in_specs=[anywhere] * 3,
        out_specs=(anywhere,) * 3,
        scratch_shapes=[dma((3,))],
        compiler_params=pltpu.CompilerParams(vmem_limit_bytes=VMEM_LIMIT),
    )(*[pltpu.with_memory_space_constraint(r, pltpu.VMEM) for r in results])


def solution(mesh):
    in_specs = (
        P("ep", None), P(), P(None, "tp"), P("tp", None), P("tp", None), P("tp"),
        P("tp", None, None), P("tp", None, None), P("tp", None, None), P("tp", None, None), P("tp"),
        P("ep", "tp", None), P("ep", "tp", None), P("tp", None), P(), P(), P("ep", None),
        P(None, ("ep", "tp")), P(None, ("ep", "tp")), P("ep", "tp"),
    )
    out_specs = (P("ep", "tp"), P("ep", "tp", None), P("ep", "tp", None))
    return jax.shard_map(shards, mesh=mesh, in_specs=in_specs, out_specs=out_specs, check_vma=False)
```

```python
import jax
import jax.numpy as jnp
from jax import lax
from jax.experimental import pallas as pl
from jax.experimental.pallas import tpu as pltpu
from jax.sharding import PartitionSpec as P

EPS = 1e-06
F32, BF16, I32 = jnp.float32, jnp.bfloat16, jnp.int32
MESH = pl.DeviceIdType.MESH
NX, NY, NC, NZ = 4, 4, 2, 16
SEQ, WIDTH, QUARTER = 4, 2048, 512
GROUPS, STATE, CHANNELS = 16, 64, 256
HID = 128
CHUNKS = ((0, 4), (4, 8), (8, 16))
SUMS = (1, 1, 0)
FAR_FIRST = (8, 7, 9, 6, 10, 5, 11, 4, 12, 3, 13, 2, 14, 1, 15)
VMEM_LIMIT = 67043328 - 72 * 1024
LOAD_GROUP = (0, 0, 1, 2, 2, 2, 2, 2, 4, 4, 4, 3, 3, 5, 6, 6, 6, 7, 7, 8)
PLANE = sorted(
    [(dx, dy) for dx in range(NX) for dy in range(NY)],
    key=lambda d: min(d[0], NX - d[0]) + min(d[1], NY - d[1]),
)


def iota(shape, dim):
    return lax.broadcasted_iota(I32, shape, dim)


def dot(a, b):
    return jnp.dot(a, b, preferred_element_type=F32)


def dot_t(a, b):
    return lax.dot_general(a, b, (((1,), (1,)), ((), ())), preferred_element_type=F32)


def split(x):
    high = x.astype(BF16)
    return high, (x - high.astype(F32)).astype(BF16)


def row_of(block):
    block = block.astype(F32)
    return jnp.concatenate([block[i : i + 1, :] for i in range(block.shape[0])], axis=1)


def rms(floats, gain):
    scale = lax.rsqrt(jnp.mean(floats * floats, axis=-1, keepdims=True) + EPS)
    return (floats * scale * gain).astype(BF16)


def kernel(*refs):
    hbm, outs, scratch = refs[:20], refs[20:23], refs[23:]
    (tok_h, gain_h, inw_h, decay_h, freq_h, step_h, inr_h, ini_h, outr_h, outi_h) = hbm[:10]
    (skip_h, str_h, sti_h, outw_h, fgain_h, ids_h, rw_h, gw_h, uw_h, dw_h) = hbm[10:]
    mixed_o, newr_o, newi_o = outs
    (tok, gain, inw, decay, freq, steps, inr, ini, outr, outi) = scratch[:10]
    (skip, st_r, st_i, outw, fgain, ids, rw, gw, uw, dw) = scratch[10:20]
    (delta, norm32, hid32, pick32, pick, zin) = scratch[20:26]
    sum32, zout, out32 = scratch[26:29]
    load, sent, dr_sem, zr_sem, gr_sem, fr_sem, hr_sem, rr_sem, br_sem, near_sem, far_sem = scratch[29:40]
    gat, hid, send, recv, back = (scratch[40 + i :: 5] for i in range(5))
    D_SENT, Z_SENT, G_SENT, F_SENT, H_SENT, R_SENT, B_SENT = (sent.at[i] for i in range(7))

    ep, y = lax.axis_index("ep"), lax.axis_index("tp")
    z, x, c = ep // 8, (ep // 2) % NX, ep % 2

    def at(zz, xx, cc, yy):
        return (zz * 8 + xx * 2 + cc, yy)

    def chunk_of(home):
        return lax.min(home // 4, 2)

    def turn(a, d, n):
        return lax.rem(a + d, n)

    def landed(ref, sem):
        pltpu.make_async_remote_copy(
            ref, ref, D_SENT, sem, device_id=at(z, x, 1 - c, y), device_id_type=MESH
        ).wait_recv()

    sent_by_all, sent_by, sent_home = [], ([], []), []

    def send_away(source, target, send_sem, recv_sem, device, sent_list, alike):
        pltpu.make_async_remote_copy(
            source, target, send_sem, recv_sem, device_id=device, device_id_type=MESH
        ).start()
        sent_list.append((alike, send_sem))

    def left(alike, sem):
        ref = alike[0].at[alike[1]]
        pltpu.make_async_remote_copy(
            ref, ref, sem, dr_sem, device_id=at(z, x, 1 - c, y), device_id_type=MESH
        ).wait_send()

    barrier = pltpu.get_barrier_semaphore()

    def enter(device):
        pl.semaphore_signal(barrier, inc=1, device_id=device, device_id_type=MESH)

    wide = pl.multiple_of((ep // 32) * 128, 128)
    sources = list(hbm)
    sources[15] = ids_h.at[:, pl.ds(wide, 128)]
    loads = [
        pltpu.make_async_copy(source, target, load.at[LOAD_GROUP[i]])
        for i, (source, target) in enumerate(zip(sources, scratch[:20]))
    ]
    @pl.when(c == 1)
    def _():
        for d in FAR_FIRST:
            enter(at(turn(z, d, NZ), x, 1, y))

    for i in (0, 1, 2):
        loads[i].start()
    for d in range(1, NY):
        enter(at(z, x, 0, turn(y, d, NY)))
    for dx, dy in PLANE:
        if dx or dy:
            enter(at(z, turn(x, dx, NX), 1, turn(y, dy, NY)))
    enter(at(z, x, 1 - c, y))
    near_count = 2 * (NY - 1) + 1
    far_count = (NZ - 1) + 2 * (NX * NY - 1) + 1

    for i in (3, 4, 5, 6, 7, 11, 12, 8, 9, 10, 13, 14, 15, 16, 17, 18, 19):
        loads[i].start()

    loads[0].wait()
    loads[1].wait()
    tokens = tok[...].astype(F32)
    normed_in = rms(tokens, row_of(gain[...]))
    loads[2].wait()
    u = dot(normed_in, inw[...]).astype(BF16).astype(F32)

    rows = SEQ * GROUPS
    own_group = iota((rows, CHANNELS), 0) % GROUPS == iota((rows, CHANNELS), 1) // 16
    spread = jnp.broadcast_to(u[:, None, :], (SEQ, GROUPS, CHANNELS)).reshape(rows, CHANNELS)
    spread = jnp.where(own_group, spread, 0.0).astype(BF16)
    for i in (3, 4, 5, 6, 7):
        loads[i].wait()
    group_row = iota((GROUPS, STATE), 0)
    log_step = jnp.zeros((GROUPS, STATE), F32)
    for g in range(GROUPS):
        log_step = jnp.where(group_row == g, steps[g], log_step)
    step_size = jnp.exp(log_step)
    lam_real, frequency = -decay[...], freq[...]
    magnitude = jnp.exp(lam_real * step_size)
    turned = frequency * step_size
    bar_real = magnitude * jnp.cos(turned)
    bar_imag = magnitude * jnp.sin(turned)
    denom = lam_real * lam_real + frequency * frequency
    minus_one = bar_real - 1.0
    factor_real = (minus_one * lam_real + bar_imag * frequency) / denom
    factor_imag = (bar_imag * lam_real - minus_one * frequency) / denom

    def per_row(v):
        return jnp.broadcast_to(v[None], (SEQ, GROUPS, STATE)).reshape(rows, STATE)

    def drive(ref):
        high, low = split(ref[...].reshape(CHANNELS, STATE))
        return dot(spread, high) + dot(spread, low)

    drive_r, drive_i = drive(inr), drive(ini)
    bar_real, bar_imag = per_row(bar_real), per_row(bar_imag)
    factor_real, factor_imag = per_row(factor_real), per_row(factor_imag)
    loads[11].wait()
    loads[12].wait()
    state_r, state_i = st_r[...].reshape(rows, STATE), st_i[...].reshape(rows, STATE)
    new_r = (bar_real * state_r - bar_imag * state_i) + (factor_real * drive_r - factor_imag * drive_i)
    new_i = (bar_real * state_i + bar_imag * state_r) + (factor_real * drive_i + factor_imag * drive_r)
    newr_o[...] = new_r.reshape(SEQ, GROUPS, STATE)
    newi_o[...] = new_i.reshape(SEQ, GROUPS, STATE)

    for i in (8, 9, 10):
        loads[i].wait()

    def read(values, ref):
        high, low = split(values)
        ref_high, ref_low = split(ref[...].reshape(CHANNELS, STATE))
        return dot_t(high, ref_high) + dot_t(high, ref_low) + dot_t(low, ref_high)

    readout = jnp.where(own_group, read(new_r, outr) - read(new_i, outi), 0.0)
    readout = readout.reshape(SEQ, GROUPS, CHANNELS).sum(axis=1)
    readout = readout + row_of(skip[...]) * u
    activated = jax.nn.gelu(readout).astype(BF16)
    loads[13].wait()
    delta[y] = dot(activated, outw[...]).astype(BF16)

    @pl.when(c == 0)
    def _():
        pl.semaphore_wait(barrier, near_count)
        pl.semaphore_signal(near_sem, inc=1, device_id=at(z, x, 1, y), device_id_type=MESH)

    @pl.when(c == 1)
    def _():
        pl.semaphore_wait(near_sem, 1)

    delta_copies = [
        pltpu.make_async_remote_copy(
            delta.at[y], delta.at[y], D_SENT, dr_sem,
            device_id=at(z, x, c, turn(y, d, NY)), device_id_type=MESH,
        )
        for d in range(1, NY)
    ]
    for copy in delta_copies:
        copy.start()

    for i in (14, 15, 16):
        loads[i].wait()
    first = (ep % 32) * SEQ
    names = [[ids[k, first + s] for k in range(2)] for s in range(SEQ)]
    weights = [[rw[k, s] for k in range(2)] for s in range(SEQ)]

    def table(expert, slot, shape):
        taken = jnp.zeros(shape, I32)
        picks, scales = [], []
        for s in range(SEQ):
            routes = [expert == names[s][k] for k in range(2)]
            named = routes[0] | routes[1]
            here = named & (taken == slot)
            picks.append(jnp.where(here, 1.0, 0.0))
            scale = jnp.where(routes[0], weights[s][0], 0.0) + jnp.where(routes[1], weights[s][1], 0.0)
            scales.append(jnp.where(here, scale, 0.0))
            taken = taken + jnp.where(named, 1, 0)
        return picks, scales

    pick_row = iota((16, QUARTER), 0)
    picks, _ = table(pick_row // 2, pick_row % 2, (16, QUARTER))
    ffn_gain = row_of(fgain[...])

    landed(delta.at[0 : NY - 1], dr_sem)
    total = tokens
    for i in range(NY):
        total = total + delta[i].astype(F32)
    hidden_state = total.astype(BF16).astype(F32)
    hid32[...] = hidden_state
    norm32[...] = rms(hidden_state, ffn_gain).astype(F32)
    lanes = pl.ds(pl.multiple_of(y * QUARTER, QUARTER), QUARTER)
    own = norm32[:, lanes]
    chosen = picks[0] * own[0:1, :]
    for s in range(1, SEQ):
        chosen = chosen + picks[s] * own[s : s + 1, :]
    pick32[...] = chosen
    for e in range(8):
        pick[e] = pick32[2 * e : 2 * e + 2, :].astype(BF16)

    @pl.when(c == 1)
    def _():
        pl.semaphore_wait(barrier, far_count)
        pl.semaphore_signal(far_sem, inc=1, device_id=at(z, x, 0, y), device_id_type=MESH)

    @pl.when(c == 0)
    def _():
        pl.semaphore_wait(far_sem, 1)

    for d in FAR_FIRST:
        to = turn(z, d, NZ)
        send_away(pick.at[to // 2], zin.at[z, c], Z_SENT, zr_sem.at[chunk_of(z)], at(to, x, 1, y), sent_by_all, (pick, 0))
    own_slots = (pick.at[z // 2], zin.at[z, c])

    @pl.when(c == 1)
    def _():
        pltpu.make_async_copy(*own_slots, zr_sem.at[chunk_of(z)]).start()

    @pl.when(c == 0)
    def _():
        send_away(*own_slots, Z_SENT, zr_sem.at[chunk_of(z)], at(z, x, 1, y), sent_by[0], (pick, 0))

    def take_chunk(k):
        low, high = CHUNKS[k]
        block = 2 * (high - low)
        landed(zin.at[low:high], zr_sem.at[k])
        for core in range(NC):
            for i in range(high - low):
                row = core * block + 2 * i
                sum32[row : row + 2, :] = zin[low + i, core].astype(F32)
        gat[k][y, x] = sum32[0 : 2 * block, :].astype(BF16)

    def pass_on(slots, alike, k, dx, dy):
        to = at(z, turn(x, dx, NX), 1, turn(y, dy, NY))
        send_away(slots, slots, G_SENT, gr_sem.at[k, dx], to, sent_by[1], alike)

    def gather_at_once(k):
        for dx, dy in reversed(PLANE):
            if dx or dy:
                pass_on(gat[k].at[y, x], (gat[k], (0, 0)), k, dx, dy)

    def gather_along_y(k):
        for dy in (2, 1, 3):
            pass_on(gat[k].at[y, x], (gat[k], (0, 0)), k, 0, dy)

    def gather_along_x(k):
        spread_chunk(k, (0,))
        for dx in (2, 1, 3):
            pass_on(gat[k].at[:, x], (gat[k], (slice(None), 0)), k, dx, 0)

    def spread_chunk(k, distances):
        for dx in distances:
            rows_x = turn(x, NX - dx, NX)
            landed(gat[k].at[(0 if dx else 1) : NY, rows_x], gr_sem.at[k, dx])
            slots = gat[k].at[:, rows_x]
            send_away(slots, slots, F_SENT, fr_sem.at[k], at(z, x, 0, y), sent_by[1], (gat[k], (slice(None), 0)))

    def up_chunk(k):
        @pl.when(c == 0)
        def _():
            landed(gat[k], fr_sem.at[k])

        rows = hid[k].shape[0]
        gate_pre = jnp.zeros((rows, HID), F32)
        up_pre = jnp.zeros((rows, HID), F32)
        for q in range(NY):
            block = gat[k][q].reshape(rows, QUARTER)
            gate_pre = gate_pre + dot(block, gw[q * QUARTER : (q + 1) * QUARTER, :])
            up_pre = up_pre + dot(block, uw[q * QUARTER : (q + 1) * QUARTER, :])
        units = pl.ds(pl.multiple_of(y * HID, HID), HID)
        hid[k][:, units] = (jax.nn.silu(gate_pre) * up_pre).astype(BF16)
        own_units = hid[k].at[:, units]
        for d in (2, 1, 3):
            to = at(z, x, c, turn(y, d, NY))
            send_away(own_units, own_units, H_SENT, hr_sem.at[k], to, sent_by_all, (hid[k], (slice(None), slice(0, HID))))

    def down_chunk(k):
        landed(hid[k].at[:, 0 : (NY - 1) * HID], hr_sem.at[k])
        send[k][...] = dot(hid[k][...], dw[...]).astype(BF16).reshape(send[k].shape)
        for dx in (2, 1, 3):
            to = turn(x, dx, NX)
            slot = recv[k].at[2 * dx - 1 + c]
            send_away(send[k].at[to], slot, R_SENT, rr_sem.at[k], at(z, to, SUMS[k], y), sent_by_all, (send[k], 0))

        @pl.when(c != SUMS[k])
        def _():
            home = at(z, x, SUMS[k], y)
            kept = sent_by[1 - SUMS[k]]
            send_away(send[k].at[x], recv[k].at[0], R_SENT, rr_sem.at[k], home, kept, (send[k], 0))

    def home_chunk(k):
        landed(recv[k], rr_sem.at[k])
        total = send[k][x].astype(F32)
        for i in range(NC * NX - 1):
            total = total + recv[k][i].astype(F32)
        low, high = CHUNKS[k]
        block = 2 * (high - low)
        sum32[0 : 2 * block, :] = total
        for core in range(NC):
            for i in range(high - low):
                row = core * block + 2 * i
                back[k][i, core] = sum32[row : row + 2, :].astype(BF16)
        for i in range(high - low):
            home = low + i
            slots, other = back[k].at[i, 1 - SUMS[k]], at(home, x, 1 - SUMS[k], y)
            send_away(slots, zout.at[z], B_SENT, br_sem, other, sent_by[SUMS[k]], (pick, 0))

            @pl.when(z != home)
            def _():
                slots, same = back[k].at[i, SUMS[k]], at(home, x, SUMS[k], y)
                send_away(slots, zout.at[z], B_SENT, br_sem, same, sent_home, (pick, 0))

            @pl.when(z == home)
            def _():
                pltpu.make_async_copy(back[k].at[i, SUMS[k]], zout.at[z], br_sem).start()

    on_core_1 = pl.when(c == 1)

    @on_core_1
    def _():
        take_chunk(0)
        gather_at_once(0)
        take_chunk(1)
        gather_along_y(1)
        take_chunk(2)
        gather_along_y(2)
        spread_chunk(0, (0, 1, 3, 2))
        gather_along_x(1)
        gather_along_x(2)

    loads[17].wait()
    loads[18].wait()
    up_chunk(0)
    on_core_1(lambda: spread_chunk(1, (1, 3, 2)))
    loads[19].wait()
    down_chunk(0)
    on_core_1(lambda: spread_chunk(2, (1, 3, 2)))
    up_chunk(1)
    up_chunk(2)
    on_core_1(lambda: home_chunk(0))
    down_chunk(1)
    down_chunk(2)
    on_core_1(lambda: home_chunk(1))
    pl.when(c == SUMS[2])(lambda: home_chunk(2))

    back_row = iota((2 * NZ, QUARTER), 0)
    _, scales = table(back_row // 4, back_row % 2, (2 * NZ, QUARTER))
    landed(zout, br_sem)
    for p in range(NZ):
        out32[2 * p : 2 * p + 2, :] = zout[p].astype(F32)
    pieces = out32[...]
    routed = [jnp.sum(scales[s] * pieces, axis=0, keepdims=True) for s in range(SEQ)]
    mixed_o[...] = (hid32[:, lanes] + jnp.concatenate(routed, axis=0)).astype(BF16)

    for copy in delta_copies:
        copy.wait_send()
    for copy in sent_by_all:
        left(*copy)
    for core in range(NC):

        @pl.when(c == core)
        def _():
            for copy in sent_by[core]:
                left(*copy)

    for home, copy in enumerate(sent_home):

        @pl.when((c == SUMS[0 if home < 4 else 1 if home < 8 else 2]) & (z != home))
        def _():
            left(*copy)


def store_kernel(*refs):
    sources, targets, sem = refs[:3], refs[3:6], refs[6]
    copies = [pltpu.make_async_copy(s, t, sem.at[i]) for i, (s, t) in enumerate(zip(sources, targets))]
    for copy in copies:
        copy.start()
    for copy in copies:
        copy.wait()


def shards(*args):
    args = list(args)
    for i in (1, 14):
        args[i] = args[i].reshape(16, 128)
    args[10] = args[10].reshape(2, 128)
    for i in (6, 7):
        args[i] = args[i].transpose(0, 2, 1)
    args[15], args[16] = args[15].T, args[16].T
    held = []
    for i, arg in enumerate(args):
        if i in (5, 16):
            held.append(pltpu.SMEM(arg.shape, arg.dtype))
        elif i == 15:
            held.append(pltpu.SMEM((2, 128), arg.dtype))
        else:
            held.append(pltpu.VMEM(arg.shape, arg.dtype))
    dma = pltpu.SemaphoreType.DMA
    shapes = (((SEQ, QUARTER), BF16), ((SEQ, GROUPS, STATE), F32), ((SEQ, GROUPS, STATE), F32))
    scratch = held + [
        pltpu.VMEM((NY, SEQ, WIDTH), BF16),
        pltpu.VMEM((SEQ, WIDTH), F32),
        pltpu.VMEM((SEQ, WIDTH), F32),
        pltpu.VMEM((16, QUARTER), F32),
        pltpu.VMEM((8, 2, QUARTER), BF16),
        pltpu.VMEM((NZ, NC, 2, QUARTER), BF16),
        pltpu.VMEM((32, QUARTER), F32),
        pltpu.VMEM((NZ, 2, QUARTER), BF16),
        pltpu.VMEM((2 * NZ, QUARTER), F32),
        dma((9,)), dma((7,)),
        dma, dma((3,)), dma((3, NX)), dma((3,)), dma((3,)), dma((3,)), dma,
        pltpu.SemaphoreType.REGULAR,
        pltpu.SemaphoreType.REGULAR,
    ]
    for low, high in CHUNKS:
        block = 2 * NC * (high - low)
        scratch += [
            pltpu.VMEM((NY, NX, block, QUARTER), BF16),
            pltpu.VMEM((NX * block, NY * HID), BF16),
            pltpu.VMEM((NX, block, QUARTER), BF16),
            pltpu.VMEM((NC * NX - 1, block, QUARTER), BF16),
            pltpu.VMEM((high - low, NC, 2, QUARTER), BF16),
        ]
    anywhere = pl.BlockSpec(memory_space=pl.ANY)
    near = pl.BlockSpec(memory_space=pltpu.VMEM)
    results = pl.pallas_call(
        kernel,
        out_shape=tuple(pltpu.VMEM(*shape) for shape in shapes),
        in_specs=[anywhere] * 20,
        out_specs=(near,) * 3,
        scratch_shapes=scratch,
        compiler_params=pltpu.CompilerParams(
            collective_id=0, has_side_effects=True, vmem_limit_bytes=VMEM_LIMIT
        ),
    )(*args)
    return pl.pallas_call(
        store_kernel,
        out_shape=tuple(jax.ShapeDtypeStruct(*shape) for shape in shapes),
        in_specs=[anywhere] * 3,
        out_specs=(anywhere,) * 3,
        scratch_shapes=[dma((3,))],
        compiler_params=pltpu.CompilerParams(vmem_limit_bytes=VMEM_LIMIT),
    )(*[pltpu.with_memory_space_constraint(r, pltpu.VMEM) for r in results])


def solution(mesh):
    in_specs = (
        P("ep", None), P(), P(None, "tp"), P("tp", None), P("tp", None), P("tp"),
        P("tp", None, None), P("tp", None, None), P("tp", None, None), P("tp", None, None), P("tp"),
        P("ep", "tp", None), P("ep", "tp", None), P("tp", None), P(), P(), P("ep", None),
        P(None, ("ep", "tp")), P(None, ("ep", "tp")), P("ep", "tp"),
    )
    out_specs = (P("ep", "tp"), P("ep", "tp", None), P("ep", "tp", None))
    return jax.shard_map(shards, mesh=mesh, in_specs=in_specs, out_specs=out_specs, check_vma=False)
```

```python
import jax
import jax.numpy as jnp
from jax import lax
from jax.experimental import pallas as pl
from jax.experimental.pallas import tpu as pltpu
from jax.sharding import PartitionSpec as P

EPS = 1e-06
F32, BF16, I32 = jnp.float32, jnp.bfloat16, jnp.int32
MESH = pl.DeviceIdType.MESH
NX, NY, NC, NZ = 4, 4, 2, 16
SEQ, WIDTH, QUARTER = 4, 2048, 512
GROUPS, STATE, CHANNELS = 16, 64, 256
HID = 128
CHUNKS = ((0, 4), (4, 8), (8, 12), (12, 16))
X_FIRST = 3
SUMS = (1, 1, 1, 0)
FAR_FIRST = (8, 7, 9, 6, 10, 5, 11, 4, 12, 3, 13, 2, 14, 1, 15)
VMEM_LIMIT = 67043328 - 72 * 1024
LOAD_GROUP = (0, 0, 1, 2, 2, 2, 2, 2, 4, 4, 4, 3, 3, 5, 6, 6, 6, 7, 7, 8)
PLANE = sorted(
    [(dx, dy) for dx in range(NX) for dy in range(NY)],
    key=lambda d: min(d[0], NX - d[0]) + min(d[1], NY - d[1]),
)


def iota(shape, dim):
    return lax.broadcasted_iota(I32, shape, dim)


def dot(a, b):
    return jnp.dot(a, b, preferred_element_type=F32)


def dot_t(a, b):
    return lax.dot_general(a, b, (((1,), (1,)), ((), ())), preferred_element_type=F32)


def split(x):
    high = x.astype(BF16)
    return high, (x - high.astype(F32)).astype(BF16)


def row_of(block):
    block = block.astype(F32)
    return jnp.concatenate([block[i : i + 1, :] for i in range(block.shape[0])], axis=1)


def rms(floats, gain):
    scale = lax.rsqrt(jnp.mean(floats * floats, axis=-1, keepdims=True) + EPS)
    return (floats * scale * gain).astype(BF16)


def kernel(*refs):
    hbm, outs, scratch = refs[:20], refs[20:23], refs[23:]
    (tok_h, gain_h, inw_h, decay_h, freq_h, step_h, inr_h, ini_h, outr_h, outi_h) = hbm[:10]
    (skip_h, str_h, sti_h, outw_h, fgain_h, ids_h, rw_h, gw_h, uw_h, dw_h) = hbm[10:]
    mixed_o, newr_o, newi_o = outs
    (tok, gain, inw, decay, freq, steps, inr, ini, outr, outi) = scratch[:10]
    (skip, st_r, st_i, outw, fgain, ids, rw, gw, uw, dw) = scratch[10:20]
    (delta, norm32, hid32, pick32, pick, zin) = scratch[20:26]
    sum32, zout, out32 = scratch[26:29]
    load, sent, dr_sem, zr_sem, gr_sem, fr_sem, hr_sem, rr_sem, br_sem, near_sem, far_sem = scratch[29:40]
    gat, hid, send, recv, back = (scratch[40 + i :: 5] for i in range(5))
    D_SENT, Z_SENT, G_SENT, F_SENT, H_SENT, R_SENT, B_SENT = (sent.at[i] for i in range(7))

    ep, y = lax.axis_index("ep"), lax.axis_index("tp")
    z, x, c = ep // 8, (ep // 2) % NX, ep % 2

    def at(zz, xx, cc, yy):
        return (zz * 8 + xx * 2 + cc, yy)

    def chunk_of(home):
        return home // 4

    def turn(a, d, n):
        return lax.rem(a + d, n)

    def landed(ref, sem):
        pltpu.make_async_remote_copy(
            ref, ref, D_SENT, sem, device_id=at(z, x, 1 - c, y), device_id_type=MESH
        ).wait_recv()

    sent_by_all, sent_by, sent_home = [], ([], []), []

    def send_away(source, target, send_sem, recv_sem, device, sent_list, alike):
        pltpu.make_async_remote_copy(
            source, target, send_sem, recv_sem, device_id=device, device_id_type=MESH
        ).start()
        sent_list.append((alike, send_sem))

    def left(alike, sem):
        ref = alike[0].at[alike[1]]
        pltpu.make_async_remote_copy(
            ref, ref, sem, dr_sem, device_id=at(z, x, 1 - c, y), device_id_type=MESH
        ).wait_send()

    barrier = pltpu.get_barrier_semaphore()

    def enter(device):
        pl.semaphore_signal(barrier, inc=1, device_id=device, device_id_type=MESH)

    wide = pl.multiple_of((ep // 32) * 128, 128)
    sources = list(hbm)
    sources[15] = ids_h.at[:, pl.ds(wide, 128)]
    loads = [
        pltpu.make_async_copy(source, target, load.at[LOAD_GROUP[i]])
        for i, (source, target) in enumerate(zip(sources, scratch[:20]))
    ]
    @pl.when(c == 1)
    def _():
        for d in FAR_FIRST:
            enter(at(turn(z, d, NZ), x, 1, y))

    for i in (0, 1, 2):
        loads[i].start()
    for d in range(1, NY):
        enter(at(z, x, 0, turn(y, d, NY)))
    for dx, dy in PLANE:
        if dx or dy:
            enter(at(z, turn(x, dx, NX), 1, turn(y, dy, NY)))
    enter(at(z, x, 1 - c, y))
    near_count = 2 * (NY - 1) + 1
    far_count = (NZ - 1) + 2 * (NX * NY - 1) + 1

    for i in (3, 4, 5, 6, 7, 11, 12, 8, 9, 10, 13, 14, 15, 16, 17, 18, 19):
        loads[i].start()

    loads[0].wait()
    loads[1].wait()
    tokens = tok[...].astype(F32)
    normed_in = rms(tokens, row_of(gain[...]))
    loads[2].wait()
    u = dot(normed_in, inw[...]).astype(BF16).astype(F32)

    rows = SEQ * GROUPS
    own_group = iota((rows, CHANNELS), 0) % GROUPS == iota((rows, CHANNELS), 1) // 16
    spread = jnp.broadcast_to(u[:, None, :], (SEQ, GROUPS, CHANNELS)).reshape(rows, CHANNELS)
    spread = jnp.where(own_group, spread, 0.0).astype(BF16)
    for i in (3, 4, 5, 6, 7):
        loads[i].wait()
    group_row = iota((GROUPS, STATE), 0)
    log_step = jnp.zeros((GROUPS, STATE), F32)
    for g in range(GROUPS):
        log_step = jnp.where(group_row == g, steps[g], log_step)
    step_size = jnp.exp(log_step)
    lam_real, frequency = -decay[...], freq[...]
    magnitude = jnp.exp(lam_real * step_size)
    turned = frequency * step_size
    bar_real = magnitude * jnp.cos(turned)
    bar_imag = magnitude * jnp.sin(turned)
    denom = lam_real * lam_real + frequency * frequency
    minus_one = bar_real - 1.0
    factor_real = (minus_one * lam_real + bar_imag * frequency) / denom
    factor_imag = (bar_imag * lam_real - minus_one * frequency) / denom

    def per_row(v):
        return jnp.broadcast_to(v[None], (SEQ, GROUPS, STATE)).reshape(rows, STATE)

    def drive(ref):
        high, low = split(ref[...].reshape(CHANNELS, STATE))
        return dot(spread, high) + dot(spread, low)

    drive_r, drive_i = drive(inr), drive(ini)
    bar_real, bar_imag = per_row(bar_real), per_row(bar_imag)
    factor_real, factor_imag = per_row(factor_real), per_row(factor_imag)
    loads[11].wait()
    loads[12].wait()
    state_r, state_i = st_r[...].reshape(rows, STATE), st_i[...].reshape(rows, STATE)
    new_r = (bar_real * state_r - bar_imag * state_i) + (factor_real * drive_r - factor_imag * drive_i)
    new_i = (bar_real * state_i + bar_imag * state_r) + (factor_real * drive_i + factor_imag * drive_r)
    newr_o[...] = new_r.reshape(SEQ, GROUPS, STATE)
    newi_o[...] = new_i.reshape(SEQ, GROUPS, STATE)

    for i in (8, 9, 10):
        loads[i].wait()

    def read(values, ref):
        high, low = split(values)
        ref_high, ref_low = split(ref[...].reshape(CHANNELS, STATE))
        return dot_t(high, ref_high) + dot_t(high, ref_low) + dot_t(low, ref_high)

    readout = jnp.where(own_group, read(new_r, outr) - read(new_i, outi), 0.0)
    readout = readout.reshape(SEQ, GROUPS, CHANNELS).sum(axis=1)
    readout = readout + row_of(skip[...]) * u
    activated = jax.nn.gelu(readout).astype(BF16)
    loads[13].wait()
    delta[y] = dot(activated, outw[...]).astype(BF16)

    @pl.when(c == 0)
    def _():
        pl.semaphore_wait(barrier, near_count)
        pl.semaphore_signal(near_sem, inc=1, device_id=at(z, x, 1, y), device_id_type=MESH)

    @pl.when(c == 1)
    def _():
        pl.semaphore_wait(near_sem, 1)

    delta_copies = [
        pltpu.make_async_remote_copy(
            delta.at[y], delta.at[y], D_SENT, dr_sem,
            device_id=at(z, x, c, turn(y, d, NY)), device_id_type=MESH,
        )
        for d in range(1, NY)
    ]
    for copy in delta_copies:
        copy.start()

    for i in (14, 15, 16):
        loads[i].wait()
    first = (ep % 32) * SEQ
    names = [[ids[k, first + s] for k in range(2)] for s in range(SEQ)]
    weights = [[rw[k, s] for k in range(2)] for s in range(SEQ)]

    def table(expert, slot, shape):
        taken = jnp.zeros(shape, I32)
        picks, scales = [], []
        for s in range(SEQ):
            routes = [expert == names[s][k] for k in range(2)]
            named = routes[0] | routes[1]
            here = named & (taken == slot)
            picks.append(jnp.where(here, 1.0, 0.0))
            scale = jnp.where(routes[0], weights[s][0], 0.0) + jnp.where(routes[1], weights[s][1], 0.0)
            scales.append(jnp.where(here, scale, 0.0))
            taken = taken + jnp.where(named, 1, 0)
        return picks, scales

    pick_row = iota((16, QUARTER), 0)
    picks, _ = table(pick_row // 2, pick_row % 2, (16, QUARTER))
    ffn_gain = row_of(fgain[...])

    landed(delta.at[0 : NY - 1], dr_sem)
    total = tokens
    for i in range(NY):
        total = total + delta[i].astype(F32)
    hidden_state = total.astype(BF16).astype(F32)
    hid32[...] = hidden_state
    norm32[...] = rms(hidden_state, ffn_gain).astype(F32)
    lanes = pl.ds(pl.multiple_of(y * QUARTER, QUARTER), QUARTER)
    own = norm32[:, lanes]
    chosen = picks[0] * own[0:1, :]
    for s in range(1, SEQ):
        chosen = chosen + picks[s] * own[s : s + 1, :]
    pick32[...] = chosen
    for e in range(8):
        pick[e] = pick32[2 * e : 2 * e + 2, :].astype(BF16)

    @pl.when(c == 1)
    def _():
        pl.semaphore_wait(barrier, far_count)
        pl.semaphore_signal(far_sem, inc=1, device_id=at(z, x, 0, y), device_id_type=MESH)

    @pl.when(c == 0)
    def _():
        pl.semaphore_wait(far_sem, 1)

    for d in FAR_FIRST:
        to = turn(z, d, NZ)
        send_away(pick.at[to // 2], zin.at[z, c], Z_SENT, zr_sem.at[chunk_of(z)], at(to, x, 1, y), sent_by_all, (pick, 0))
    own_slots = (pick.at[z // 2], zin.at[z, c])

    @pl.when(c == 1)
    def _():
        pltpu.make_async_copy(*own_slots, zr_sem.at[chunk_of(z)]).start()

    @pl.when(c == 0)
    def _():
        send_away(*own_slots, Z_SENT, zr_sem.at[chunk_of(z)], at(z, x, 1, y), sent_by[0], (pick, 0))

    def take_chunk(k):
        low, high = CHUNKS[k]
        block = 2 * (high - low)
        landed(zin.at[low:high], zr_sem.at[k])
        for core in range(NC):
            for i in range(high - low):
                row = core * block + 2 * i
                sum32[row : row + 2, :] = zin[low + i, core].astype(F32)
        gat[k][y, x] = sum32[0 : 2 * block, :].astype(BF16)

    def pass_on(slots, alike, k, sem, dx, dy):
        to = at(z, turn(x, dx, NX), 1, turn(y, dy, NY))
        send_away(slots, slots, G_SENT, gr_sem.at[k, sem], to, sent_by[1], (gat[k], alike))

    def line(k, distance):
        if k == X_FIRST:
            return gat[k].at[turn(y, NY - distance, NY), :]
        return gat[k].at[:, turn(x, NX - distance, NX)]

    def gather_at_once(k):
        for dx, dy in reversed(PLANE):
            if dx or dy:
                pass_on(gat[k].at[y, x], (0, 0), k, dx, dx, dy)

    def gather_first(k):
        for d in (2, 1, 3):
            dx, dy = (d, 0) if k == X_FIRST else (0, d)
            pass_on(gat[k].at[y, x], (0, 0), k, 0, dx, dy)

    def gather_second(k):
        spread_chunk(k, (0,))
        for d in (2, 1, 3):
            dx, dy = (0, d) if k == X_FIRST else (d, 0)
            pass_on(line(k, 0), (slice(None), 0), k, d, dx, dy)

    def spread_chunk(k, distances):
        for d in distances:
            landed(gat[k].at[0, (0 if d else 1) : NX], gr_sem.at[k, d])
            send_away(
                line(k, d), line(k, d), F_SENT, fr_sem.at[k], at(z, x, 0, y), sent_by[1], (gat[k], (slice(None), 0))
            )

    def up_chunk(k):
        @pl.when(c == 0)
        def _():
            landed(gat[k], fr_sem.at[k])

        rows = hid[k].shape[0]
        gate_pre = jnp.zeros((rows, HID), F32)
        up_pre = jnp.zeros((rows, HID), F32)
        for q in range(NY):
            block = gat[k][q].reshape(rows, QUARTER)
            gate_pre = gate_pre + dot(block, gw[q * QUARTER : (q + 1) * QUARTER, :])
            up_pre = up_pre + dot(block, uw[q * QUARTER : (q + 1) * QUARTER, :])
        units = pl.ds(pl.multiple_of(y * HID, HID), HID)
        hid[k][:, units] = (jax.nn.silu(gate_pre) * up_pre).astype(BF16)
        own_units = hid[k].at[:, units]
        for d in (2, 1, 3):
            to = at(z, x, c, turn(y, d, NY))
            send_away(own_units, own_units, H_SENT, hr_sem.at[k], to, sent_by_all, (hid[k], (slice(None), slice(0, HID))))

    def down_chunk(k):
        landed(hid[k].at[:, 0 : (NY - 1) * HID], hr_sem.at[k])
        send[k][...] = dot(hid[k][...], dw[...]).astype(BF16).reshape(send[k].shape)
        for dx in (2, 1, 3):
            to = turn(x, dx, NX)
            slot = recv[k].at[2 * dx - 1 + c]
            send_away(send[k].at[to], slot, R_SENT, rr_sem.at[k], at(z, to, SUMS[k], y), sent_by_all, (send[k], 0))

        @pl.when(c != SUMS[k])
        def _():
            home = at(z, x, SUMS[k], y)
            kept = sent_by[1 - SUMS[k]]
            send_away(send[k].at[x], recv[k].at[0], R_SENT, rr_sem.at[k], home, kept, (send[k], 0))

    def home_chunk(k):
        landed(recv[k], rr_sem.at[k])
        total = send[k][x].astype(F32)
        for i in range(NC * NX - 1):
            total = total + recv[k][i].astype(F32)
        low, high = CHUNKS[k]
        block = 2 * (high - low)
        sum32[0 : 2 * block, :] = total
        for core in range(NC):
            for i in range(high - low):
                row = core * block + 2 * i
                back[k][i, core] = sum32[row : row + 2, :].astype(BF16)
        for i in range(high - low):
            home = low + i
            slots, other = back[k].at[i, 1 - SUMS[k]], at(home, x, 1 - SUMS[k], y)
            send_away(slots, zout.at[z], B_SENT, br_sem, other, sent_by[SUMS[k]], (pick, 0))

            @pl.when(z != home)
            def _():
                slots, same = back[k].at[i, SUMS[k]], at(home, x, SUMS[k], y)
                send_away(slots, zout.at[z], B_SENT, br_sem, same, sent_home, (pick, 0))

            @pl.when(z == home)
            def _():
                pltpu.make_async_copy(back[k].at[i, SUMS[k]], zout.at[z], br_sem).start()

    on_core_1 = pl.when(c == 1)

    @on_core_1
    def _():
        take_chunk(0)
        gather_at_once(0)
        for k in (1, 2, 3):
            take_chunk(k)
            gather_first(k)
        spread_chunk(0, (0, 1, 3, 2))
        gather_second(1)
        gather_second(2)

    loads[17].wait()
    loads[18].wait()
    up_chunk(0)

    @on_core_1
    def _():
        gather_second(3)
        spread_chunk(1, (1, 3, 2))

    loads[19].wait()
    down_chunk(0)
    on_core_1(lambda: spread_chunk(2, (1, 3, 2)))
    up_chunk(1)
    up_chunk(2)
    on_core_1(lambda: spread_chunk(3, (1, 3, 2)))
    up_chunk(3)
    on_core_1(lambda: home_chunk(0))
    down_chunk(1)
    down_chunk(2)
    down_chunk(3)
    on_core_1(lambda: home_chunk(1))
    on_core_1(lambda: home_chunk(2))
    pl.when(c == SUMS[3])(lambda: home_chunk(3))

    back_row = iota((2 * NZ, QUARTER), 0)
    _, scales = table(back_row // 4, back_row % 2, (2 * NZ, QUARTER))
    landed(zout, br_sem)
    for p in range(NZ):
        out32[2 * p : 2 * p + 2, :] = zout[p].astype(F32)
    pieces = out32[...]
    routed = [jnp.sum(scales[s] * pieces, axis=0, keepdims=True) for s in range(SEQ)]
    mixed_o[...] = (hid32[:, lanes] + jnp.concatenate(routed, axis=0)).astype(BF16)

    for copy in delta_copies:
        copy.wait_send()
    for copy in sent_by_all:
        left(*copy)
    for core in range(NC):

        @pl.when(c == core)
        def _():
            for copy in sent_by[core]:
                left(*copy)

    for home, copy in enumerate(sent_home):

        @pl.when((c == SUMS[home // 4]) & (z != home))
        def _():
            left(*copy)


def store_kernel(*refs):
    sources, targets, sem = refs[:3], refs[3:6], refs[6]
    copies = [pltpu.make_async_copy(s, t, sem.at[i]) for i, (s, t) in enumerate(zip(sources, targets))]
    for copy in copies:
        copy.start()
    for copy in copies:
        copy.wait()


def shards(*args):
    args = list(args)
    for i in (1, 14):
        args[i] = args[i].reshape(16, 128)
    args[10] = args[10].reshape(2, 128)
    for i in (6, 7):
        args[i] = args[i].transpose(0, 2, 1)
    args[15], args[16] = args[15].T, args[16].T
    held = []
    for i, arg in enumerate(args):
        if i in (5, 16):
            held.append(pltpu.SMEM(arg.shape, arg.dtype))
        elif i == 15:
            held.append(pltpu.SMEM((2, 128), arg.dtype))
        else:
            held.append(pltpu.VMEM(arg.shape, arg.dtype))
    dma = pltpu.SemaphoreType.DMA
    shapes = (((SEQ, QUARTER), BF16), ((SEQ, GROUPS, STATE), F32), ((SEQ, GROUPS, STATE), F32))
    scratch = held + [
        pltpu.VMEM((NY, SEQ, WIDTH), BF16),
        pltpu.VMEM((SEQ, WIDTH), F32),
        pltpu.VMEM((SEQ, WIDTH), F32),
        pltpu.VMEM((16, QUARTER), F32),
        pltpu.VMEM((8, 2, QUARTER), BF16),
        pltpu.VMEM((NZ, NC, 2, QUARTER), BF16),
        pltpu.VMEM((16, QUARTER), F32),
        pltpu.VMEM((NZ, 2, QUARTER), BF16),
        pltpu.VMEM((2 * NZ, QUARTER), F32),
        dma((9,)), dma((7,)),
        dma, dma((4,)), dma((4, NX)), dma((4,)), dma((4,)), dma((4,)), dma,
        pltpu.SemaphoreType.REGULAR,
        pltpu.SemaphoreType.REGULAR,
    ]
    for low, high in CHUNKS:
        block = 2 * NC * (high - low)
        scratch += [
            pltpu.VMEM((NY, NX, block, QUARTER), BF16),
            pltpu.VMEM((NX * block, NY * HID), BF16),
            pltpu.VMEM((NX, block, QUARTER), BF16),
            pltpu.VMEM((NC * NX - 1, block, QUARTER), BF16),
            pltpu.VMEM((high - low, NC, 2, QUARTER), BF16),
        ]
    anywhere = pl.BlockSpec(memory_space=pl.ANY)
    near = pl.BlockSpec(memory_space=pltpu.VMEM)
    results = pl.pallas_call(
        kernel,
        out_shape=tuple(pltpu.VMEM(*shape) for shape in shapes),
        in_specs=[anywhere] * 20,
        out_specs=(near,) * 3,
        scratch_shapes=scratch,
        compiler_params=pltpu.CompilerParams(
            collective_id=0, has_side_effects=True, vmem_limit_bytes=VMEM_LIMIT
        ),
    )(*args)
    return pl.pallas_call(
        store_kernel,
        out_shape=tuple(jax.ShapeDtypeStruct(*shape) for shape in shapes),
        in_specs=[anywhere] * 3,
        out_specs=(anywhere,) * 3,
        scratch_shapes=[dma((3,))],
        compiler_params=pltpu.CompilerParams(vmem_limit_bytes=VMEM_LIMIT),
    )(*[pltpu.with_memory_space_constraint(r, pltpu.VMEM) for r in results])


def solution(mesh):
    in_specs = (
        P("ep", None), P(), P(None, "tp"), P("tp", None), P("tp", None), P("tp"),
        P("tp", None, None), P("tp", None, None), P("tp", None, None), P("tp", None, None), P("tp"),
        P("ep", "tp", None), P("ep", "tp", None), P("tp", None), P(), P(), P("ep", None),
        P(None, ("ep", "tp")), P(None, ("ep", "tp")), P("ep", "tp"),
    )
    out_specs = (P("ep", "tp"), P("ep", "tp", None), P("ep", "tp", None))
    return jax.shard_map(shards, mesh=mesh, in_specs=in_specs, out_specs=out_specs, check_vma=False)
```

```python
import jax
import jax.numpy as jnp
from jax import lax
from jax.experimental import pallas as pl
from jax.experimental.pallas import tpu as pltpu
from jax.sharding import PartitionSpec as P

EPS = 1e-06
F32, BF16, I32 = jnp.float32, jnp.bfloat16, jnp.int32
MESH = pl.DeviceIdType.MESH
NX, NY, NC, NZ = 4, 4, 2, 16
SEQ, WIDTH, QUARTER = 4, 2048, 512
GROUPS, STATE, CHANNELS = 16, 64, 256
HID = 128
CHUNKS = ((0, 4), (4, 8), (8, 12), (12, 16))
X_FIRST = 3
SUMS = (1, 1, 1, 0)
FAR_FIRST = (8, 7, 9, 6, 10, 5, 11, 4, 12, 3, 13, 2, 14, 1, 15)
VMEM_LIMIT = 67043328 - 72 * 1024
LOAD_GROUP = (0, 0, 1, 2, 2, 2, 2, 2, 4, 4, 4, 3, 3, 5, 6, 6, 6, 7, 7, 8)
PLANE = sorted(
    [(dx, dy) for dx in range(NX) for dy in range(NY)],
    key=lambda d: min(d[0], NX - d[0]) + min(d[1], NY - d[1]),
)


def iota(shape, dim):
    return lax.broadcasted_iota(I32, shape, dim)


def dot(a, b):
    return jnp.dot(a, b, preferred_element_type=F32)


def dot_t(a, b):
    return lax.dot_general(a, b, (((1,), (1,)), ((), ())), preferred_element_type=F32)


def split(x):
    high = x.astype(BF16)
    return high, (x - high.astype(F32)).astype(BF16)


def row_of(block):
    block = block.astype(F32)
    return jnp.concatenate([block[i : i + 1, :] for i in range(block.shape[0])], axis=1)


def rms(floats, gain):
    scale = lax.rsqrt(jnp.mean(floats * floats, axis=-1, keepdims=True) + EPS)
    return (floats * scale * gain).astype(BF16)


def kernel(*refs):
    hbm, outs, scratch = refs[:20], refs[20:23], refs[23:]
    (tok_h, gain_h, inw_h, decay_h, freq_h, step_h, inr_h, ini_h, outr_h, outi_h) = hbm[:10]
    (skip_h, str_h, sti_h, outw_h, fgain_h, ids_h, rw_h, gw_h, uw_h, dw_h) = hbm[10:]
    mixed_o, newr_o, newi_o = outs
    (tok, gain, inw, decay, freq, steps, inr, ini, outr, outi) = scratch[:10]
    (skip, st_r, st_i, outw, fgain, ids, rw, gw, uw, dw) = scratch[10:20]
    (delta, norm32, hid32, pick32, pick, zin) = scratch[20:26]
    sum32, zout, out32 = scratch[26:29]
    load, sent, dr_sem, zr_sem, gr_sem, fr_sem, hr_sem, rr_sem, br_sem, near_sem, far_sem = scratch[29:40]
    gat, hid, send, recv, back = (scratch[40 + i :: 5] for i in range(5))
    D_SENT, Z_SENT, G_SENT, F_SENT, H_SENT, R_SENT, B_SENT = (sent.at[i] for i in range(7))

    ep, y = lax.axis_index("ep"), lax.axis_index("tp")
    z, x, c = ep // 8, (ep // 2) % NX, ep % 2

    def at(zz, xx, cc, yy):
        return (zz * 8 + xx * 2 + cc, yy)

    def chunk_of(home):
        return home // 4

    def turn(a, d, n):
        return lax.rem(a + d, n)

    def landed(ref, sem):
        pltpu.make_async_remote_copy(
            ref, ref, D_SENT, sem, device_id=at(z, x, 1 - c, y), device_id_type=MESH
        ).wait_recv()

    sent_by_all, sent_by, sent_home = [], ([], []), []

    def send_away(source, target, send_sem, recv_sem, device, sent_list, alike):
        pltpu.make_async_remote_copy(
            source, target, send_sem, recv_sem, device_id=device, device_id_type=MESH
        ).start()
        sent_list.append((alike, send_sem))

    def left(alike, sem):
        ref = alike[0].at[alike[1]]
        pltpu.make_async_remote_copy(
            ref, ref, sem, dr_sem, device_id=at(z, x, 1 - c, y), device_id_type=MESH
        ).wait_send()

    barrier = pltpu.get_barrier_semaphore()

    def enter(device):
        pl.semaphore_signal(barrier, inc=1, device_id=device, device_id_type=MESH)

    wide = pl.multiple_of((ep // 32) * 128, 128)
    sources = list(hbm)
    sources[15] = ids_h.at[:, pl.ds(wide, 128)]
    loads = [
        pltpu.make_async_copy(source, target, load.at[LOAD_GROUP[i]])
        for i, (source, target) in enumerate(zip(sources, scratch[:20]))
    ]
    @pl.when(c == 1)
    def _():
        for d in FAR_FIRST:
            enter(at(turn(z, d, NZ), x, 1, y))

    for i in (0, 1, 2):
        loads[i].start()
    for d in range(1, NY):
        enter(at(z, x, 0, turn(y, d, NY)))
    for dx, dy in PLANE:
        if dx or dy:
            enter(at(z, turn(x, dx, NX), 1, turn(y, dy, NY)))
    enter(at(z, x, 1 - c, y))
    near_count = 2 * (NY - 1) + 1
    far_count = (NZ - 1) + 2 * (NX * NY - 1) + 1

    for i in (3, 4, 5, 6, 7, 11, 12, 8, 9, 10, 13, 14, 15, 16, 17, 18, 19):
        loads[i].start()

    loads[0].wait()
    loads[1].wait()
    tokens = tok[...].astype(F32)
    normed_in = rms(tokens, row_of(gain[...]))
    loads[2].wait()
    u = dot(normed_in, inw[...]).astype(BF16).astype(F32)

    rows = SEQ * GROUPS
    own_group = iota((rows, CHANNELS), 0) % GROUPS == iota((rows, CHANNELS), 1) // 16
    spread = jnp.broadcast_to(u[:, None, :], (SEQ, GROUPS, CHANNELS)).reshape(rows, CHANNELS)
    spread = jnp.where(own_group, spread, 0.0).astype(BF16)
    for i in (3, 4, 5, 6, 7):
        loads[i].wait()
    group_row = iota((GROUPS, STATE), 0)
    log_step = jnp.zeros((GROUPS, STATE), F32)
    for g in range(GROUPS):
        log_step = jnp.where(group_row == g, steps[g], log_step)
    step_size = jnp.exp(log_step)
    lam_real, frequency = -decay[...], freq[...]
    magnitude = jnp.exp(lam_real * step_size)
    turned = frequency * step_size
    bar_real = magnitude * jnp.cos(turned)
    bar_imag = magnitude * jnp.sin(turned)
    denom = lam_real * lam_real + frequency * frequency
    minus_one = bar_real - 1.0
    factor_real = (minus_one * lam_real + bar_imag * frequency) / denom
    factor_imag = (bar_imag * lam_real - minus_one * frequency) / denom

    def per_row(v):
        return jnp.broadcast_to(v[None], (SEQ, GROUPS, STATE)).reshape(rows, STATE)

    def drive(ref):
        high, low = split(ref[...].reshape(CHANNELS, STATE))
        return dot(spread, high) + dot(spread, low)

    drive_r, drive_i = drive(inr), drive(ini)
    bar_real, bar_imag = per_row(bar_real), per_row(bar_imag)
    factor_real, factor_imag = per_row(factor_real), per_row(factor_imag)
    loads[11].wait()
    loads[12].wait()
    state_r, state_i = st_r[...].reshape(rows, STATE), st_i[...].reshape(rows, STATE)
    new_r = (bar_real * state_r - bar_imag * state_i) + (factor_real * drive_r - factor_imag * drive_i)
    new_i = (bar_real * state_i + bar_imag * state_r) + (factor_real * drive_i + factor_imag * drive_r)
    newr_o[...] = new_r.reshape(SEQ, GROUPS, STATE)
    newi_o[...] = new_i.reshape(SEQ, GROUPS, STATE)

    for i in (8, 9, 10):
        loads[i].wait()

    def read(values, ref):
        high, low = split(values)
        ref_high, ref_low = split(ref[...].reshape(CHANNELS, STATE))
        return dot_t(high, ref_high) + dot_t(high, ref_low) + dot_t(low, ref_high)

    readout = jnp.where(own_group, read(new_r, outr) - read(new_i, outi), 0.0)
    readout = readout.reshape(SEQ, GROUPS, CHANNELS).sum(axis=1)
    readout = readout + row_of(skip[...]) * u
    activated = jax.nn.gelu(readout).astype(BF16)
    loads[13].wait()
    delta[y] = dot(activated, outw[...]).astype(BF16)

    @pl.when(c == 0)
    def _():
        pl.semaphore_wait(barrier, near_count)
        pl.semaphore_signal(near_sem, inc=1, device_id=at(z, x, 1, y), device_id_type=MESH)

    @pl.when(c == 1)
    def _():
        pl.semaphore_wait(near_sem, 1)

    delta_copies = [
        pltpu.make_async_remote_copy(
            delta.at[y], delta.at[y], D_SENT, dr_sem,
            device_id=at(z, x, c, turn(y, d, NY)), device_id_type=MESH,
        )
        for d in range(1, NY)
    ]
    for copy in delta_copies:
        copy.start()

    for i in (14, 15, 16):
        loads[i].wait()
    first = (ep % 32) * SEQ
    names = [[ids[k, first + s] for k in range(2)] for s in range(SEQ)]
    weights = [[rw[k, s] for k in range(2)] for s in range(SEQ)]

    def table(expert, slot, shape):
        taken = jnp.zeros(shape, I32)
        picks, scales = [], []
        for s in range(SEQ):
            routes = [expert == names[s][k] for k in range(2)]
            named = routes[0] | routes[1]
            here = named & (taken == slot)
            picks.append(jnp.where(here, 1.0, 0.0))
            scale = jnp.where(routes[0], weights[s][0], 0.0) + jnp.where(routes[1], weights[s][1], 0.0)
            scales.append(jnp.where(here, scale, 0.0))
            taken = taken + jnp.where(named, 1, 0)
        return picks, scales

    pick_row = iota((16, QUARTER), 0)
    picks, _ = table(pick_row // 2, pick_row % 2, (16, QUARTER))
    ffn_gain = row_of(fgain[...])

    landed(delta.at[0 : NY - 1], dr_sem)
    total = tokens
    for i in range(NY):
        total = total + delta[i].astype(F32)
    hidden_state = total.astype(BF16).astype(F32)
    hid32[...] = hidden_state
    norm32[...] = rms(hidden_state, ffn_gain).astype(F32)
    lanes = pl.ds(pl.multiple_of(y * QUARTER, QUARTER), QUARTER)
    own = norm32[:, lanes]
    chosen = picks[0] * own[0:1, :]
    for s in range(1, SEQ):
        chosen = chosen + picks[s] * own[s : s + 1, :]
    pick32[...] = chosen
    for e in range(8):
        pick[e] = pick32[2 * e : 2 * e + 2, :].astype(BF16)

    @pl.when(c == 1)
    def _():
        pl.semaphore_wait(barrier, far_count)
        pl.semaphore_signal(far_sem, inc=1, device_id=at(z, x, 0, y), device_id_type=MESH)

    @pl.when(c == 0)
    def _():
        pl.semaphore_wait(far_sem, 1)

    for d in FAR_FIRST:
        to = turn(z, d, NZ)
        send_away(pick.at[to // 2], zin.at[z, c], Z_SENT, zr_sem.at[chunk_of(z)], at(to, x, 1, y), sent_by_all, (pick, 0))
    own_slots = (pick.at[z // 2], zin.at[z, c])

    @pl.when(c == 1)
    def _():
        pltpu.make_async_copy(*own_slots, zr_sem.at[chunk_of(z)]).start()

    @pl.when(c == 0)
    def _():
        send_away(*own_slots, Z_SENT, zr_sem.at[chunk_of(z)], at(z, x, 1, y), sent_by[0], (pick, 0))

    def take_chunk(k):
        low, high = CHUNKS[k]
        block = 2 * (high - low)
        landed(zin.at[low:high], zr_sem.at[k])
        for core in range(NC):
            for i in range(high - low):
                row = core * block + 2 * i
                sum32[row : row + 2, :] = zin[low + i, core].astype(F32)
        gat[k][y, x] = sum32[0 : 2 * block, :].astype(BF16)

    def pass_on(slots, alike, k, sem, dx, dy):
        to = at(z, turn(x, dx, NX), 1, turn(y, dy, NY))
        send_away(slots, slots, G_SENT, gr_sem.at[k, sem], to, sent_by[1], (gat[k], alike))

    def line(k, distance):
        if k == X_FIRST:
            return gat[k].at[turn(y, NY - distance, NY), :]
        return gat[k].at[:, turn(x, NX - distance, NX)]

    def gather_at_once(k):
        for dx, dy in reversed(PLANE):
            if dx or dy:
                pass_on(gat[k].at[y, x], (0, 0), k, dx, dx, dy)

    def gather_first(k):
        for d in (2, 1, 3):
            dx, dy = (d, 0) if k == X_FIRST else (0, d)
            pass_on(gat[k].at[y, x], (0, 0), k, 0, dx, dy)

    def gather_second(k):
        spread_chunk(k, (0,))
        for d in (2, 1, 3):
            dx, dy = (0, d) if k == X_FIRST else (d, 0)
            pass_on(line(k, 0), (slice(None), 0), k, d, dx, dy)

    def spread_chunk(k, distances):
        for d in distances:
            landed(gat[k].at[0, (0 if d else 1) : NX], gr_sem.at[k, d])
            send_away(
                line(k, d), line(k, d), F_SENT, fr_sem.at[k], at(z, x, 0, y), sent_by[1], (gat[k], (slice(None), 0))
            )

    def up_chunk(k):
        @pl.when(c == 0)
        def _():
            landed(gat[k], fr_sem.at[k])

        rows = hid[k].shape[0]
        gate_pre = jnp.zeros((rows, HID), F32)
        up_pre = jnp.zeros((rows, HID), F32)
        for q in range(NY):
            block = gat[k][q].reshape(rows, QUARTER)
            gate_pre = gate_pre + dot(block, gw[q * QUARTER : (q + 1) * QUARTER, :])
            up_pre = up_pre + dot(block, uw[q * QUARTER : (q + 1) * QUARTER, :])
        units = pl.ds(pl.multiple_of(y * HID, HID), HID)
        hid[k][:, units] = (jax.nn.silu(gate_pre) * up_pre).astype(BF16)
        own_units = hid[k].at[:, units]
        for d in (2, 1, 3):
            to = at(z, x, c, turn(y, d, NY))
            send_away(own_units, own_units, H_SENT, hr_sem.at[k], to, sent_by_all, (hid[k], (slice(None), slice(0, HID))))

    def down_chunk(k):
        landed(hid[k].at[:, 0 : (NY - 1) * HID], hr_sem.at[k])
        send[k][...] = dot(hid[k][...], dw[...]).astype(BF16).reshape(send[k].shape)
        for dx in (2, 1, 3):
            to = turn(x, dx, NX)
            slot = recv[k].at[2 * dx - 1 + c]
            send_away(send[k].at[to], slot, R_SENT, rr_sem.at[k], at(z, to, SUMS[k], y), sent_by_all, (send[k], 0))

        @pl.when(c != SUMS[k])
        def _():
            home = at(z, x, SUMS[k], y)
            kept = sent_by[1 - SUMS[k]]
            send_away(send[k].at[x], recv[k].at[0], R_SENT, rr_sem.at[k], home, kept, (send[k], 0))

    def home_chunk(k):
        landed(recv[k], rr_sem.at[k])
        total = send[k][x].astype(F32)
        for i in range(NC * NX - 1):
            total = total + recv[k][i].astype(F32)
        low, high = CHUNKS[k]
        block = 2 * (high - low)
        sum32[0 : 2 * block, :] = total
        for core in range(NC):
            for i in range(high - low):
                row = core * block + 2 * i
                back[k][i, core] = sum32[row : row + 2, :].astype(BF16)
        for i in range(high - low):
            home = low + i
            slots, other = back[k].at[i, 1 - SUMS[k]], at(home, x, 1 - SUMS[k], y)
            send_away(slots, zout.at[z], B_SENT, br_sem, other, sent_by[SUMS[k]], (pick, 0))

            @pl.when(z != home)
            def _():
                slots, same = back[k].at[i, SUMS[k]], at(home, x, SUMS[k], y)
                send_away(slots, zout.at[z], B_SENT, br_sem, same, sent_home, (pick, 0))

            @pl.when(z == home)
            def _():
                pltpu.make_async_copy(back[k].at[i, SUMS[k]], zout.at[z], br_sem).start()

    on_core_1 = pl.when(c == 1)

    @on_core_1
    def _():
        take_chunk(0)
        gather_at_once(0)
        for k in (1, 2, 3):
            take_chunk(k)
            gather_first(k)
        spread_chunk(0, (0, 1, 3, 2))
        gather_second(1)
        gather_second(2)

    loads[17].wait()
    loads[18].wait()
    up_chunk(0)

    @on_core_1
    def _():
        spread_chunk(1, (1, 3, 2))
        gather_second(3)

    loads[19].wait()
    down_chunk(0)
    on_core_1(lambda: spread_chunk(2, (1, 3, 2)))
    up_chunk(1)
    up_chunk(2)
    on_core_1(lambda: spread_chunk(3, (1, 3, 2)))
    up_chunk(3)
    on_core_1(lambda: home_chunk(0))
    down_chunk(1)
    down_chunk(2)
    down_chunk(3)
    on_core_1(lambda: home_chunk(1))
    on_core_1(lambda: home_chunk(2))
    pl.when(c == SUMS[3])(lambda: home_chunk(3))

    back_row = iota((2 * NZ, QUARTER), 0)
    _, scales = table(back_row // 4, back_row % 2, (2 * NZ, QUARTER))
    landed(zout, br_sem)
    for p in range(NZ):
        out32[2 * p : 2 * p + 2, :] = zout[p].astype(F32)
    pieces = out32[...]
    routed = [jnp.sum(scales[s] * pieces, axis=0, keepdims=True) for s in range(SEQ)]
    mixed_o[...] = (hid32[:, lanes] + jnp.concatenate(routed, axis=0)).astype(BF16)

    for copy in delta_copies:
        copy.wait_send()
    for copy in sent_by_all:
        left(*copy)
    for core in range(NC):

        @pl.when(c == core)
        def _():
            for copy in sent_by[core]:
                left(*copy)

    for home, copy in enumerate(sent_home):

        @pl.when((c == SUMS[home // 4]) & (z != home))
        def _():
            left(*copy)


def store_kernel(*refs):
    sources, targets, sem = refs[:3], refs[3:6], refs[6]
    copies = [pltpu.make_async_copy(s, t, sem.at[i]) for i, (s, t) in enumerate(zip(sources, targets))]
    for copy in copies:
        copy.start()
    for copy in copies:
        copy.wait()


def shards(*args):
    args = list(args)
    for i in (1, 14):
        args[i] = args[i].reshape(16, 128)
    args[10] = args[10].reshape(2, 128)
    for i in (6, 7):
        args[i] = args[i].transpose(0, 2, 1)
    args[15], args[16] = args[15].T, args[16].T
    held = []
    for i, arg in enumerate(args):
        if i in (5, 16):
            held.append(pltpu.SMEM(arg.shape, arg.dtype))
        elif i == 15:
            held.append(pltpu.SMEM((2, 128), arg.dtype))
        else:
            held.append(pltpu.VMEM(arg.shape, arg.dtype))
    dma = pltpu.SemaphoreType.DMA
    shapes = (((SEQ, QUARTER), BF16), ((SEQ, GROUPS, STATE), F32), ((SEQ, GROUPS, STATE), F32))
    scratch = held + [
        pltpu.VMEM((NY, SEQ, WIDTH), BF16),
        pltpu.VMEM((SEQ, WIDTH), F32),
        pltpu.VMEM((SEQ, WIDTH), F32),
        pltpu.VMEM((16, QUARTER), F32),
        pltpu.VMEM((8, 2, QUARTER), BF16),
        pltpu.VMEM((NZ, NC, 2, QUARTER), BF16),
        pltpu.VMEM((16, QUARTER), F32),
        pltpu.VMEM((NZ, 2, QUARTER), BF16),
        pltpu.VMEM((2 * NZ, QUARTER), F32),
        dma((9,)), dma((7,)),
        dma, dma((4,)), dma((4, NX)), dma((4,)), dma((4,)), dma((4,)), dma,
        pltpu.SemaphoreType.REGULAR,
        pltpu.SemaphoreType.REGULAR,
    ]
    for low, high in CHUNKS:
        block = 2 * NC * (high - low)
        scratch += [
            pltpu.VMEM((NY, NX, block, QUARTER), BF16),
            pltpu.VMEM((NX * block, NY * HID), BF16),
            pltpu.VMEM((NX, block, QUARTER), BF16),
            pltpu.VMEM((NC * NX - 1, block, QUARTER), BF16),
            pltpu.VMEM((high - low, NC, 2, QUARTER), BF16),
        ]
    anywhere = pl.BlockSpec(memory_space=pl.ANY)
    near = pl.BlockSpec(memory_space=pltpu.VMEM)
    results = pl.pallas_call(
        kernel,
        out_shape=tuple(pltpu.VMEM(*shape) for shape in shapes),
        in_specs=[anywhere] * 20,
        out_specs=(near,) * 3,
        scratch_shapes=scratch,
        compiler_params=pltpu.CompilerParams(
            collective_id=0, has_side_effects=True, vmem_limit_bytes=VMEM_LIMIT
        ),
    )(*args)
    return pl.pallas_call(
        store_kernel,
        out_shape=tuple(jax.ShapeDtypeStruct(*shape) for shape in shapes),
        in_specs=[anywhere] * 3,
        out_specs=(anywhere,) * 3,
        scratch_shapes=[dma((3,))],
        compiler_params=pltpu.CompilerParams(vmem_limit_bytes=VMEM_LIMIT),
    )(*[pltpu.with_memory_space_constraint(r, pltpu.VMEM) for r in results])


def solution(mesh):
    in_specs = (
        P("ep", None), P(), P(None, "tp"), P("tp", None), P("tp", None), P("tp"),
        P("tp", None, None), P("tp", None, None), P("tp", None, None), P("tp", None, None), P("tp"),
        P("ep", "tp", None), P("ep", "tp", None), P("tp", None), P(), P(), P("ep", None),
        P(None, ("ep", "tp")), P(None, ("ep", "tp")), P("ep", "tp"),
    )
    out_specs = (P("ep", "tp"), P("ep", "tp", None), P("ep", "tp", None))
    return jax.shard_map(shards, mesh=mesh, in_specs=in_specs, out_specs=out_specs, check_vma=False)
```

```python
import jax
import jax.numpy as jnp
from jax import lax
from jax.experimental import pallas as pl
from jax.experimental.pallas import tpu as pltpu
from jax.sharding import PartitionSpec as P

EPS = 1e-06
F32, BF16, I32 = jnp.float32, jnp.bfloat16, jnp.int32
MESH = pl.DeviceIdType.MESH
NX, NY, NC, NZ = 4, 4, 2, 16
SEQ, WIDTH, QUARTER = 4, 2048, 512
GROUPS, STATE, CHANNELS = 16, 64, 256
HID = 128
CHUNKS = ((0, 4), (4, 8), (8, 12), (12, 16))
X_FIRST = 3
SUMS = (1, 1, 1, 0)
FAR_FIRST = (8, 7, 9, 6, 10, 5, 11, 4, 12, 3, 13, 2, 14, 1, 15)
VMEM_LIMIT = 67043328 - 72 * 1024
LOAD_GROUP = (0, 0, 1, 2, 2, 2, 2, 2, 4, 4, 4, 3, 3, 5, 6, 6, 6, 7, 7, 8)
PLANE = sorted(
    [(dx, dy) for dx in range(NX) for dy in range(NY)],
    key=lambda d: min(d[0], NX - d[0]) + min(d[1], NY - d[1]),
)


def iota(shape, dim):
    return lax.broadcasted_iota(I32, shape, dim)


def dot(a, b):
    return jnp.dot(a, b, preferred_element_type=F32)


def dot_t(a, b):
    return lax.dot_general(a, b, (((1,), (1,)), ((), ())), preferred_element_type=F32)


def split(x):
    high = x.astype(BF16)
    return high, (x - high.astype(F32)).astype(BF16)


def row_of(block):
    block = block.astype(F32)
    return jnp.concatenate([block[i : i + 1, :] for i in range(block.shape[0])], axis=1)


def rms(floats, gain):
    scale = lax.rsqrt(jnp.mean(floats * floats, axis=-1, keepdims=True) + EPS)
    return (floats * scale * gain).astype(BF16)


def kernel(*refs):
    hbm, outs, scratch = refs[:20], refs[20:23], refs[23:]
    (tok_h, gain_h, inw_h, decay_h, freq_h, step_h, inr_h, ini_h, outr_h, outi_h) = hbm[:10]
    (skip_h, str_h, sti_h, outw_h, fgain_h, ids_h, rw_h, gw_h, uw_h, dw_h) = hbm[10:]
    mixed_o, newr_o, newi_o = outs
    (tok, gain, inw, decay, freq, steps, inr, ini, outr, outi) = scratch[:10]
    (skip, st_r, st_i, outw, fgain, ids, rw, gw, uw, dw) = scratch[10:20]
    (delta, norm32, hid32, pick32, pick, zin) = scratch[20:26]
    sum32, zout, out32 = scratch[26:29]
    load, sent, dr_sem, zr_sem, gr_sem, fr_sem, hr_sem, rr_sem, br_sem, near_sem, far_sem = scratch[29:40]
    gat, hid, send, recv, back = (scratch[40 + i :: 5] for i in range(5))
    D_SENT = Z_SENT = G_SENT = F_SENT = H_SENT = R_SENT = B_SENT = sent

    ep, y = lax.axis_index("ep"), lax.axis_index("tp")
    z, x, c = ep // 8, (ep // 2) % NX, ep % 2

    def at(zz, xx, cc, yy):
        return (zz * 8 + xx * 2 + cc, yy)

    def chunk_of(home):
        return home // 4

    def turn(a, d, n):
        return lax.rem(a + d, n)

    def landed(ref, sem):
        pltpu.make_async_remote_copy(
            ref, ref, D_SENT, sem, device_id=at(z, x, 1 - c, y), device_id_type=MESH
        ).wait_recv()

    sent_by_all, sent_by, sent_home = [], ([], []), []

    def send_away(source, target, send_sem, recv_sem, device, sent_list, alike):
        pltpu.make_async_remote_copy(
            source, target, send_sem, recv_sem, device_id=device, device_id_type=MESH
        ).start()
        sent_list.append((alike, send_sem))

    def left(alike, sem):
        ref = alike[0].at[alike[1]]
        pltpu.make_async_remote_copy(
            ref, ref, sem, dr_sem, device_id=at(z, x, 1 - c, y), device_id_type=MESH
        ).wait_send()

    barrier = pltpu.get_barrier_semaphore()

    def enter(device):
        pl.semaphore_signal(barrier, inc=1, device_id=device, device_id_type=MESH)

    wide = pl.multiple_of((ep // 32) * 128, 128)
    sources = list(hbm)
    sources[15] = ids_h.at[:, pl.ds(wide, 128)]
    loads = [
        pltpu.make_async_copy(source, target, load.at[LOAD_GROUP[i]])
        for i, (source, target) in enumerate(zip(sources, scratch[:20]))
    ]
    @pl.when(c == 1)
    def _():
        for d in FAR_FIRST:
            enter(at(turn(z, d, NZ), x, 1, y))

    for i in (0, 1, 2):
        loads[i].start()
    for d in range(1, NY):
        enter(at(z, x, 0, turn(y, d, NY)))
    for dx, dy in PLANE:
        if dx or dy:
            enter(at(z, turn(x, dx, NX), 1, turn(y, dy, NY)))
    enter(at(z, x, 1 - c, y))
    near_count = 2 * (NY - 1) + 1
    far_count = (NZ - 1) + 2 * (NX * NY - 1) + 1

    for i in (3, 4, 5, 6, 7, 11, 12, 8, 9, 10, 13, 14, 15, 16, 17, 18, 19):
        loads[i].start()

    loads[0].wait()
    loads[1].wait()
    tokens = tok[...].astype(F32)
    normed_in = rms(tokens, row_of(gain[...]))
    loads[2].wait()
    u = dot(normed_in, inw[...]).astype(BF16).astype(F32)

    rows = SEQ * GROUPS
    own_group = iota((rows, CHANNELS), 0) % GROUPS == iota((rows, CHANNELS), 1) // 16
    spread = jnp.broadcast_to(u[:, None, :], (SEQ, GROUPS, CHANNELS)).reshape(rows, CHANNELS)
    spread = jnp.where(own_group, spread, 0.0).astype(BF16)
    for i in (3, 4, 5, 6, 7):
        loads[i].wait()
    group_row = iota((GROUPS, STATE), 0)
    log_step = jnp.zeros((GROUPS, STATE), F32)
    for g in range(GROUPS):
        log_step = jnp.where(group_row == g, steps[g], log_step)
    step_size = jnp.exp(log_step)
    lam_real, frequency = -decay[...], freq[...]
    magnitude = jnp.exp(lam_real * step_size)
    turned = frequency * step_size
    bar_real = magnitude * jnp.cos(turned)
    bar_imag = magnitude * jnp.sin(turned)
    denom = lam_real * lam_real + frequency * frequency
    minus_one = bar_real - 1.0
    factor_real = (minus_one * lam_real + bar_imag * frequency) / denom
    factor_imag = (bar_imag * lam_real - minus_one * frequency) / denom

    def per_row(v):
        return jnp.broadcast_to(v[None], (SEQ, GROUPS, STATE)).reshape(rows, STATE)

    def drive(ref):
        high, low = split(ref[...].reshape(CHANNELS, STATE))
        return dot(spread, high) + dot(spread, low)

    drive_r, drive_i = drive(inr), drive(ini)
    bar_real, bar_imag = per_row(bar_real), per_row(bar_imag)
    factor_real, factor_imag = per_row(factor_real), per_row(factor_imag)
    loads[11].wait()
    loads[12].wait()
    state_r, state_i = st_r[...].reshape(rows, STATE), st_i[...].reshape(rows, STATE)
    new_r = (bar_real * state_r - bar_imag * state_i) + (factor_real * drive_r - factor_imag * drive_i)
    new_i = (bar_real * state_i + bar_imag * state_r) + (factor_real * drive_i + factor_imag * drive_r)
    newr_o[...] = new_r.reshape(SEQ, GROUPS, STATE)
    newi_o[...] = new_i.reshape(SEQ, GROUPS, STATE)

    for i in (8, 9, 10):
        loads[i].wait()

    def read(values, ref):
        high, low = split(values)
        ref_high, ref_low = split(ref[...].reshape(CHANNELS, STATE))
        return dot_t(high, ref_high) + dot_t(high, ref_low) + dot_t(low, ref_high)

    readout = jnp.where(own_group, read(new_r, outr) - read(new_i, outi), 0.0)
    readout = readout.reshape(SEQ, GROUPS, CHANNELS).sum(axis=1)
    readout = readout + row_of(skip[...]) * u
    activated = jax.nn.gelu(readout).astype(BF16)
    loads[13].wait()
    delta[y] = dot(activated, outw[...]).astype(BF16)

    @pl.when(c == 0)
    def _():
        pl.semaphore_wait(barrier, near_count)
        pl.semaphore_signal(near_sem, inc=1, device_id=at(z, x, 1, y), device_id_type=MESH)

    @pl.when(c == 1)
    def _():
        pl.semaphore_wait(near_sem, 1)

    delta_copies = [
        pltpu.make_async_remote_copy(
            delta.at[y], delta.at[y], D_SENT, dr_sem,
            device_id=at(z, x, c, turn(y, d, NY)), device_id_type=MESH,
        )
        for d in range(1, NY)
    ]
    for copy in delta_copies:
        copy.start()

    for i in (14, 15, 16):
        loads[i].wait()
    first = (ep % 32) * SEQ
    names = [[ids[k, first + s] for k in range(2)] for s in range(SEQ)]
    weights = [[rw[k, s] for k in range(2)] for s in range(SEQ)]

    def table(expert, slot, shape):
        taken = jnp.zeros(shape, I32)
        picks, scales = [], []
        for s in range(SEQ):
            routes = [expert == names[s][k] for k in range(2)]
            named = routes[0] | routes[1]
            here = named & (taken == slot)
            picks.append(jnp.where(here, 1.0, 0.0))
            scale = jnp.where(routes[0], weights[s][0], 0.0) + jnp.where(routes[1], weights[s][1], 0.0)
            scales.append(jnp.where(here, scale, 0.0))
            taken = taken + jnp.where(named, 1, 0)
        return picks, scales

    pick_row = iota((16, QUARTER), 0)
    picks, _ = table(pick_row // 2, pick_row % 2, (16, QUARTER))
    ffn_gain = row_of(fgain[...])

    landed(delta.at[0 : NY - 1], dr_sem)
    total = tokens
    for i in range(NY):
        total = total + delta[i].astype(F32)
    hidden_state = total.astype(BF16).astype(F32)
    hid32[...] = hidden_state
    norm32[...] = rms(hidden_state, ffn_gain).astype(F32)
    lanes = pl.ds(pl.multiple_of(y * QUARTER, QUARTER), QUARTER)
    own = norm32[:, lanes]
    chosen = picks[0] * own[0:1, :]
    for s in range(1, SEQ):
        chosen = chosen + picks[s] * own[s : s + 1, :]
    pick32[...] = chosen
    for e in range(8):
        pick[e] = pick32[2 * e : 2 * e + 2, :].astype(BF16)

    @pl.when(c == 1)
    def _():
        pl.semaphore_wait(barrier, far_count)
        pl.semaphore_signal(far_sem, inc=1, device_id=at(z, x, 0, y), device_id_type=MESH)

    @pl.when(c == 0)
    def _():
        pl.semaphore_wait(far_sem, 1)

    for d in FAR_FIRST:
        to = turn(z, d, NZ)
        send_away(pick.at[to // 2], zin.at[z, c], Z_SENT, zr_sem.at[chunk_of(z)], at(to, x, 1, y), sent_by_all, (pick, 0))
    own_slots = (pick.at[z // 2], zin.at[z, c])

    @pl.when(c == 1)
    def _():
        pltpu.make_async_copy(*own_slots, zr_sem.at[chunk_of(z)]).start()

    @pl.when(c == 0)
    def _():
        send_away(*own_slots, Z_SENT, zr_sem.at[chunk_of(z)], at(z, x, 1, y), sent_by[0], (pick, 0))

    def take_chunk(k):
        low, high = CHUNKS[k]
        block = 2 * (high - low)
        landed(zin.at[low:high], zr_sem.at[k])
        for core in range(NC):
            for i in range(high - low):
                row = core * block + 2 * i
                sum32[row : row + 2, :] = zin[low + i, core].astype(F32)
        gat[k][y, x] = sum32[0 : 2 * block, :].astype(BF16)

    def pass_on(slots, alike, k, sem, dx, dy):
        to = at(z, turn(x, dx, NX), 1, turn(y, dy, NY))
        send_away(slots, slots, G_SENT, gr_sem.at[k, sem], to, sent_by[1], (gat[k], alike))

    def line(k, distance):
        if k == X_FIRST:
            return gat[k].at[turn(y, NY - distance, NY), :]
        return gat[k].at[:, turn(x, NX - distance, NX)]

    def gather_at_once(k):
        for dx, dy in reversed(PLANE):
            if dx or dy:
                pass_on(gat[k].at[y, x], (0, 0), k, dx, dx, dy)

    def gather_first(k):
        for d in (2, 1, 3):
            dx, dy = (d, 0) if k == X_FIRST else (0, d)
            pass_on(gat[k].at[y, x], (0, 0), k, 0, dx, dy)

    def gather_second(k):
        spread_chunk(k, (0,))
        for d in (2, 1, 3):
            dx, dy = (0, d) if k == X_FIRST else (d, 0)
            pass_on(line(k, 0), (slice(None), 0), k, d, dx, dy)

    def spread_chunk(k, distances):
        for d in distances:
            landed(gat[k].at[0, (0 if d else 1) : NX], gr_sem.at[k, d])
            send_away(
                line(k, d), line(k, d), F_SENT, fr_sem.at[k], at(z, x, 0, y), sent_by[1], (gat[k], (slice(None), 0))
            )

    def up_chunk(k):
        @pl.when(c == 0)
        def _():
            landed(gat[k], fr_sem.at[k])

        rows = hid[k].shape[0]
        gate_pre = jnp.zeros((rows, HID), F32)
        up_pre = jnp.zeros((rows, HID), F32)
        for q in range(NY):
            block = gat[k][q].reshape(rows, QUARTER)
            gate_pre = gate_pre + dot(block, gw[q * QUARTER : (q + 1) * QUARTER, :])
            up_pre = up_pre + dot(block, uw[q * QUARTER : (q + 1) * QUARTER, :])
        units = pl.ds(pl.multiple_of(y * HID, HID), HID)
        hid[k][:, units] = (jax.nn.silu(gate_pre) * up_pre).astype(BF16)
        own_units = hid[k].at[:, units]
        for d in (2, 1, 3):
            to = at(z, x, c, turn(y, d, NY))
            send_away(own_units, own_units, H_SENT, hr_sem.at[k], to, sent_by_all, (hid[k], (slice(None), slice(0, HID))))

    def down_chunk(k):
        landed(hid[k].at[:, 0 : (NY - 1) * HID], hr_sem.at[k])
        send[k][...] = dot(hid[k][...], dw[...]).astype(BF16).reshape(send[k].shape)
        for dx in (2, 1, 3):
            to = turn(x, dx, NX)
            slot = recv[k].at[2 * dx - 1 + c]
            send_away(send[k].at[to], slot, R_SENT, rr_sem.at[k], at(z, to, SUMS[k], y), sent_by_all, (send[k], 0))

        @pl.when(c != SUMS[k])
        def _():
            home = at(z, x, SUMS[k], y)
            kept = sent_by[1 - SUMS[k]]
            send_away(send[k].at[x], recv[k].at[0], R_SENT, rr_sem.at[k], home, kept, (send[k], 0))

    def home_chunk(k):
        landed(recv[k], rr_sem.at[k])
        total = send[k][x].astype(F32)
        for i in range(NC * NX - 1):
            total = total + recv[k][i].astype(F32)
        low, high = CHUNKS[k]
        block = 2 * (high - low)
        sum32[0 : 2 * block, :] = total
        for i in range(high - low):
            for core in range(NC):
                row = core * block + 2 * i
                back[k][i, core] = sum32[row : row + 2, :].astype(BF16)
            home = low + i
            slots, other = back[k].at[i, 1 - SUMS[k]], at(home, x, 1 - SUMS[k], y)
            send_away(slots, zout.at[z], B_SENT, br_sem, other, sent_by[SUMS[k]], (pick, 0))

            @pl.when(z != home)
            def _():
                slots, same = back[k].at[i, SUMS[k]], at(home, x, SUMS[k], y)
                send_away(slots, zout.at[z], B_SENT, br_sem, same, sent_home, (pick, 0))

            @pl.when(z == home)
            def _():
                pltpu.make_async_copy(back[k].at[i, SUMS[k]], zout.at[z], br_sem).start()

    on_core_1 = pl.when(c == 1)

    @on_core_1
    def _():
        take_chunk(0)
        gather_at_once(0)
        for k in (1, 2, 3):
            take_chunk(k)
            gather_first(k)
        spread_chunk(0, (0, 1, 3, 2))
        gather_second(1)
        gather_second(2)

    loads[17].wait()
    loads[18].wait()
    up_chunk(0)

    @on_core_1
    def _():
        spread_chunk(1, (1, 3, 2))
        gather_second(3)

    loads[19].wait()
    down_chunk(0)
    on_core_1(lambda: spread_chunk(2, (1, 3, 2)))
    up_chunk(1)
    up_chunk(2)
    on_core_1(lambda: spread_chunk(3, (1, 3, 2)))
    up_chunk(3)
    on_core_1(lambda: home_chunk(0))
    down_chunk(1)
    down_chunk(2)
    down_chunk(3)
    on_core_1(lambda: home_chunk(1))
    on_core_1(lambda: home_chunk(2))
    pl.when(c == SUMS[3])(lambda: home_chunk(3))

    back_row = iota((2 * NZ, QUARTER), 0)
    _, scales = table(back_row // 4, back_row % 2, (2 * NZ, QUARTER))
    landed(zout, br_sem)
    for p in range(NZ):
        out32[2 * p : 2 * p + 2, :] = zout[p].astype(F32)
    pieces = out32[...]
    routed = [jnp.sum(scales[s] * pieces, axis=0, keepdims=True) for s in range(SEQ)]
    mixed_o[...] = (hid32[:, lanes] + jnp.concatenate(routed, axis=0)).astype(BF16)

    for copy in delta_copies:
        copy.wait_send()
    for copy in sent_by_all:
        left(*copy)
    for core in range(NC):

        @pl.when(c == core)
        def _():
            for copy in sent_by[core]:
                left(*copy)

    for home, copy in enumerate(sent_home):

        @pl.when((c == SUMS[home // 4]) & (z != home))
        def _():
            left(*copy)


def store_kernel(*refs):
    sources, targets, sem = refs[:3], refs[3:6], refs[6]
    copies = [pltpu.make_async_copy(s, t, sem.at[i]) for i, (s, t) in enumerate(zip(sources, targets))]
    for copy in copies:
        copy.start()
    for copy in copies:
        copy.wait()


def shards(*args):
    args = list(args)
    for i in (1, 14):
        args[i] = args[i].reshape(16, 128)
    args[10] = args[10].reshape(2, 128)
    for i in (6, 7):
        args[i] = args[i].transpose(0, 2, 1)
    args[15], args[16] = args[15].T, args[16].T
    held = []
    for i, arg in enumerate(args):
        if i in (5, 16):
            held.append(pltpu.SMEM(arg.shape, arg.dtype))
        elif i == 15:
            held.append(pltpu.SMEM((2, 128), arg.dtype))
        else:
            held.append(pltpu.VMEM(arg.shape, arg.dtype))
    dma = pltpu.SemaphoreType.DMA
    shapes = (((SEQ, QUARTER), BF16), ((SEQ, GROUPS, STATE), F32), ((SEQ, GROUPS, STATE), F32))
    scratch = held + [
        pltpu.VMEM((NY, SEQ, WIDTH), BF16),
        pltpu.VMEM((SEQ, WIDTH), F32),
        pltpu.VMEM((SEQ, WIDTH), F32),
        pltpu.VMEM((16, QUARTER), F32),
        pltpu.VMEM((8, 2, QUARTER), BF16),
        pltpu.VMEM((NZ, NC, 2, QUARTER), BF16),
        pltpu.VMEM((16, QUARTER), F32),
        pltpu.VMEM((NZ, 2, QUARTER), BF16),
        pltpu.VMEM((2 * NZ, QUARTER), F32),
        dma((9,)), dma,
        dma, dma((4,)), dma((4, NX)), dma((4,)), dma((4,)), dma((4,)), dma,
        pltpu.SemaphoreType.REGULAR,
        pltpu.SemaphoreType.REGULAR,
    ]
    for low, high in CHUNKS:
        block = 2 * NC * (high - low)
        scratch += [
            pltpu.VMEM((NY, NX, block, QUARTER), BF16),
            pltpu.VMEM((NX * block, NY * HID), BF16),
            pltpu.VMEM((NX, block, QUARTER), BF16),
            pltpu.VMEM((NC * NX - 1, block, QUARTER), BF16),
            pltpu.VMEM((high - low, NC, 2, QUARTER), BF16),
        ]
    anywhere = pl.BlockSpec(memory_space=pl.ANY)
    near = pl.BlockSpec(memory_space=pltpu.VMEM)
    results = pl.pallas_call(
        kernel,
        out_shape=tuple(pltpu.VMEM(*shape) for shape in shapes),
        in_specs=[anywhere] * 20,
        out_specs=(near,) * 3,
        scratch_shapes=scratch,
        compiler_params=pltpu.CompilerParams(
            collective_id=0, has_side_effects=True, vmem_limit_bytes=VMEM_LIMIT
        ),
    )(*args)
    return pl.pallas_call(
        store_kernel,
        out_shape=tuple(jax.ShapeDtypeStruct(*shape) for shape in shapes),
        in_specs=[anywhere] * 3,
        out_specs=(anywhere,) * 3,
        scratch_shapes=[dma((3,))],
        compiler_params=pltpu.CompilerParams(vmem_limit_bytes=VMEM_LIMIT),
    )(*[pltpu.with_memory_space_constraint(r, pltpu.VMEM) for r in results])


def solution(mesh):
    in_specs = (
        P("ep", None), P(), P(None, "tp"), P("tp", None), P("tp", None), P("tp"),
        P("tp", None, None), P("tp", None, None), P("tp", None, None), P("tp", None, None), P("tp"),
        P("ep", "tp", None), P("ep", "tp", None), P("tp", None), P(), P(), P("ep", None),
        P(None, ("ep", "tp")), P(None, ("ep", "tp")), P("ep", "tp"),
    )
    out_specs = (P("ep", "tp"), P("ep", "tp", None), P("ep", "tp", None))
    return jax.shard_map(shards, mesh=mesh, in_specs=in_specs, out_specs=out_specs, check_vma=False)
```
